32 devices in a mesh: grp: 2 (over y), sp: 8 (over z, core), tp: 2 (over x).
Axes of the slice: x: 2, y: 2, z: 4, core: 2. Of those that a mesh axis runs over, the one named last changes fastest.
Arguments:
- queries_a: bfloat16 [4096, 2, 512], P(('grp', 'sp'), None, 'tp'), parts along dimension 0, may hold values from -120 to 120
- keys_a: bfloat16 [4096, 2, 512], P(('grp', 'sp'), None, 'tp'), parts along dimension 0, may hold values from -6 to 6
- values_a: bfloat16 [4096, 1024], P(('grp', 'sp'), 'tp'), parts along dimension 0, may hold values from -6 to 6
- queries_b: bfloat16 [4096, 2, 512], P(('grp', 'sp'), None, 'tp'), parts along dimension 0, may hold values from -120 to 120
- keys_b: bfloat16 [4096, 2, 512], P(('grp', 'sp'), None, 'tp'), parts along dimension 0, may hold values from -6 to 6
- values_b: bfloat16 [4096, 1024], P(('grp', 'sp'), 'tp'), parts along dimension 0, may hold values from -6 to 6
- lambdas: float32 [12], replicated, may hold values from 0.3 to 0.8
- head_gain_a: float32 [256], replicated, may hold values from 0.1 to 1.9
- head_gain_b: float32 [128], replicated, may hold values from 0.1 to 1.9
- out_a: bfloat16 [1024, 2048], P('tp'), may hold values from -0.125 to 0.125
- out_b: bfloat16 [1024, 2048], P('tp'), may hold values from -0.125 to 0.125
- residual: bfloat16 [4096, 2048], P(('grp', 'sp', 'tp')), parts along dimension 0, may hold values from -6 to 6
- gain_mix: float32 [2048], replicated, may hold values from 0.1 to 1.9
- gain_pre: float32 [2048], replicated, may hold values from 0.1 to 1.9
- gain_post: float32 [2048], replicated, may hold values from 0.1 to 1.9
- routes: int32 [4096, 4], P(('grp', 'sp', 'tp')), parts along dimension 0, may hold values from 0 to 7, all different within a row; in each aligned block of 128 rows (0 to 127, 128 to 255, ...) at most 80 rows name the same one
- route_weights: float32 [4096, 4], P(('grp', 'sp', 'tp')), parts along dimension 0, may hold values from 0.05 to 1
- expert_gate: bfloat16 [8, 2048, 2048], P('sp', None, 'tp'), may hold values from -1 to 1
- expert_up: bfloat16 [8, 2048, 2048], P('sp', None, 'tp'), may hold values from -1 to 1
- expert_down: bfloat16 [8, 2048, 2048], P('sp', 'tp'), may hold values from -0.125 to 0.125
Outputs:
- layer_out: bfloat16 [4096, 2048], P(('grp', 'sp', 'tp')), parts along dimension 0
The draws below stay inside these ranges and needn't reach their ends.
There are 2 independent parts, one for each index of `grp`. The reference program is written for one: setup_inputs(seed, part) draws one part's arguments, and reference() takes and returns one part's arrays. A program takes and returns all parts, laid end to end along the dimension named above; an argument that names none is the same for every part. Nothing has to cross between parts.
Inputs may be any that keep to these rules, and one draw needn't show every extreme that they name: `routes`: in each aligned block of 128 rows (the rows of one device) no expert is named by more than 80 rows, a bound that some blocks reach.
All inputs are finite; a program needn't handle non-finite values.
Results may differ from the reference program's by a relative error of at most 0.018.
Values may be sent and summed in bfloat16 or wider, within the bound.
A program may use at most 128 MiB of HBM per device.

```python
import math
import jax
import jax.numpy as jnp
import numpy as np
from jax import lax

HA = 4
HB = 8
DA = 128
DB = 64
D = 2048
FF = 2048
TOP_K = 4
TOK_DEV = 256
TOKENS = 2048
TOKSUB = 128
EXPERTS = 8
CAP = 80
N_TP = 2


def pair_fields(key, salt, width):
    keys = jnp.clip(jax.random.normal(jax.random.fold_in(key, salt), (TOKENS, 2, width), jnp.float32) * 1.32, -6.0, 6.0)
    queries = jnp.clip(jax.random.normal(jax.random.fold_in(key, salt + 1), (TOKENS, 2, width), jnp.float32) * 1.32, -6.0, 6.0)
    return (queries, keys)


def draw_queries_a(key, part):
    queries, keys = pair_fields(key, 11, HA * DA)
    return queries.astype(jnp.bfloat16)


def draw_keys_a(key, part):
    queries, keys = pair_fields(key, 11, HA * DA)
    return keys.astype(jnp.bfloat16)


def draw_queries_b(key, part):
    queries, keys = pair_fields(key, 21, HB * DB)
    return queries.astype(jnp.bfloat16)


def draw_keys_b(key, part):
    queries, keys = pair_fields(key, 21, HB * DB)
    return keys.astype(jnp.bfloat16)


def expert_field(key, salt):
    base = jnp.clip(jax.random.normal(jax.random.fold_in(key, salt), (EXPERTS, D, FF), jnp.float32), -6.0, 6.0)
    factor = 1.0
    return jnp.clip(base * factor / jnp.sqrt(jnp.float32(D)), -1.0, 1.0)


def draw_expert_gate(key, part):
    return expert_field(key, 31).astype(jnp.bfloat16)


def draw_expert_up(key, part):
    return expert_field(key, 37).astype(jnp.bfloat16)


def block_scale(key, dims, cuts, smallest, high):
    def one(position, parts):
        heights = jax.random.uniform(jax.random.fold_in(jax.random.fold_in(key, 6), position), (parts,), jnp.float32, smallest / len(cuts), high / len(cuts))
        return jnp.repeat(jnp.exp(heights), dims[position] // parts).reshape((-1,) + (1,) * (len(dims) - position - 1))

    loudness = one(*cuts[0])
    for cut in cuts[1:]:
        loudness = loudness * one(*cut)
    return loudness


def assign_block(key, own, number, rows, amount, top, most, skew):
    ranking = jax.random.permutation(key, amount)
    packed, common = load_shares(amount, rows * top, most, skew, True), load_shares(amount, rows * top, most, skew, False)
    places = jnp.arange(amount)

    def named(lengths, rotation):
        used = int((lengths > 0).sum())
        fixed = max(1, used // 4)
        moved = fixed + (places - fixed + rotation * (used - fixed)) % max(1, amount - fixed)
        return jnp.zeros((amount,), jnp.int32).at[ranking[jnp.where(places < fixed, places, moved)]].set(jnp.asarray(lengths, jnp.int32))

    lengths = jnp.where(number % 4 == 0, named(packed, number // 4), named(common, number - number // 4 - 1))
    mixed = jax.random.permutation(jax.random.fold_in(own, 3), amount)
    source_of, sink = mixed[0:amount // 2 * 2:2], mixed[1:amount // 2 * 2:2]
    room = jnp.minimum(lengths[source_of] - 1, most - lengths[sink]) // 2
    room = jnp.where((source_of == ranking[0]) | (sink == ranking[0]) | (lengths[sink] == 0), 0, jnp.maximum(room, 0))
    moved = jax.random.randint(jax.random.fold_in(own, 4), (amount // 2,), 0, 1 << 20) % (room + 1)
    lengths = lengths.at[source_of].add(-moved).at[sink].add(moved)
    items = jnp.searchsorted(jnp.cumsum(lengths), jnp.arange(rows * top), side="right").astype(jnp.int32)
    grid = items.reshape(top, rows).T
    grid = grid[jax.random.permutation(jax.random.fold_in(own, 1), rows)]
    rotation = jax.random.randint(jax.random.fold_in(own, 2), (rows, 1), 0, top)
    return jnp.take_along_axis(grid, (jnp.arange(top)[None, :] + rotation) % top, axis=1)


def load_shares(amount, total, limit, lean, full):
    weights = [(1 << 20) // math.isqrt(standing ** lean) + 1 for standing in range(1, amount + 1)]
    largest = limit if full else min(limit, max(-(-total // amount), total * weights[0] // sum(weights)))
    least = 1 if total - largest >= amount - 1 else 0
    given, spare = [largest] + [least] * (amount - 1), total - largest - least * (amount - 1)
    while spare > 0:
        candidates = [i for i in range(1, amount) if given[i] < largest] or [i for i in range(1, amount) if given[i] < limit]
        pool, budget = sum([weights[i] for i in candidates]), spare
        for i in candidates:
            extra = min(limit - given[i], max(1, budget * weights[i] // pool), spare)
            given[i] = given[i] + extra
            spare = spare - extra
    return np.array(given)


def centred(stream_key, dims, deviation, most, split=(), kind=jnp.bfloat16):
    drawn = jax.random.normal(stream_key, dims, jnp.float32) * deviation
    if len(split) > 0:
        drawn = block_scale(stream_key, dims, split, -0.22, 0.18) * drawn
    return jnp.clip(drawn, min=-most, max=most).astype(kind)


def setup_inputs(seed: int = 0, part: int = 0) -> dict:
    seeds = jax.random.split(jax.random.key(seed), 21)
    part_splits = jax.random.split(jax.random.fold_in(seeds[20], part), 21)
    queries_a = draw_queries_a(jax.random.fold_in(jax.random.fold_in(seeds[20], part), 71), part)
    keys_a = draw_keys_a(jax.random.fold_in(jax.random.fold_in(seeds[20], part), 71), part)
    values_a = centred(part_splits[2], (TOKENS, HA * 2 * DA), 1.0, 6.0, ((0, 8), (1, 2)))
    queries_b = draw_queries_b(jax.random.fold_in(jax.random.fold_in(seeds[20], part), 71), part)
    keys_b = draw_keys_b(jax.random.fold_in(jax.random.fold_in(seeds[20], part), 71), part)
    values_b = centred(part_splits[5], (TOKENS, HB * 2 * DB), 1.0, 6.0, ((0, 8), (1, 2)))
    lambdas = jnp.clip(jax.random.uniform(seeds[6], (HA + HB,), jnp.float32, 0.3, 0.8), 0.3, 0.8)
    head_gain_a = jnp.clip(1.0 + 0.18 * jax.random.normal(seeds[7], (2 * DA,), jnp.float32), 0.1, 1.9)
    head_gain_b = jnp.clip(1.0 + 0.18 * jax.random.normal(seeds[8], (2 * DB,), jnp.float32), 0.1, 1.9)
    out_a = centred(seeds[9], (HA * 2 * DA, D), D ** -0.5, 0.125, ((0, 2),))
    out_b = centred(seeds[10], (HB * 2 * DB, D), D ** -0.5, 0.125, ((0, 2),))
    residual = centred(part_splits[11], (TOKENS, D), 1.0, 6.0, ((0, 16),))
    gain_mix = jnp.clip(1.0 + 0.18 * jax.random.normal(seeds[12], (D,), jnp.float32), 0.1, 1.9)
    gain_pre = jnp.clip(1.0 + 0.18 * jax.random.normal(seeds[13], (D,), jnp.float32), 0.1, 1.9)
    gain_post = jnp.clip(1.0 + 0.18 * jax.random.normal(seeds[14], (D,), jnp.float32), 0.1, 1.9)
    routes_keys = jax.random.split(jax.random.fold_in(part_splits[15], 1), TOKENS // TOKSUB)
    routes_turns = jax.random.permutation(jax.random.fold_in(part_splits[15], 3), TOKENS // TOKSUB)
    routes = jax.vmap(lambda own, number: assign_block(jax.random.fold_in(part_splits[15], 2), own, number, TOKSUB, EXPERTS, TOP_K, CAP, 1))(routes_keys, routes_turns).reshape((TOKENS, TOP_K))
    route_weights = jnp.clip(0.05 + 0.95 * jax.random.uniform(part_splits[16], (TOKENS, TOP_K), jnp.float32) ** block_scale(part_splits[16], (TOKENS, TOP_K), ((0, 16),), -0.2, 0.2), 0.05, 1.0)
    expert_gate = draw_expert_gate(jax.random.fold_in(seeds[20], 71), part)
    expert_up = draw_expert_up(jax.random.fold_in(seeds[20], 71), part)
    expert_down = centred(seeds[19], (EXPERTS, FF, D), FF ** -0.5, 0.125, ((0, 8), (1, 2)))
    return dict(queries_a=queries_a, keys_a=keys_a, values_a=values_a, queries_b=queries_b, keys_b=keys_b, values_b=values_b, lambdas=lambdas, head_gain_a=head_gain_a, head_gain_b=head_gain_b, out_a=out_a, out_b=out_b, residual=residual, gain_mix=gain_mix, gain_pre=gain_pre, gain_post=gain_post, routes=routes, route_weights=route_weights, expert_gate=expert_gate, expert_up=expert_up, expert_down=expert_down)


def rms_norm(values, gain_vec):
    return values * lax.rsqrt(lax.optimization_barrier(jnp.mean(values * values, -1, keepdims=True)) + 1e-06) * gain_vec.astype(jnp.float32)

def attend_group(queries, keys, values, weights_two, gain_vec, head_size):
    heads = queries.shape[2] // head_size
    query_all = queries.astype(jnp.float32).reshape(TOKENS, 2, heads, head_size)
    key_all = keys.astype(jnp.float32).reshape(TOKENS, 2, heads, head_size)
    value_all = values.astype(jnp.float32).reshape(TOKENS, heads, 2 * head_size)
    span_rows = 512 if TOKENS % 512 == 0 else TOKENS
    key_pos = jnp.arange(TOKENS, dtype=jnp.int32)

    def one_block(first_row):
        query_rows = lax.dynamic_slice_in_dim(query_all, first_row, span_rows, 0)
        query_pos = first_row + jnp.arange(span_rows, dtype=jnp.int32)
        visible = (key_pos[None, :] <= query_pos[:, None])[None, :, None, :]
        scores = jnp.einsum('qmhd,kmhd->mqhk', query_rows, key_all, precision=lax.Precision.HIGHEST) * head_size ** (-0.5)
        scores = jnp.where(visible, scores, -1e+30)
        row_top = lax.optimization_barrier(jnp.max(scores, -1, keepdims=True))
        exp_terms = jnp.where(visible, jnp.exp(scores - row_top), 0.0)
        totals = lax.optimization_barrier(jnp.sum(exp_terms, -1))
        rounded = lax.optimization_barrier(exp_terms.astype(jnp.bfloat16)).astype(jnp.float32)
        accum = jnp.einsum('mqhk,khe->mqhe', rounded, value_all, precision=lax.Precision.HIGHEST)
        mixture = accum[0] / totals[0][..., None] - weights_two[None, :, None] * accum[1] / totals[1][..., None]
        normed = rms_norm(mixture, gain_vec)
        return normed.reshape(span_rows, heads * 2 * head_size).astype(jnp.bfloat16)
    firsts = jnp.arange(0, TOKENS, span_rows, dtype=jnp.int32)
    return lax.map(one_block, firsts).reshape(TOKENS, heads * 2 * head_size)

def slot_numbers(flat_ids):
    onehot = (flat_ids[:, None] == jnp.arange(EXPERTS, dtype=jnp.int32)[None, :]).astype(jnp.int32)
    before = jnp.cumsum(onehot, 0) - onehot
    return lax.optimization_barrier(jnp.sum(before * onehot, 1)).astype(jnp.int32)

def reference(queries_a, keys_a, values_a, queries_b, keys_b, values_b, lambdas, head_gain_a, head_gain_b, out_a, out_b, residual, gain_mix, gain_pre, gain_post, routes, route_weights, expert_gate, expert_up, expert_down):
    heads_out_a = attend_group(queries_a, keys_a, values_a, lambdas[:HA], head_gain_a, DA)
    heads_out_b = attend_group(queries_b, keys_b, values_b, lambdas[HA:], head_gain_b, DB)
    width_a = heads_out_a.shape[1] // N_TP
    width_b = heads_out_b.shape[1] // N_TP
    mixed_rows = jnp.zeros((TOKENS, D), jnp.float32)
    for part_index in range(N_TP):
        part_a = jnp.dot(heads_out_a[:, part_index * width_a:(part_index + 1) * width_a], out_a[part_index * width_a:(part_index + 1) * width_a], preferred_element_type=jnp.float32)
        part_b = jnp.dot(heads_out_b[:, part_index * width_b:(part_index + 1) * width_b], out_b[part_index * width_b:(part_index + 1) * width_b], preferred_element_type=jnp.float32)
        mixed_rows = mixed_rows + lax.optimization_barrier((part_a + part_b).astype(jnp.bfloat16)).astype(jnp.float32)
    after_mix = (residual.astype(jnp.float32) + rms_norm(mixed_rows, gain_mix)).astype(jnp.bfloat16)
    normed = rms_norm(after_mix.astype(jnp.float32), gain_pre).astype(jnp.bfloat16)
    sub_rows = TOK_DEV // N_TP
    blocks = TOKENS // sub_rows
    route_blocks = routes.astype(jnp.int32).reshape(blocks, sub_rows * TOP_K)
    slot_ids = jax.vmap(slot_numbers)(route_blocks)
    block_ids = jnp.broadcast_to(jnp.arange(blocks, dtype=jnp.int32)[:, None], route_blocks.shape)
    token_ids = jnp.repeat(jnp.arange(TOKENS, dtype=jnp.int32).reshape(blocks, sub_rows), TOP_K, axis=1)
    table = jnp.full((EXPERTS, blocks, CAP), TOKENS, jnp.int32).at[route_blocks, block_ids, slot_ids].set(token_ids)
    padded = jnp.concatenate([normed, jnp.zeros((1, D), jnp.bfloat16)], 0)
    hidden_block = FF // N_TP

    def expert_work(expert_id):
        rows = padded[table[expert_id].reshape(-1)]
        gate_pre = jnp.dot(rows, expert_gate[expert_id], preferred_element_type=jnp.float32)
        up_pre = jnp.dot(rows, expert_up[expert_id], preferred_element_type=jnp.float32)
        glu_part = jnp.minimum(gate_pre, 7.0)
        lin_part = jnp.clip(up_pre, -7.0, 7.0)
        hidden = (glu_part * jax.nn.sigmoid(1.702 * glu_part) * (lin_part + 1.0)).astype(jnp.bfloat16)
        summed = jnp.zeros((rows.shape[0], D), jnp.float32)
        for part_index in range(N_TP):
            piece_sum = jnp.dot(hidden[:, part_index * hidden_block:(part_index + 1) * hidden_block], expert_down[expert_id][part_index * hidden_block:(part_index + 1) * hidden_block], preferred_element_type=jnp.float32)
            summed = summed + lax.optimization_barrier(piece_sum.astype(jnp.bfloat16)).astype(jnp.float32)
        return summed.astype(jnp.bfloat16).reshape(blocks, CAP, D)
    outputs = lax.map(expert_work, jnp.arange(EXPERTS, dtype=jnp.int32))
    picked = outputs[route_blocks, block_ids, slot_ids].astype(jnp.float32)
    weighted = picked * route_weights.reshape(blocks, sub_rows * TOP_K)[..., None].astype(jnp.float32)
    routed = lax.optimization_barrier(jnp.sum(weighted.reshape(TOKENS, TOP_K, D), 1))
    return (after_mix.astype(jnp.float32) + rms_norm(routed, gain_post)).astype(jnp.bfloat16)
```

```python
import jax
import jax.numpy as jnp
from jax import lax
from jax.experimental import pallas as pl
from jax.experimental.pallas import tpu as pltpu
from jax.sharding import PartitionSpec as P

HA = 4
DA = 128
DB = 64


def rms_norm(values, gain_vec):
    return values * lax.rsqrt(jnp.mean(values * values, -1, keepdims=True) + 1e-06) * gain_vec


MESH = pl.DeviceIdType.MESH
CORES = 2
PIECES = 2
LOG2E = 1.4426950408889634
VMEM_BYTES = 60 * 1024 * 1024


def place():
    sp = lax.axis_index("sp")
    return sp // CORES, sp % CORES, lax.axis_index("tp")


def greet(chips, tps):
    chip, core, tp = place()
    barrier = pltpu.get_barrier_semaphore()
    for step in range(1, chips):
        other = (chip + step) % chips
        pl.semaphore_signal(
            barrier, inc=1, device_id={"sp": other * CORES + core, "tp": tp}, device_id_type=MESH
        )
    for step in range(1, tps):
        pl.semaphore_signal(
            barrier,
            inc=1,
            device_id={"sp": chip * CORES + core, "tp": (tp + step) % tps},
            device_id_type=MESH,
        )
    pl.semaphore_signal(
        barrier, inc=1, device_id={"sp": chip * CORES + 1 - core, "tp": tp}, device_id_type=MESH
    )
    pl.semaphore_wait(barrier, chips - 1 + tps - 1 + 1)


def gather_kernel(chips, tps, own_ref, all_ref, send_sem, recv_sem, own_sem):
    chip, core, tp = place()
    greet(chips, tps)
    started = []

    def block(chip_of, core_of, tp_of, piece):
        return ((chip_of * CORES + core_of) * tps + tp_of) * PIECES + piece

    def send(source, index, sp_to, tp_to):
        copy = pltpu.make_async_remote_copy(
            src_ref=source,
            dst_ref=all_ref.at[index],
            send_sem=send_sem.at[len(started)],
            recv_sem=recv_sem.at[index],
            device_id={"sp": sp_to, "tp": tp_to},
            device_id_type=MESH,
        )
        copy.start()
        started.append(copy)

    def arrived(index):
        pltpu.make_async_copy(all_ref.at[index], all_ref.at[index], recv_sem.at[index]).wait()

    for piece in range(PIECES):
        own = block(chip, core, tp, piece)
        for step in range(1, tps):
            send(own_ref.at[piece], own, chip * CORES + core, (tp + step) % tps)
        for step in range(1, chips):
            send(own_ref.at[piece], own, (chip + step) % chips * CORES + core, tp)
        send(own_ref.at[piece], own, chip * CORES + 1 - core, tp)
    mine = pltpu.make_async_copy(
        own_ref, all_ref.at[pl.ds(block(chip, core, tp, 0), PIECES)], own_sem
    )
    mine.start()

    def from_tp(chip_of, piece):
        for step in range(1, tps):
            index = block(chip_of, core, (tp + step) % tps, piece)
            arrived(index)
            send(all_ref.at[index], index, chip * CORES + 1 - core, tp)

    order = [(step, piece) for step in range(chips) for piece in range(PIECES)]
    for place_in, (step, piece) in enumerate(order):
        if step > 0:
            index = block((chip - step + chips) % chips, core, tp, piece)
            arrived(index)
            for tp_step in range(1, tps):
                send(all_ref.at[index], index, chip * CORES + core, (tp + tp_step) % tps)
            send(all_ref.at[index], index, chip * CORES + 1 - core, tp)
            done, done_piece = order[place_in - PIECES]
            from_tp((chip - done + chips) % chips, done_piece)
    for piece in range(PIECES):
        from_tp((chip + 1) % chips, piece)
    for step, piece in order:
        for tp_of in range(tps):
            arrived(block((chip - step + chips) % chips, 1 - core, (tp + tp_of) % tps, piece))
    mine.wait()
    for copy in started:
        copy.wait_send()


def gather_rows(own, chips, tps):
    blocks = chips * CORES * tps * PIECES
    sends = (chips - 1 + tps - 1 + 1 + (chips - 1) * tps + chips * (tps - 1)) * PIECES
    rows, width = own.shape
    own = own.reshape(PIECES, rows // PIECES, width)
    return pl.pallas_call(
        lambda *refs: gather_kernel(chips, tps, *refs),
        name="gather_rows",
        out_shape=jax.ShapeDtypeStruct((blocks,) + own.shape[1:], own.dtype),
        in_specs=[pl.BlockSpec(memory_space=pl.ANY)],
        out_specs=pl.BlockSpec(memory_space=pl.ANY),
        scratch_shapes=[
            pltpu.SemaphoreType.DMA((sends,)),
            pltpu.SemaphoreType.DMA((blocks,)),
            pltpu.SemaphoreType.DMA,
        ],
        compiler_params=pltpu.CompilerParams(collective_id=1, has_side_effects=True),
    )(own).reshape(-1, rows, width)


def add_rows(target, index, source, source_index):
    rows = target.shape[1]
    chunk = min(rows, 16)

    @pl.loop(0, rows // chunk)
    def _(part):
        span = pl.ds(pl.multiple_of(part * chunk, chunk), chunk)
        target[index, span, :] = (
            target[index, span, :].astype(jnp.float32)
            + source[source_index, span, :].astype(jnp.float32)
        ).astype(target.dtype)


def scatter_kernel(
    chips, tps, part_ref, out_ref, acc, core_in, tp_in, chip_in, load_sem, send_sem, core_sem, tp_sem, chip_sem
):
    chip, core, tp = place()
    load = []
    started = []
    order = [(step, piece) for step in range(chips) for piece in range(PIECES)]
    for step, piece in order:
        for tp_step in range(tps):
            chip_of, tp_of = (chip + 1 + step) % chips, (tp + 1 + tp_step) % tps
            copy = pltpu.make_async_copy(
                part_ref.at[((chip_of * CORES + core) * tps + tp_of) * PIECES + piece],
                acc.at[(chip_of * tps + tp_of) * PIECES + piece],
                load_sem.at[len(load)],
            )
            copy.start()
            load.append(copy)
    greet(chips, tps)

    def send(source, target, recv_sem, sp_to, tp_to):
        copy = pltpu.make_async_remote_copy(
            src_ref=source,
            dst_ref=target,
            send_sem=send_sem.at[len(started)],
            recv_sem=recv_sem,
            device_id={"sp": sp_to, "tp": tp_to},
            device_id_type=MESH,
        )
        copy.start()
        started.append(copy)

    def arrived(target, index, sem):
        pltpu.make_async_copy(target.at[index], target.at[index], sem).wait()

    for step, piece in order:
        chip_of = (chip + 1 + step) % chips
        for tp_step in range(tps):
            tp_of = (tp + 1 + tp_step) % tps
            index = (chip_of * tps + tp_of) * PIECES + piece
            send(
                part_ref.at[((chip_of * CORES + 1 - core) * tps + tp_of) * PIECES + piece],
                core_in.at[index],
                core_sem.at[index],
                chip * CORES + 1 - core,
                tp,
            )

    def chip_stage(step, piece):
        chip_of = (chip + 1 + step) % chips
        kept = (chip_of * tps + tp) * PIECES + piece
        for tp_step in range(1, tps):
            index = (chip_of * tps + (tp + tp_step) % tps) * PIECES + piece
            arrived(tp_in, index, tp_sem.at[index])
            add_rows(acc, kept, tp_in, index)
        if step < chips - 1:
            slot = chip * PIECES + piece
            send(acc.at[kept], chip_in.at[slot], chip_sem.at[slot], chip_of * CORES + core, tp)

    for number, (step, piece) in enumerate(order):
        chip_of = (chip + 1 + step) % chips
        for tp_step in range(tps):
            tp_of = (tp + 1 + tp_step) % tps
            index = (chip_of * tps + tp_of) * PIECES + piece
            load[number * tps + tp_step].wait()
            arrived(core_in, index, core_sem.at[index])
            add_rows(acc, index, core_in, index)
            if tp_step < tps - 1:
                slot = (chip_of * tps + tp) * PIECES + piece
                send(
                    acc.at[index], tp_in.at[slot], tp_sem.at[slot], chip * CORES + core, tp_of
                )
        if number > 0:
            chip_stage(*order[number - 1])
    chip_stage(*order[-1])
    rows = out_ref.shape[1]
    chunk = min(rows, 16)
    for step in range(1, chips):
        for piece in range(PIECES):
            source = (chip - step + chips) % chips * PIECES + piece
            kept = (chip * tps + tp) * PIECES + piece
            arrived(chip_in, source, chip_sem.at[source])
            if step < chips - 1:
                add_rows(acc, kept, chip_in, source)
            else:

                @pl.loop(0, rows // chunk)
                def _(part):
                    span = pl.ds(pl.multiple_of(part * chunk, chunk), chunk)
                    out_ref[piece, span, :] = acc[kept, span, :].astype(jnp.float32) + chip_in[
                        source, span, :
                    ].astype(jnp.float32)

    for copy in started:
        copy.wait_send()


def scatter_rows(parts, chips, tps):
    blocks, rows, width = parts.shape
    half = chips * tps * PIECES
    sends = half + (chips * (tps - 1) + chips - 1) * PIECES
    rows = rows // PIECES
    return pl.pallas_call(
        lambda *refs: scatter_kernel(chips, tps, *refs),
        name="scatter_rows",
        out_shape=jax.ShapeDtypeStruct((PIECES, rows, width), jnp.float32),
        in_specs=[pl.BlockSpec(memory_space=pl.ANY)],
        out_specs=pl.BlockSpec(memory_space=pltpu.VMEM),
        scratch_shapes=[
            pltpu.VMEM((half, rows, width), parts.dtype),
            pltpu.VMEM((half, rows, width), parts.dtype),
            pltpu.VMEM((half, rows, width), parts.dtype),
            pltpu.VMEM((chips * PIECES, rows, width), parts.dtype),
            pltpu.SemaphoreType.DMA((half,)),
            pltpu.SemaphoreType.DMA((sends,)),
            pltpu.SemaphoreType.DMA((half,)),
            pltpu.SemaphoreType.DMA((half,)),
            pltpu.SemaphoreType.DMA((chips * PIECES,)),
        ],
        compiler_params=pltpu.CompilerParams(
            collective_id=2, has_side_effects=True, vmem_limit_bytes=VMEM_BYTES
        ),
    )(parts.reshape(-1, rows, width)).reshape(PIECES * rows, width)


def attend_kernel(
    chips, heads_a, heads_b, query_ref, own_ref, lambda_ref, gain_a_ref, gain_b_ref, out_ref,
    held, top, total, accum_a, accum_b, own_sem, up_sem, side_sem, recv_sem,
):
    chip, core, tp = place()
    me = chip * CORES + core
    rows = own_ref.shape[0]
    mine = pltpu.make_async_copy(own_ref, held.at[me], own_sem)
    mine.start()
    barrier = pltpu.get_barrier_semaphore()

    def hello(sp_to):
        pl.semaphore_signal(barrier, inc=1, device_id={"sp": sp_to, "tp": tp}, device_id_type=MESH)

    hello(chip * CORES + 1 - core)

    @pl.when(chip > 0)
    def _():
        hello(me - CORES)

    @pl.when(chip < chips - 1)
    def _():
        hello(me + CORES)

    pl.semaphore_wait(
        barrier, 1 + jnp.where(chip > 0, 1, 0) + jnp.where(chip < chips - 1, 1, 0)
    )

    top[...] = jnp.full_like(top, -1e30)
    total[...] = jnp.zeros_like(total)
    accum_a[...] = jnp.zeros_like(accum_a)
    accum_b[...] = jnp.zeros_like(accum_b)
    mine.wait()

    def copy_up(back, index):
        return pltpu.make_async_remote_copy(
            src_ref=held.at[index], dst_ref=held.at[index], send_sem=up_sem.at[back],
            recv_sem=recv_sem.at[index], device_id={"sp": me + CORES, "tp": tp}, device_id_type=MESH,
        )

    def copy_side(back, index):
        return pltpu.make_async_remote_copy(
            src_ref=held.at[index], dst_ref=held.at[index], send_sem=side_sem.at[back],
            recv_sem=recv_sem.at[index], device_id={"sp": chip * CORES + 1 - core, "tp": tp},
            device_id_type=MESH,
        )

    base_va = 2 * heads_a * DA
    base_kb = base_va + heads_a * 2 * DA
    base_vb = base_kb + 2 * heads_b * DB
    base_qb = 2 * heads_a * DA
    ahead = lax.broadcasted_iota(jnp.int32, (rows, rows), 0) - lax.broadcasted_iota(
        jnp.int32, (rows, rows), 1
    )

    def flash(index):
        shown = ahead + (me - index) * rows >= 0

        def one(slot, query, key, value, accum, part, size):
            scores = lax.dot_general(
                query, key, (((1,), (1,)), ((), ())), preferred_element_type=jnp.float32
            )
            scores = jnp.where(shown, scores, -1e30)
            before = top[slot]
            after = jnp.maximum(before, jnp.max(scores, -1, keepdims=True))
            factor = size ** (-0.5) * LOG2E
            terms = jnp.exp2((scores - after) * factor)
            rescale = jnp.exp2((before - after) * factor)
            top[slot] = after
            total[slot] = total[slot] * rescale + jnp.sum(terms, -1, keepdims=True)
            accum[part] = accum[part] * rescale + jnp.dot(
                terms.astype(jnp.bfloat16), value, preferred_element_type=jnp.float32
            )

        for head in range(heads_a):
            value = held[index, :, base_va + head * 2 * DA : base_va + (head + 1) * 2 * DA]
            for pair in range(2):
                at = (pair * heads_a + head) * DA
                part = pair * heads_a + head
                one(
                    part, query_ref[:, at : at + DA], held[index, :, at : at + DA], value,
                    accum_a, part, DA,
                )
        for head in range(heads_b):
            value = held[index, :, base_vb + head * 2 * DB : base_vb + (head + 1) * 2 * DB]
            for pair in range(2):
                part = pair * heads_b + head
                at = base_qb + part * 2 * DB
                key_at = base_kb + part // 2 * 2 * DB
                one(
                    2 * heads_a + part, query_ref[:, at : at + 2 * DB],
                    held[index, :, key_at : key_at + 2 * DB], value, accum_b, part, DB,
                )

    def step(number, carry):
        back = number // 2
        side = number % 2
        source = chip - back

        @pl.when(source >= 0)
        def _():
            index = source * CORES + jnp.where(side == 0, core, 1 - core)

            @pl.when(number > 0)
            def _():
                pltpu.make_async_copy(held.at[index], held.at[index], recv_sem.at[index]).wait()

            @pl.when(side == 0)
            def _():
                @pl.when(chip < chips - 1)
                def _():
                    copy_up(back, index).start()

                copy_side(back, index).start()

            @pl.when(index <= me)
            def _():
                flash(index)

        return carry

    lax.fori_loop(0, 2 * chips, step, 0)

    def finish(head, parts, accum, slots, lam, gain_ref, at, wide):
        mixture = accum[parts[0]] / total[slots[0]] - lam * accum[parts[1]] / total[slots[1]]
        out_ref[:, at : at + wide] = rms_norm(mixture, gain_ref[...]).astype(out_ref.dtype)

    for head in range(heads_a):
        parts = (head, heads_a + head)
        finish(head, parts, accum_a, parts, lambda_ref[0:1, head : head + 1], gain_a_ref,
               head * 2 * DA, 2 * DA)
    for head in range(heads_b):
        parts = (head, heads_b + head)
        slots = (2 * heads_a + head, 2 * heads_a + heads_b + head)
        finish(head, parts, accum_b, slots, lambda_ref[0:1, heads_a + head : heads_a + head + 1],
               gain_b_ref, heads_a * 2 * DA + head * 2 * DB, 2 * DB)

    def settle(back, carry):
        @pl.when(chip - back >= 0)
        def _():
            index = (chip - back) * CORES + core

            @pl.when(chip < chips - 1)
            def _():
                copy_up(back, index).wait_send()

            copy_side(back, index).wait_send()

        return carry

    lax.fori_loop(0, chips, settle, 0)


def attend_blocks(queries, own, lambdas, gain_a, gain_b, chips, heads_a, heads_b):
    rows, width = own.shape
    vmem = pl.BlockSpec(memory_space=pltpu.VMEM)
    return pl.pallas_call(
        lambda *refs: attend_kernel(chips, heads_a, heads_b, *refs),
        name="attend_blocks",
        out_shape=jax.ShapeDtypeStruct((rows, heads_a * 2 * DA + heads_b * 2 * DB), jnp.bfloat16),
        in_specs=[vmem, pl.BlockSpec(memory_space=pl.ANY), vmem, vmem, vmem],
        out_specs=vmem,
        scratch_shapes=[
            pltpu.VMEM((chips * CORES, rows, width), own.dtype),
            pltpu.VMEM((2 * (heads_a + heads_b), rows, 1), jnp.float32),
            pltpu.VMEM((2 * (heads_a + heads_b), rows, 1), jnp.float32),
            pltpu.VMEM((2 * heads_a, rows, 2 * DA), jnp.float32),
            pltpu.VMEM((2 * heads_b, rows, 2 * DB), jnp.float32),
            pltpu.SemaphoreType.DMA,
            pltpu.SemaphoreType.DMA((chips,)),
            pltpu.SemaphoreType.DMA((chips,)),
            pltpu.SemaphoreType.DMA((chips * CORES,)),
        ],
        compiler_params=pltpu.CompilerParams(
            collective_id=3, has_side_effects=True, vmem_limit_bytes=VMEM_BYTES
        ),
    )(queries, own, lambdas, gain_a, gain_b)


def share_kernel(tps, part_ref, out_ref, arrived, send_sem, recv_sem):
    tp = lax.axis_index("tp")
    barrier = pltpu.get_barrier_semaphore()
    for step in range(1, tps):
        pl.semaphore_signal(barrier, inc=1, device_id={"tp": (tp + step) % tps}, device_id_type=MESH)
    pl.semaphore_wait(barrier, tps - 1)
    started = []
    for step in range(1, tps):
        other = (tp + step) % tps
        copy = pltpu.make_async_remote_copy(
            src_ref=part_ref.at[other], dst_ref=arrived.at[step - 1], send_sem=send_sem.at[step - 1],
            recv_sem=recv_sem.at[step - 1], device_id={"tp": other}, device_id_type=MESH,
        )
        copy.start()
        started.append(copy)
    rows = out_ref.shape[0]
    chunk = min(rows, 16)
    for step in range(1, tps):
        started[step - 1].wait()

        @pl.loop(0, rows // chunk)
        def _(part):
            span = pl.ds(pl.multiple_of(part * chunk, chunk), chunk)
            first = part_ref[tp, span, :].astype(jnp.float32) if step == 1 else out_ref[span, :]
            out_ref[span, :] = first + arrived[step - 1, span, :].astype(jnp.float32)


def share_rows(parts, tps):
    _, rows, width = parts.shape
    vmem = pl.BlockSpec(memory_space=pltpu.VMEM)
    return pl.pallas_call(
        lambda *refs: share_kernel(tps, *refs),
        name="share_rows",
        out_shape=jax.ShapeDtypeStruct((rows, width), jnp.float32),
        in_specs=[vmem],
        out_specs=vmem,
        scratch_shapes=[
            pltpu.VMEM((tps - 1, rows, width), parts.dtype),
            pltpu.SemaphoreType.DMA((tps - 1,)),
            pltpu.SemaphoreType.DMA((tps - 1,)),
        ],
        compiler_params=pltpu.CompilerParams(collective_id=4, has_side_effects=True),
    )(parts)


def spread_pairs(queries, heads):
    rows = queries.shape[0]
    pairs = queries.reshape(rows, 2 * heads // 2, 1, 2, DB)
    keep = jnp.eye(2, dtype=queries.dtype).reshape(1, 1, 2, 2, 1)
    return (pairs * keep).reshape(rows, 2 * heads * 2 * DB)


def expert_parts(gathered, expert, experts, capacity, width, weights):
    gate, up, down = weights
    blocks, rows, _ = gathered.shape
    shares = lax.dynamic_slice_in_dim(gathered[:, :, width:], expert, 1, 2)[:, :, 0]
    named = shares > 0
    order = jnp.arange(rows, dtype=jnp.int32)
    slots = jnp.dot(
        named.astype(jnp.bfloat16),
        (order[:, None] < order[None, :]).astype(jnp.bfloat16),
        preferred_element_type=jnp.float32,
    ).astype(jnp.int32)
    picks = (slots[:, None, :] == jnp.arange(capacity, dtype=jnp.int32)[None, :, None]) & named[:, None, :]
    rows_in = jnp.einsum(
        "bct,btd->bcd",
        picks.astype(jnp.bfloat16),
        gathered[:, :, :width],
        preferred_element_type=jnp.float32,
    ).astype(jnp.bfloat16)
    rows_in = rows_in.reshape(blocks * capacity, width)
    gate_pre = jnp.dot(rows_in, gate, preferred_element_type=jnp.float32)
    up_pre = jnp.dot(rows_in, up, preferred_element_type=jnp.float32)
    glu_part = jnp.minimum(gate_pre, 7.0)
    lin_part = jnp.clip(up_pre, -7.0, 7.0)
    hidden = (glu_part * jax.nn.sigmoid(1.702 * glu_part) * (lin_part + 1.0)).astype(jnp.bfloat16)
    outs = jnp.dot(hidden, down, preferred_element_type=jnp.float32).astype(jnp.bfloat16)
    back = jnp.where(picks, shares[:, None, :], 0).astype(jnp.bfloat16)
    return jnp.einsum(
        "bct,bcd->btd",
        back,
        outs.reshape(blocks, capacity, width),
        preferred_element_type=jnp.float32,
    ).astype(jnp.bfloat16)


def meet(chips, tps):
    chip, core, tp = place()
    barrier = pltpu.get_barrier_semaphore()
    others = 0
    for chip_step in range(chips):
        for core_step in range(CORES):
            for tp_step in range(tps):
                if chip_step + core_step + tp_step > 0:
                    others += 1
                    pl.semaphore_signal(
                        barrier,
                        inc=1,
                        device_id={
                            "sp": (chip + chip_step) % chips * CORES + (core + core_step) % CORES,
                            "tp": (tp + tp_step) % tps,
                        },
                        device_id_type=MESH,
                    )
    pl.semaphore_wait(barrier, others)


def group_at(chip, chips, step):
    near = jnp.minimum(chip, chips - 1 - chip)
    both = jnp.where(step % 2 == 1, chip - (step + 1) // 2, chip + step // 2)
    past = jnp.where(chip <= chips - 1 - chip, chip + step - near, chip - step + near)
    return jnp.where(step <= 2 * near, both, past)


def experts_kernel(
    chips, tps, capacity,
    own_ref, meta_ref, gate_ref, up_ref, down_ref, out_ref,
    rows_all, meta_all, gate, up, down, rows_in, hidden, back, part, core_in, x_in, z_in,
    load_sem, weight_sem, row_sem, meta_send, meta_recv, up_sem, dn_sem, x_sem, side_sem,
    core_send, core_recv, xs_send, xs_recv, zs_send, zs_recv,
):
    chip, core, tp = place()
    experts = meta_ref.shape[0] // 2
    piece_rows, width = rows_all.shape[2], rows_all.shape[3]
    rows = piece_rows * PIECES
    ff = gate.shape[1]
    members = CORES * tps
    side_sp = chip * CORES + 1 - core

    def blk(chip_of, core_of, tp_of):
        return (chip_of * CORES + core_of) * tps + tp_of

    def remote(src, dst, send, recv, sp_to, tp_to):
        return pltpu.make_async_remote_copy(
            src_ref=src, dst_ref=dst, send_sem=send, recv_sem=recv,
            device_id={"sp": sp_to, "tp": tp_to}, device_id_type=MESH,
        )

    def rows_copy(block, piece, send, sp_to, tp_to):
        ref = rows_all.at[block, piece]
        return remote(ref, ref, send, row_sem.at[block, piece], sp_to, tp_to)

    def go_up(chip_of, piece):
        return rows_copy(blk(chip_of, core, tp), piece, up_sem.at[chip_of, piece],
                         (chip + 1) * CORES + core, tp)

    def go_dn(chip_of, piece):
        return rows_copy(blk(chip_of, core, tp), piece, dn_sem.at[chip_of, piece],
                         (chip - 1) * CORES + core, tp)

    def go_x(chip_of, step, piece):
        return rows_copy(blk(chip_of, core, tp), piece, x_sem.at[chip_of, step - 1, piece],
                         chip * CORES + core, (tp + step) % tps)

    def go_side(chip_of, tp_of, piece):
        return rows_copy(blk(chip_of, core, tp_of), piece, side_sem.at[chip_of, tp_of, piece],
                         side_sp, tp)

    def wait_rows(block, piece):
        ref = rows_all.at[block, piece]
        pltpu.make_async_copy(ref, ref, row_sem.at[block, piece]).wait()

    mine = blk(chip, core, tp)
    loads = [
        pltpu.make_async_copy(own_ref.at[piece], rows_all.at[mine, piece], load_sem.at[piece])
        for piece in range(PIECES)
    ]
    weights = [
        pltpu.make_async_copy(src, dst, weight_sem.at[number])
        for number, (src, dst) in enumerate(((gate_ref, gate), (up_ref, up), (down_ref, down)))
    ]
    for copy in loads + weights:
        copy.start()
    meta_all[mine] = meta_ref[...]
    meet(chips, tps)

    for piece in range(PIECES):
        loads[piece].wait()
        for step in range(1, tps):
            go_x(chip, step, piece).start()

        @pl.when(chip < chips - 1)
        def _():
            go_up(chip, piece).start()

        @pl.when(chip > 0)
        def _():
            go_dn(chip, piece).start()

        go_side(chip, tp, piece).start()

    def meta_copy(number, chip_step, core_step, tp_step):
        return remote(
            meta_ref, meta_all.at[mine], meta_send.at[number], meta_recv.at[mine],
            (chip + chip_step) % chips * CORES + (core + core_step) % CORES, (tp + tp_step) % tps,
        )

    meta_steps = [
        (chip_step, core_step, tp_step)
        for chip_step in range(chips) for core_step in range(CORES) for tp_step in range(tps)
        if chip_step + core_step + tp_step > 0
    ]
    for number, steps in enumerate(meta_steps):
        meta_copy(number, *steps).start()

    def relay(chip_of, piece, upward):
        wait_rows(blk(chip_of, core, tp), piece)
        for step in range(1, tps):
            go_x(chip_of, step, piece).start()
        if upward:
            @pl.when(chip < chips - 1)
            def _():
                go_up(chip_of, piece).start()
        else:
            @pl.when(chip > 0)
            def _():
                go_dn(chip_of, piece).start()
        go_side(chip_of, tp, piece).start()

    def compute(group):
        order = lax.broadcasted_iota(jnp.int32, (capacity, rows), 0).astype(jnp.float32)
        expert = chip * CORES + core
        for member in range(members):
            block = group * members + member
            slot = meta_all[block, pl.ds(expert, 1), :]
            share = meta_all[block, pl.ds(experts + expert, 1), :]
            hit = slot == order
            picks = jnp.where(hit, 1.0, 0.0).astype(jnp.bfloat16)
            back[member] = jnp.where(hit, share, 0.0).astype(jnp.bfloat16)
            values = rows_all[block].reshape(rows, width)
            rows_in[member * capacity : (member + 1) * capacity, :] = jnp.dot(
                picks, values, preferred_element_type=jnp.float32
            ).astype(jnp.bfloat16)
        cut = min(ff, 256)

        @pl.loop(0, ff // cut)
        def _(number):
            cols = pl.ds(pl.multiple_of(number * cut, cut), cut)
            gate_pre = jnp.dot(rows_in[...], gate[:, cols], preferred_element_type=jnp.float32)
            up_pre = jnp.dot(rows_in[...], up[:, cols], preferred_element_type=jnp.float32)
            glu_part = jnp.minimum(gate_pre, 7.0)
            lin_part = jnp.clip(up_pre, -7.0, 7.0)
            hidden[:, cols] = (
                glu_part * jax.nn.sigmoid(1.702 * glu_part) * (lin_part + 1.0)
            ).astype(jnp.bfloat16)

        wide = min(width, 256)

        @pl.loop(0, width // wide)
        def _(number):
            cols = pl.ds(pl.multiple_of(number * wide, wide), wide)
            outs = jnp.dot(
                hidden[...], down[:, cols], preferred_element_type=jnp.float32
            ).astype(jnp.bfloat16)
            for member in range(members):
                spread = lax.dot_general(
                    back[member], outs[member * capacity : (member + 1) * capacity],
                    (((0,), (0,)), ((), ())), preferred_element_type=jnp.float32,
                ).astype(jnp.bfloat16)
                part[group * members + member, :, :, cols] = spread.reshape(
                    PIECES, piece_rows, wide
                )

    def add(target, index, source, source_index):
        chunk = min(piece_rows, 16)

        @pl.loop(0, piece_rows // chunk)
        def _(number):
            span = pl.ds(pl.multiple_of(number * chunk, chunk), chunk)
            target[index + (span,)] = (
                target[index + (span,)].astype(jnp.float32)
                + source[source_index + (span,)].astype(jnp.float32)
            ).astype(target.dtype)

    def core_copy(group, tp_of):
        return remote(part.at[blk(group, 1 - core, tp_of)], core_in.at[group, tp_of],
                      core_send.at[group, tp_of], core_recv.at[group, tp_of], side_sp, tp)

    def part_x(group, step, piece):
        return remote(part.at[blk(group, core, (tp + step) % tps), piece],
                      x_in.at[group, step - 1, piece], xs_send.at[group, step - 1, piece],
                      xs_recv.at[group, step - 1, piece], chip * CORES + core, (tp + step) % tps)

    def part_z(way, group, piece):
        return remote(part.at[blk(group, core, tp), piece], z_in.at[way, group, piece],
                      zs_send.at[way, group, piece], zs_recv.at[way, group, piece],
                      (chip + 1 - 2 * way) * CORES + core, tp)

    def arrived(ref, sem):
        pltpu.make_async_copy(ref, ref, sem).wait()

    def cross(group):
        for tp_of in range(tps):
            core_copy(group, tp_of).start()
        for step in list(range(1, tps)) + [0]:
            tp_of = (tp + step) % tps
            arrived(core_in.at[group, tp_of], core_recv.at[group, tp_of])
            for piece in range(PIECES):
                add(part, (blk(group, core, tp_of), piece), core_in, (group, tp_of, piece))
                if step > 0:
                    part_x(group, step, piece).start()

    def settle(group):
        for piece in range(PIECES):
            for step in range(1, tps):
                arrived(x_in.at[group, step - 1, piece], xs_recv.at[group, step - 1, piece])
                add(part, (blk(group, core, tp), piece), x_in, (group, step - 1, piece))

            @pl.when((chip == 0) & (group > 0))
            def _():
                part_z(0, group, piece).start()

            @pl.when((chip == chips - 1) & (group < chips - 1))
            def _():
                part_z(1, group, piece).start()

    def wave(step, carry):
        @pl.when(step < chips)
        def _():
            for piece in range(PIECES):
                @pl.when(chip - step >= 0)
                def _():
                    relay(chip - step, piece, True)

                @pl.when(chip + step < chips)
                def _():
                    relay(chip + step, piece, False)

        group = group_at(chip, chips, step - 1)
        for piece in range(PIECES):
            for tp_step in range(1, tps):
                tp_of = (tp + tp_step) % tps
                wait_rows(blk(group, core, tp_of), piece)
                go_side(group, tp_of, piece).start()

        @pl.when(step == 1)
        def _():
            for steps in meta_steps:
                block = blk((chip + steps[0]) % chips, (core + steps[1]) % CORES, (tp + steps[2]) % tps)
                arrived(meta_all.at[block], meta_recv.at[block])
            for copy in weights:
                copy.wait()

        for piece in range(PIECES):
            for tp_of in range(tps):
                wait_rows(blk(group, 1 - core, tp_of), piece)
        compute(group)
        cross(group)

        @pl.when(step > 1)
        def _():
            settle(group_at(chip, chips, step - 2))

        return carry

    lax.fori_loop(1, chips + 1, wave, 0)
    settle(group_at(chip, chips, chips - 1))

    def chain(number, carry):
        for way in range(2):
            group = number if way == 0 else chips - 1 - number
            if way == 0:
                passes = (chip > 0) & (chip < group)
            else:
                passes = (chip < chips - 1) & (chip > group)

            @pl.when(passes)
            def _():
                for piece in range(PIECES):
                    arrived(z_in.at[way, group, piece], zs_recv.at[way, group, piece])
                    add(part, (blk(group, core, tp), piece), z_in, (way, group, piece))
                    part_z(way, group, piece).start()

        return carry

    lax.fori_loop(1, chips, chain, 0)

    chunk = min(piece_rows, 16)
    for piece in range(PIECES):
        @pl.loop(0, piece_rows // chunk)
        def _(number):
            span = pl.ds(pl.multiple_of(number * chunk, chunk), chunk)
            out_ref[piece, span, :] = part[mine, piece, span, :].astype(jnp.float32)

        for way in range(2):
            @pl.when(chip > 0 if way == 0 else chip < chips - 1)
            def _():
                arrived(z_in.at[way, chip, piece], zs_recv.at[way, chip, piece])

                @pl.loop(0, piece_rows // chunk)
                def _(number):
                    span = pl.ds(pl.multiple_of(number * chunk, chunk), chunk)
                    out_ref[piece, span, :] = out_ref[piece, span, :] + z_in[
                        way, chip, piece, span, :
                    ].astype(jnp.float32)

    for number, steps in enumerate(meta_steps):
        meta_copy(number, *steps).wait_send()

    def finish(group, carry):
        for piece in range(PIECES):
            for step in range(1, tps):
                go_x(group, step, piece).wait_send()
                part_x(group, step, piece).wait_send()
            for tp_of in range(tps):
                go_side(group, tp_of, piece).wait_send()

            @pl.when((group <= chip) & (chip < chips - 1))
            def _():
                go_up(group, piece).wait_send()

            @pl.when((group >= chip) & (chip > 0))
            def _():
                go_dn(group, piece).wait_send()

            @pl.when(group > chip)
            def _():
                part_z(0, group, piece).wait_send()

            @pl.when(group < chip)
            def _():
                part_z(1, group, piece).wait_send()

        for tp_of in range(tps):
            core_copy(group, tp_of).wait_send()
        return carry

    lax.fori_loop(0, chips, finish, 0)


def experts_bytes(rows, width, ff, chips, tps, capacity):
    blocks = chips * CORES * tps
    members = CORES * tps
    buffers = blocks * 2 + chips * (2 * tps - 1 + 2) + 2
    return 2 * (
        rows * width * buffers + 3 * width * ff + members * capacity * (width + ff) + 2 * rows * width
    )


def run_experts(normed, meta, gate, up, down, chips, tps, capacity):
    rows, width = normed.shape
    ff = gate.shape[1]
    blocks = chips * CORES * tps
    members = CORES * tps
    piece_rows = rows // PIECES
    vmem = pl.BlockSpec(memory_space=pltpu.VMEM)
    any_space = pl.BlockSpec(memory_space=pl.ANY)
    dma = pltpu.SemaphoreType.DMA
    bf16 = jnp.bfloat16
    return pl.pallas_call(
        lambda *refs: experts_kernel(chips, tps, capacity, *refs),
        name="run_experts",
        out_shape=jax.ShapeDtypeStruct((PIECES, piece_rows, width), jnp.float32),
        in_specs=[any_space, vmem, any_space, any_space, any_space],
        out_specs=vmem,
        scratch_shapes=[
            pltpu.VMEM((blocks, PIECES, piece_rows, width), bf16),
            pltpu.VMEM((blocks,) + meta.shape, meta.dtype),
            pltpu.VMEM(gate.shape, bf16),
            pltpu.VMEM(up.shape, bf16),
            pltpu.VMEM(down.shape, bf16),
            pltpu.VMEM((members * capacity, width), bf16),
            pltpu.VMEM((members * capacity, ff), bf16),
            pltpu.VMEM((members, capacity, rows), bf16),
            pltpu.VMEM((blocks, PIECES, piece_rows, width), bf16),
            pltpu.VMEM((chips, tps, PIECES, piece_rows, width), bf16),
            pltpu.VMEM((chips, tps - 1, PIECES, piece_rows, width), bf16),
            pltpu.VMEM((2, chips, PIECES, piece_rows, width), bf16),
            dma((PIECES,)),
            dma((3,)),
            dma((blocks, PIECES)),
            dma((blocks - 1,)),
            dma((blocks,)),
            dma((chips, PIECES)),
            dma((chips, PIECES)),
            dma((chips, tps - 1, PIECES)),
            dma((chips, tps, PIECES)),
            dma((chips, tps)),
            dma((chips, tps)),
            dma((chips, tps - 1, PIECES)),
            dma((chips, tps - 1, PIECES)),
            dma((2, chips, PIECES)),
            dma((2, chips, PIECES)),
        ],
        compiler_params=pltpu.CompilerParams(
            collective_id=5, has_side_effects=True, vmem_limit_bytes=VMEM_BYTES
        ),
    )(normed.reshape(PIECES, piece_rows, width), meta, gate, up, down).reshape(rows, width)


def slot_table(routes, route_weights, experts):
    rows = routes.shape[0]
    chosen = routes[None, :, :] == jnp.arange(experts, dtype=jnp.int32)[:, None, None]
    shares = jnp.sum(jnp.where(chosen, route_weights[None], 0.0), 2)
    named = jnp.any(chosen, 2)
    order = jnp.arange(rows, dtype=jnp.int32)
    slots = jnp.dot(
        named.astype(jnp.bfloat16),
        (order[:, None] < order[None, :]).astype(jnp.bfloat16),
        preferred_element_type=jnp.float32,
    )
    return jnp.concatenate([jnp.where(named, slots, -1.0), shares], 0)


def spread_experts(normed, routes, route_weights, seq_slot, experts, capacity, chips, tps, weights):
    width = normed.shape[1]
    extra = -(-experts // 128) * 128
    shares = jnp.sum(
        jnp.where(
            routes[:, :, None] == jnp.arange(extra, dtype=jnp.int32)[None, None, :],
            route_weights[:, :, None],
            0.0,
        ),
        1,
    ).astype(jnp.bfloat16)
    gathered = gather_rows(jnp.concatenate([normed, shares], 1), chips, tps)
    parts = expert_parts(gathered, seq_slot, experts, capacity, width, weights)
    return scatter_rows(parts, chips, tps)


def per_device(
    queries_a,
    keys_a,
    values_a,
    queries_b,
    keys_b,
    values_b,
    lambdas,
    head_gain_a,
    head_gain_b,
    out_a,
    out_b,
    residual,
    gain_mix,
    gain_pre,
    gain_post,
    routes,
    route_weights,
    expert_gate,
    expert_up,
    expert_down,
):
    length = queries_a.shape[0]
    heads_a = queries_a.shape[2] // DA
    heads_b = queries_b.shape[2] // DB
    head_slot = lax.axis_index("tp")
    seq_slot = lax.axis_index("sp")
    lambda_a = lax.dynamic_slice_in_dim(lambdas, head_slot * heads_a, heads_a)
    lambda_b = lax.dynamic_slice_in_dim(lambdas, HA + head_slot * heads_b, heads_b)
    experts, tps = lax.axis_size("sp"), lax.axis_size("tp")
    chips = experts // CORES
    own = jnp.concatenate(
        [keys_a.reshape(length, -1), values_a, keys_b.reshape(length, -1), values_b], 1
    )
    queries = jnp.concatenate([queries_a.reshape(length, -1), spread_pairs(queries_b, heads_b)], 1)
    heads_out = attend_blocks(
        queries,
        own,
        jnp.concatenate([lambda_a, lambda_b])[None],
        head_gain_a[None],
        head_gain_b[None],
        chips,
        heads_a,
        heads_b,
    )
    cut = heads_a * 2 * DA
    mixed = (
        jnp.dot(heads_out[:, :cut], out_a, preferred_element_type=jnp.float32)
        + jnp.dot(heads_out[:, cut:], out_b, preferred_element_type=jnp.float32)
    ).astype(jnp.bfloat16)
    mixed_rows = share_rows(mixed.reshape(tps, length // tps, -1), tps)
    after_mix = (residual.astype(jnp.float32) + rms_norm(mixed_rows, gain_mix)).astype(jnp.bfloat16)
    normed = rms_norm(after_mix.astype(jnp.float32), gain_pre).astype(jnp.bfloat16)
    sub_rows = residual.shape[0]
    top_count = routes.shape[1]
    capacity = min(sub_rows, (5 * sub_rows * top_count + 4 * experts - 1) // (4 * experts))
    width = residual.shape[1]
    slots = -(-capacity // 16) * 16
    if experts_bytes(sub_rows, width, expert_gate.shape[2], chips, tps, slots) < VMEM_BYTES * 9 // 10:
        routed = run_experts(
            normed, slot_table(routes, route_weights, experts), expert_gate[0], expert_up[0],
            expert_down[0], chips, tps, slots,
        )
    else:
        routed = spread_experts(
            normed, routes, route_weights, seq_slot, experts, capacity, chips, tps,
            (expert_gate[0], expert_up[0], expert_down[0]),
        )
    return (after_mix.astype(jnp.float32) + rms_norm(routed, gain_post)).astype(jnp.bfloat16)


def solution(mesh):
    in_specs = (
        P(("grp", "sp"), None, "tp"),
        P(("grp", "sp"), None, "tp"),
        P(("grp", "sp"), "tp"),
        P(("grp", "sp"), None, "tp"),
        P(("grp", "sp"), None, "tp"),
        P(("grp", "sp"), "tp"),
        P(),
        P(),
        P(),
        P("tp", None),
        P("tp", None),
        P(("grp", "sp", "tp"), None),
        P(),
        P(),
        P(),
        P(("grp", "sp", "tp"), None),
        P(("grp", "sp", "tp"), None),
        P("sp", None, "tp"),
        P("sp", None, "tp"),
        P("sp", "tp", None),
    )
    out_specs = P(("grp", "sp", "tp"), None)
    return jax.shard_map(
        per_device, mesh=mesh, in_specs=in_specs, out_specs=out_specs, check_vma=False
    )
```

```python
import jax
import jax.numpy as jnp
from jax import lax
from jax.experimental import pallas as pl
from jax.experimental.pallas import tpu as pltpu
from jax.sharding import PartitionSpec as P

HA = 4
DA = 128
DB = 64


def rms_norm(values, gain_vec):
    return values * lax.rsqrt(jnp.mean(values * values, -1, keepdims=True) + 1e-06) * gain_vec


MESH = pl.DeviceIdType.MESH
CORES = 2
PIECES = 2
CUTS = 4
LOG2E = 1.4426950408889634
VMEM_BYTES = 60 * 1024 * 1024


def place():
    sp = lax.axis_index("sp")
    return sp // CORES, sp % CORES, lax.axis_index("tp")


def greet(chips, tps):
    chip, core, tp = place()
    barrier = pltpu.get_barrier_semaphore()
    for step in range(1, chips):
        other = (chip + step) % chips
        pl.semaphore_signal(
            barrier, inc=1, device_id={"sp": other * CORES + core, "tp": tp}, device_id_type=MESH
        )
    for step in range(1, tps):
        pl.semaphore_signal(
            barrier,
            inc=1,
            device_id={"sp": chip * CORES + core, "tp": (tp + step) % tps},
            device_id_type=MESH,
        )
    pl.semaphore_signal(
        barrier, inc=1, device_id={"sp": chip * CORES + 1 - core, "tp": tp}, device_id_type=MESH
    )
    pl.semaphore_wait(barrier, chips - 1 + tps - 1 + 1)


def gather_kernel(chips, tps, own_ref, all_ref, send_sem, recv_sem, own_sem):
    chip, core, tp = place()
    greet(chips, tps)
    started = []

    def block(chip_of, core_of, tp_of, piece):
        return ((chip_of * CORES + core_of) * tps + tp_of) * PIECES + piece

    def send(source, index, sp_to, tp_to):
        copy = pltpu.make_async_remote_copy(
            src_ref=source,
            dst_ref=all_ref.at[index],
            send_sem=send_sem.at[len(started)],
            recv_sem=recv_sem.at[index],
            device_id={"sp": sp_to, "tp": tp_to},
            device_id_type=MESH,
        )
        copy.start()
        started.append(copy)

    def arrived(index):
        pltpu.make_async_copy(all_ref.at[index], all_ref.at[index], recv_sem.at[index]).wait()

    for piece in range(PIECES):
        own = block(chip, core, tp, piece)
        for step in range(1, tps):
            send(own_ref.at[piece], own, chip * CORES + core, (tp + step) % tps)
        for step in range(1, chips):
            send(own_ref.at[piece], own, (chip + step) % chips * CORES + core, tp)
        send(own_ref.at[piece], own, chip * CORES + 1 - core, tp)
    mine = pltpu.make_async_copy(
        own_ref, all_ref.at[pl.ds(block(chip, core, tp, 0), PIECES)], own_sem
    )
    mine.start()

    def from_tp(chip_of, piece):
        for step in range(1, tps):
            index = block(chip_of, core, (tp + step) % tps, piece)
            arrived(index)
            send(all_ref.at[index], index, chip * CORES + 1 - core, tp)

    order = [(step, piece) for step in range(chips) for piece in range(PIECES)]
    for place_in, (step, piece) in enumerate(order):
        if step > 0:
            index = block((chip - step + chips) % chips, core, tp, piece)
            arrived(index)
            for tp_step in range(1, tps):
                send(all_ref.at[index], index, chip * CORES + core, (tp + tp_step) % tps)
            send(all_ref.at[index], index, chip * CORES + 1 - core, tp)
            done, done_piece = order[place_in - PIECES]
            from_tp((chip - done + chips) % chips, done_piece)
    for piece in range(PIECES):
        from_tp((chip + 1) % chips, piece)
    for step, piece in order:
        for tp_of in range(tps):
            arrived(block((chip - step + chips) % chips, 1 - core, (tp + tp_of) % tps, piece))
    mine.wait()
    for copy in started:
        copy.wait_send()


def gather_rows(own, chips, tps):
    blocks = chips * CORES * tps * PIECES
    sends = (chips - 1 + tps - 1 + 1 + (chips - 1) * tps + chips * (tps - 1)) * PIECES
    rows, width = own.shape
    own = own.reshape(PIECES, rows // PIECES, width)
    return pl.pallas_call(
        lambda *refs: gather_kernel(chips, tps, *refs),
        name="gather_rows",
        out_shape=jax.ShapeDtypeStruct((blocks,) + own.shape[1:], own.dtype),
        in_specs=[pl.BlockSpec(memory_space=pl.ANY)],
        out_specs=pl.BlockSpec(memory_space=pl.ANY),
        scratch_shapes=[
            pltpu.SemaphoreType.DMA((sends,)),
            pltpu.SemaphoreType.DMA((blocks,)),
            pltpu.SemaphoreType.DMA,
        ],
        compiler_params=pltpu.CompilerParams(collective_id=1, has_side_effects=True),
    )(own).reshape(-1, rows, width)


def add_rows(target, index, source, source_index):
    rows = target.shape[1]
    chunk = min(rows, 16)

    @pl.loop(0, rows // chunk)
    def _(part):
        span = pl.ds(pl.multiple_of(part * chunk, chunk), chunk)
        target[index, span, :] = (
            target[index, span, :].astype(jnp.float32)
            + source[source_index, span, :].astype(jnp.float32)
        ).astype(target.dtype)


def scatter_kernel(
    chips, tps, part_ref, out_ref, acc, core_in, tp_in, chip_in, load_sem, send_sem, core_sem, tp_sem, chip_sem
):
    chip, core, tp = place()
    load = []
    started = []
    order = [(step, piece) for step in range(chips) for piece in range(PIECES)]
    for step, piece in order:
        for tp_step in range(tps):
            chip_of, tp_of = (chip + 1 + step) % chips, (tp + 1 + tp_step) % tps
            copy = pltpu.make_async_copy(
                part_ref.at[((chip_of * CORES + core) * tps + tp_of) * PIECES + piece],
                acc.at[(chip_of * tps + tp_of) * PIECES + piece],
                load_sem.at[len(load)],
            )
            copy.start()
            load.append(copy)
    greet(chips, tps)

    def send(source, target, recv_sem, sp_to, tp_to):
        copy = pltpu.make_async_remote_copy(
            src_ref=source,
            dst_ref=target,
            send_sem=send_sem.at[len(started)],
            recv_sem=recv_sem,
            device_id={"sp": sp_to, "tp": tp_to},
            device_id_type=MESH,
        )
        copy.start()
        started.append(copy)

    def arrived(target, index, sem):
        pltpu.make_async_copy(target.at[index], target.at[index], sem).wait()

    for step, piece in order:
        chip_of = (chip + 1 + step) % chips
        for tp_step in range(tps):
            tp_of = (tp + 1 + tp_step) % tps
            index = (chip_of * tps + tp_of) * PIECES + piece
            send(
                part_ref.at[((chip_of * CORES + 1 - core) * tps + tp_of) * PIECES + piece],
                core_in.at[index],
                core_sem.at[index],
                chip * CORES + 1 - core,
                tp,
            )

    def chip_stage(step, piece):
        chip_of = (chip + 1 + step) % chips
        kept = (chip_of * tps + tp) * PIECES + piece
        for tp_step in range(1, tps):
            index = (chip_of * tps + (tp + tp_step) % tps) * PIECES + piece
            arrived(tp_in, index, tp_sem.at[index])
            add_rows(acc, kept, tp_in, index)
        if step < chips - 1:
            slot = chip * PIECES + piece
            send(acc.at[kept], chip_in.at[slot], chip_sem.at[slot], chip_of * CORES + core, tp)

    for number, (step, piece) in enumerate(order):
        chip_of = (chip + 1 + step) % chips
        for tp_step in range(tps):
            tp_of = (tp + 1 + tp_step) % tps
            index = (chip_of * tps + tp_of) * PIECES + piece
            load[number * tps + tp_step].wait()
            arrived(core_in, index, core_sem.at[index])
            add_rows(acc, index, core_in, index)
            if tp_step < tps - 1:
                slot = (chip_of * tps + tp) * PIECES + piece
                send(
                    acc.at[index], tp_in.at[slot], tp_sem.at[slot], chip * CORES + core, tp_of
                )
        if number > 0:
            chip_stage(*order[number - 1])
    chip_stage(*order[-1])
    rows = out_ref.shape[1]
    chunk = min(rows, 16)
    for step in range(1, chips):
        for piece in range(PIECES):
            source = (chip - step + chips) % chips * PIECES + piece
            kept = (chip * tps + tp) * PIECES + piece
            arrived(chip_in, source, chip_sem.at[source])
            if step < chips - 1:
                add_rows(acc, kept, chip_in, source)
            else:

                @pl.loop(0, rows // chunk)
                def _(part):
                    span = pl.ds(pl.multiple_of(part * chunk, chunk), chunk)
                    out_ref[piece, span, :] = acc[kept, span, :].astype(jnp.float32) + chip_in[
                        source, span, :
                    ].astype(jnp.float32)

    for copy in started:
        copy.wait_send()


def scatter_rows(parts, chips, tps):
    blocks, rows, width = parts.shape
    half = chips * tps * PIECES
    sends = half + (chips * (tps - 1) + chips - 1) * PIECES
    rows = rows // PIECES
    return pl.pallas_call(
        lambda *refs: scatter_kernel(chips, tps, *refs),
        name="scatter_rows",
        out_shape=jax.ShapeDtypeStruct((PIECES, rows, width), jnp.float32),
        in_specs=[pl.BlockSpec(memory_space=pl.ANY)],
        out_specs=pl.BlockSpec(memory_space=pltpu.VMEM),
        scratch_shapes=[
            pltpu.VMEM((half, rows, width), parts.dtype),
            pltpu.VMEM((half, rows, width), parts.dtype),
            pltpu.VMEM((half, rows, width), parts.dtype),
            pltpu.VMEM((chips * PIECES, rows, width), parts.dtype),
            pltpu.SemaphoreType.DMA((half,)),
            pltpu.SemaphoreType.DMA((sends,)),
            pltpu.SemaphoreType.DMA((half,)),
            pltpu.SemaphoreType.DMA((half,)),
            pltpu.SemaphoreType.DMA((chips * PIECES,)),
        ],
        compiler_params=pltpu.CompilerParams(
            collective_id=2, has_side_effects=True, vmem_limit_bytes=VMEM_BYTES
        ),
    )(parts.reshape(-1, rows, width)).reshape(PIECES * rows, width)


def attend_kernel(
    chips, heads_a, heads_b, query_ref, own_ref, lambda_ref, gain_a_ref, gain_b_ref, out_ref,
    held, top, total, accum_a, accum_b, own_sem, up_sem, side_sem, recv_sem,
):
    chip, core, tp = place()
    me = chip * CORES + core
    rows = own_ref.shape[0]
    mine = pltpu.make_async_copy(own_ref, held.at[me], own_sem)
    mine.start()
    barrier = pltpu.get_barrier_semaphore()

    def hello(sp_to):
        pl.semaphore_signal(barrier, inc=1, device_id={"sp": sp_to, "tp": tp}, device_id_type=MESH)

    hello(chip * CORES + 1 - core)

    @pl.when(chip > 0)
    def _():
        hello(me - CORES)

    @pl.when(chip < chips - 1)
    def _():
        hello(me + CORES)

    pl.semaphore_wait(
        barrier, 1 + jnp.where(chip > 0, 1, 0) + jnp.where(chip < chips - 1, 1, 0)
    )

    top[...] = jnp.full_like(top, -1e30)
    total[...] = jnp.zeros_like(total)
    accum_a[...] = jnp.zeros_like(accum_a)
    accum_b[...] = jnp.zeros_like(accum_b)
    mine.wait()

    def copy_up(back, index):
        return pltpu.make_async_remote_copy(
            src_ref=held.at[index], dst_ref=held.at[index], send_sem=up_sem.at[back],
            recv_sem=recv_sem.at[index], device_id={"sp": me + CORES, "tp": tp}, device_id_type=MESH,
        )

    def copy_side(back, index):
        return pltpu.make_async_remote_copy(
            src_ref=held.at[index], dst_ref=held.at[index], send_sem=side_sem.at[back],
            recv_sem=recv_sem.at[index], device_id={"sp": chip * CORES + 1 - core, "tp": tp},
            device_id_type=MESH,
        )

    base_va = 2 * heads_a * DA
    base_kb = base_va + heads_a * 2 * DA
    base_vb = base_kb + 2 * heads_b * DB
    base_qb = 2 * heads_a * DA
    ahead = lax.broadcasted_iota(jnp.int32, (rows, rows), 0) - lax.broadcasted_iota(
        jnp.int32, (rows, rows), 1
    )

    def flash(index):
        shown = ahead + (me - index) * rows >= 0

        def one(slot, query, key, value, accum, part, size):
            scores = lax.dot_general(
                query, key, (((1,), (1,)), ((), ())), preferred_element_type=jnp.float32
            )
            scores = jnp.where(shown, scores, -1e30)
            before = top[slot]
            after = jnp.maximum(before, jnp.max(scores, -1, keepdims=True))
            factor = size ** (-0.5) * LOG2E
            terms = jnp.exp2((scores - after) * factor)
            rescale = jnp.exp2((before - after) * factor)
            top[slot] = after
            total[slot] = total[slot] * rescale + jnp.sum(terms, -1, keepdims=True)
            accum[part] = accum[part] * rescale + jnp.dot(
                terms.astype(jnp.bfloat16), value, preferred_element_type=jnp.float32
            )

        for head in range(heads_a):
            value = held[index, :, base_va + head * 2 * DA : base_va + (head + 1) * 2 * DA]
            for pair in range(2):
                at = (pair * heads_a + head) * DA
                part = pair * heads_a + head
                one(
                    part, query_ref[:, at : at + DA], held[index, :, at : at + DA], value,
                    accum_a, part, DA,
                )
        for head in range(heads_b):
            value = held[index, :, base_vb + head * 2 * DB : base_vb + (head + 1) * 2 * DB]
            for pair in range(2):
                part = pair * heads_b + head
                at = base_qb + part * 2 * DB
                key_at = base_kb + part // 2 * 2 * DB
                one(
                    2 * heads_a + part, query_ref[:, at : at + 2 * DB],
                    held[index, :, key_at : key_at + 2 * DB], value, accum_b, part, DB,
                )

    def step(number, carry):
        back = number // 2
        side = number % 2
        source = chip - back

        @pl.when(source >= 0)
        def _():
            index = source * CORES + jnp.where(side == 0, core, 1 - core)

            @pl.when(number > 0)
            def _():
                pltpu.make_async_copy(held.at[index], held.at[index], recv_sem.at[index]).wait()

            @pl.when(side == 0)
            def _():
                @pl.when(chip < chips - 1)
                def _():
                    copy_up(back, index).start()

                copy_side(back, index).start()

            @pl.when(index <= me)
            def _():
                flash(index)

        return carry

    lax.fori_loop(0, 2 * chips, step, 0)

    def finish(head, parts, accum, slots, lam, gain_ref, at, wide):
        mixture = accum[parts[0]] / total[slots[0]] - lam * accum[parts[1]] / total[slots[1]]
        out_ref[:, at : at + wide] = rms_norm(mixture, gain_ref[...]).astype(out_ref.dtype)

    for head in range(heads_a):
        parts = (head, heads_a + head)
        finish(head, parts, accum_a, parts, lambda_ref[0:1, head : head + 1], gain_a_ref,
               head * 2 * DA, 2 * DA)
    for head in range(heads_b):
        parts = (head, heads_b + head)
        slots = (2 * heads_a + head, 2 * heads_a + heads_b + head)
        finish(head, parts, accum_b, slots, lambda_ref[0:1, heads_a + head : heads_a + head + 1],
               gain_b_ref, heads_a * 2 * DA + head * 2 * DB, 2 * DB)

    def settle(back, carry):
        @pl.when(chip - back >= 0)
        def _():
            index = (chip - back) * CORES + core

            @pl.when(chip < chips - 1)
            def _():
                copy_up(back, index).wait_send()

            copy_side(back, index).wait_send()

        return carry

    lax.fori_loop(0, chips, settle, 0)


def attend_blocks(queries, own, lambdas, gain_a, gain_b, chips, heads_a, heads_b):
    rows, width = own.shape
    vmem = pl.BlockSpec(memory_space=pltpu.VMEM)
    return pl.pallas_call(
        lambda *refs: attend_kernel(chips, heads_a, heads_b, *refs),
        name="attend_blocks",
        out_shape=jax.ShapeDtypeStruct((rows, heads_a * 2 * DA + heads_b * 2 * DB), jnp.bfloat16),
        in_specs=[vmem, pl.BlockSpec(memory_space=pl.ANY), vmem, vmem, vmem],
        out_specs=vmem,
        scratch_shapes=[
            pltpu.VMEM((chips * CORES, rows, width), own.dtype),
            pltpu.VMEM((2 * (heads_a + heads_b), rows, 1), jnp.float32),
            pltpu.VMEM((2 * (heads_a + heads_b), rows, 1), jnp.float32),
            pltpu.VMEM((2 * heads_a, rows, 2 * DA), jnp.float32),
            pltpu.VMEM((2 * heads_b, rows, 2 * DB), jnp.float32),
            pltpu.SemaphoreType.DMA,
            pltpu.SemaphoreType.DMA((chips,)),
            pltpu.SemaphoreType.DMA((chips,)),
            pltpu.SemaphoreType.DMA((chips * CORES,)),
        ],
        compiler_params=pltpu.CompilerParams(
            collective_id=3, has_side_effects=True, vmem_limit_bytes=VMEM_BYTES
        ),
    )(queries, own, lambdas, gain_a, gain_b)


def pivots_of(chips, slices):
    return [1, chips - 2, 0, chips - 2] if slices == chips == 4 else None


def sliced_kernel(
    chips, tps, heads_a, heads_b, pivots,
    q_ref, own_ref, lambda_ref, gain_a_ref, gain_b_ref, out_ref,
    kvs, qs, accum, top, total, o_out, o_all,
    load_sem, q_send, q_recv, dn_send, up_send, kv_recv, side_send, o_send, o_recv,
):
    chip, core, tp = place()
    rows = out_ref.shape[0]
    slices = len(pivots)
    key_width = 2 * DA
    me = chip * CORES + core

    def pivot(number):
        if isinstance(number, int):
            return pivots[number]
        return sum(jnp.where(number == n, pivots[n], 0) for n in range(slices))

    loads = []
    for number in range(slices):
        if number < heads_a:
            head, stride, q_at, k_at = number, heads_a * DA, 0, 0
        else:
            head, stride = number - heads_a, heads_b * DB
            q_at, k_at = 2 * heads_a * DA, 4 * heads_a * DA
        v_at = k_at + 2 * stride + head * 2 * DA
        moves = []
        for pair in range(2):
            at = pair * stride + head * DA
            spot = pl.ds(pair * DA, DA)
            moves.append((q_ref.at[:, pl.ds(q_at + at, DA)], qs.at[chip, number, :, spot]))
            moves.append((own_ref.at[:, pl.ds(k_at + at, DA)], kvs.at[me, number, :, spot]))
        moves.append(
            (own_ref.at[:, pl.ds(v_at, 2 * DA)], kvs.at[me, number, :, pl.ds(key_width, 2 * DA)])
        )
        loads.append([
            pltpu.make_async_copy(src, dst, load_sem.at[number, place_in])
            for place_in, (src, dst) in enumerate(moves)
        ])
    order = sorted(range(slices), key=lambda n: pivots[n])
    for number in order:
        for copy in loads[number]:
            copy.start()
    greet(chips, 1)

    def remote(src, dst, send, recv, sp_to):
        return pltpu.make_async_remote_copy(
            src_ref=src, dst_ref=dst, send_sem=send, recv_sem=recv,
            device_id={"sp": sp_to, "tp": tp}, device_id_type=MESH,
        )

    def send_q(number):
        ref = qs.at[chip, number]
        return remote(ref, ref, q_send.at[number], q_recv.at[chip, number],
                      pivot(number) * CORES + core)

    def send_kv(number, chip_to, sem):
        ref = kvs.at[me, number]
        return remote(ref, ref, sem, kv_recv.at[me, number], chip_to * CORES + core)

    def send_dn(number):
        return send_kv(number, pivot(number), dn_send.at[number])

    def send_up(number, step):
        return send_kv(number, chip + step, up_send.at[number, step - 1])

    def send_side(chip_of, number):
        ref = kvs.at[chip_of * CORES + core, number]
        return remote(ref, ref, side_send.at[chip_of, number],
                      kv_recv.at[chip_of * CORES + core, number], chip * CORES + 1 - core)

    def send_out(query, number):
        return remote(o_out.at[query, number], o_all.at[number], o_send.at[query, number],
                      o_recv.at[number], query * CORES + core)

    def arrived(ref, sem):
        pltpu.make_async_copy(ref, ref, sem).wait()

    for number in order:
        for copy in loads[number]:
            copy.wait()

        @pl.when(chip > pivots[number])
        def _():
            send_q(number).start()

        @pl.when(chip <= pivots[number])
        def _():
            send_side(chip, number).start()

    for number in order:
        @pl.when(chip > pivots[number])
        def _():
            send_dn(number).start()

    for step in reversed(range(1, chips)):
        for number in order:
            @pl.when(chip + step <= pivots[number])
            def _():
                send_up(number, step).start()

    ahead = lax.broadcasted_iota(jnp.int32, (rows, rows), 0) - lax.broadcasted_iota(
        jnp.int32, (rows, rows), 1
    )
    low_half = lax.broadcasted_iota(jnp.int32, (rows, DA), 1) < DB

    def step_one(query, number, slot, q, kv_chip, pair, v_at, wide, acc_at, size, masked):
        tiles = []
        for side in range(CORES):
            key = kvs[kv_chip * CORES + side, number, :, pair * DA : (pair + 1) * DA]
            scores = lax.dot_general(
                q, key, (((1,), (1,)), ((), ())), preferred_element_type=jnp.float32
            )
            if masked:
                scores = jnp.where(ahead + (core - side) * rows >= 0, scores, -1e30)
            tiles.append(scores)
        before = top[query, number, slot]
        after = jnp.maximum(
            before, jnp.max(jnp.maximum(tiles[0], tiles[1]), -1, keepdims=True)
        )
        factor = size ** (-0.5) * LOG2E
        terms = [jnp.exp2((scores - after) * factor) for scores in tiles]
        rescale = jnp.exp2((before - after) * factor)
        top[query, number, slot] = after
        total[query, number, slot] = total[query, number, slot] * rescale + jnp.sum(
            terms[0] + terms[1], -1, keepdims=True
        )
        fresh = sum(
            jnp.dot(
                terms[side].astype(jnp.bfloat16),
                kvs[kv_chip * CORES + side, number, :, v_at : v_at + wide],
                preferred_element_type=jnp.float32,
            )
            for side in range(CORES)
        )
        span = slice(acc_at, acc_at + wide)
        accum[query, number, pair, :, span] = accum[query, number, pair, :, span] * rescale + fresh

    def flash_a(query, kv_chip, number, masked):
        for pair in range(2):
            step_one(query, number, pair, qs[query, number, :, pair * DA : (pair + 1) * DA],
                     kv_chip, pair, key_width, 2 * DA, 0, DA, masked)

    def flash_b(query, kv_chip, number, masked):
        for pair in range(2):
            both = qs[query, number, :, pair * DA : (pair + 1) * DA]
            for head in range(2):
                keep = low_half if head == 0 else jnp.logical_not(low_half)
                q = jnp.where(keep, both, jnp.zeros_like(both))
                step_one(query, number, pair * 2 + head, q, kv_chip, pair,
                         key_width + head * 2 * DB, 2 * DB, head * 2 * DB, DB, masked)

    def relevant(query, number):
        return jnp.where(query == chip, pivot(number) >= chip, pivot(number) == chip)

    def over(body):
        def run_a(number, carry):
            body(number, flash_a)
            return carry

        def run_b(number, carry):
            body(number, flash_b)
            return carry

        lax.fori_loop(0, heads_a, run_a, 0)
        lax.fori_loop(heads_a, slices, run_b, 0)

    def pair_up(query, kv_chip, first):
        def body(number, flash):
            @pl.when(relevant(query, number))
            def _():
                @pl.when(first)
                def _():
                    top[query, number] = jnp.full(top.shape[2:], -1e30, jnp.float32)
                    total[query, number] = jnp.zeros(total.shape[2:], jnp.float32)
                    accum[query, number] = jnp.zeros(accum.shape[2:], jnp.float32)

                @pl.when(query == kv_chip)
                def _():
                    flash(query, kv_chip, number, True)

                @pl.when(query != kv_chip)
                def _():
                    flash(query, kv_chip, number, False)

        over(body)

    def mix(query, number, slots, spans, lam, gain_ref):
        mixture = (
            accum[query, number, 0, :, spans] / total[query, number, slots[0]]
            - lam * accum[query, number, 1, :, spans] / total[query, number, slots[1]]
        )
        return rms_norm(mixture, gain_ref[...]).astype(jnp.bfloat16)

    def finish(query):
        def body(number, flash):
            @pl.when(relevant(query, number))
            def _():
                if flash is flash_a:
                    lam = lambda_ref[0, tp * heads_a + number]
                    made = [mix(query, number, (0, 1), slice(0, 2 * DA), lam, gain_a_ref)]
                else:
                    made = []
                    for head in range(2):
                        lam = lambda_ref[
                            0, tps * heads_a + tp * heads_b + (number - heads_a) * 2 + head
                        ]
                        made.append(
                            mix(query, number, (head, 2 + head),
                                slice(head * 2 * DB, (head + 1) * 2 * DB), lam, gain_b_ref)
                        )
                wide = 2 * DA // len(made)
                for place_in, values in enumerate(made):
                    span = slice(place_in * wide, (place_in + 1) * wide)

                    @pl.when(query == chip)
                    def _():
                        o_all[number, :, span] = values

                    @pl.when(query != chip)
                    def _():
                        o_out[query, number, :, span] = values

                @pl.when(query != chip)
                def _():
                    send_out(query, number).start()

        over(body)

    above = chips - 1 - chip

    def event(number_of, carry):
        is_own = number_of == 0
        is_query = (number_of > 0) & (number_of <= above)
        is_below = (number_of > above) & (number_of <= above + chip)
        is_above = number_of > above + chip
        source = jnp.where(
            number_of <= above,
            chip + number_of,
            jnp.where(is_below, chip - (number_of - above), number_of - above),
        )
        kv_chip = jnp.where(number_of <= above, chip, source)
        low = jnp.where(is_below, chip, source)
        high = jnp.where(number_of <= above, source, chips - 1)

        def wait_q(number, carry):
            @pl.when(is_query & (pivot(number) == chip))
            def _():
                arrived(qs.at[source, number], q_recv.at[source, number])

            return carry

        def needs(number):
            return jnp.where(source > chip, pivot(number) == chip, pivot(number) >= chip)

        def wait_kv(number, carry):
            @pl.when((is_below | is_above) & needs(number))
            def _():
                index = source * CORES + core
                arrived(kvs.at[index, number], kv_recv.at[index, number])
                send_side(source, number).start()

            return carry

        def wait_side(number, carry):
            @pl.when((is_own | is_below | is_above) & needs(number))
            def _():
                index = source * CORES + 1 - core
                arrived(kvs.at[index, number], kv_recv.at[index, number])

            return carry

        lax.fori_loop(0, slices, wait_q, 0)
        lax.fori_loop(0, slices, wait_kv, 0)
        lax.fori_loop(0, slices, wait_side, 0)

        def queries(query, carry):
            pair_up(query, kv_chip, kv_chip == chip)

            @pl.when(
                ((query == chip) & (number_of == jnp.where(chip > 0, above + chip, 0)))
                | (is_above & (query == source))
            )
            def _():
                finish(query)

            return carry

        lax.fori_loop(low, high + 1, queries, 0)
        return carry

    lax.fori_loop(0, 1 + above + chips - 1, event, 0)

    for number in range(slices):
        @pl.when(chip > pivots[number])
        def _():
            arrived(o_all.at[number], o_recv.at[number])

        out_ref[:, number * 2 * DA : (number + 1) * 2 * DA] = o_all[number]

    for number in range(slices):
        @pl.when(chip > pivots[number])
        def _():
            send_q(number).wait_send()
            send_dn(number).wait_send()

        for step in range(1, chips):
            @pl.when(chip + step <= pivots[number])
            def _():
                send_up(number, step).wait_send()

        for chip_of in range(chips):
            @pl.when(jnp.where(chip_of > chip, pivots[number] == chip, pivots[number] >= chip))
            def _():
                send_side(chip_of, number).wait_send()

            @pl.when((chip_of > chip) & (pivots[number] == chip))
            def _():
                send_out(chip_of, number).wait_send()


def attend_sliced(queries, own, lambdas, gain_a, gain_b, chips, tps, heads_a, heads_b, pivots):
    rows = own.shape[0]
    slices = len(pivots)
    vmem = pl.BlockSpec(memory_space=pltpu.VMEM)
    any_space = pl.BlockSpec(memory_space=pl.ANY)
    dma = pltpu.SemaphoreType.DMA
    return pl.pallas_call(
        lambda *refs: sliced_kernel(chips, tps, heads_a, heads_b, pivots, *refs),
        name="attend_sliced",
        out_shape=jax.ShapeDtypeStruct((rows, slices * 2 * DA), jnp.bfloat16),
        in_specs=[any_space] * 2 + [pl.BlockSpec(memory_space=pltpu.SMEM), vmem, vmem],
        out_specs=vmem,
        scratch_shapes=[
            pltpu.VMEM((chips * CORES, slices, rows, 4 * DA), jnp.bfloat16),
            pltpu.VMEM((chips, slices, rows, 2 * DA), jnp.bfloat16),
            pltpu.VMEM((chips, slices, 2, rows, 2 * DA), jnp.float32),
            pltpu.VMEM((chips, slices, 4, rows, 1), jnp.float32),
            pltpu.VMEM((chips, slices, 4, rows, 1), jnp.float32),
            pltpu.VMEM((chips, slices, rows, 2 * DA), jnp.bfloat16),
            pltpu.VMEM((slices, rows, 2 * DA), jnp.bfloat16),
            dma((slices, 5)),
            dma((slices,)),
            dma((chips, slices)),
            dma((slices,)),
            dma((slices, chips - 1)),
            dma((chips * CORES, slices)),
            dma((chips, slices)),
            dma((chips, slices)),
            dma((slices,)),
        ],
        compiler_params=pltpu.CompilerParams(
            collective_id=6, has_side_effects=True, vmem_limit_bytes=VMEM_BYTES
        ),
    )(queries, own, lambdas, gain_a, gain_b)


def share_kernel(tps, part_ref, out_ref, arrived, send_sem, recv_sem):
    tp = lax.axis_index("tp")
    barrier = pltpu.get_barrier_semaphore()
    for step in range(1, tps):
        pl.semaphore_signal(barrier, inc=1, device_id={"tp": (tp + step) % tps}, device_id_type=MESH)
    pl.semaphore_wait(barrier, tps - 1)
    started = []
    for step in range(1, tps):
        other = (tp + step) % tps
        copy = pltpu.make_async_remote_copy(
            src_ref=part_ref.at[other], dst_ref=arrived.at[step - 1], send_sem=send_sem.at[step - 1],
            recv_sem=recv_sem.at[step - 1], device_id={"tp": other}, device_id_type=MESH,
        )
        copy.start()
        started.append(copy)
    rows = out_ref.shape[0]
    chunk = min(rows, 16)
    for step in range(1, tps):
        started[step - 1].wait()

        @pl.loop(0, rows // chunk)
        def _(part):
            span = pl.ds(pl.multiple_of(part * chunk, chunk), chunk)
            first = part_ref[tp, span, :].astype(jnp.float32) if step == 1 else out_ref[span, :]
            out_ref[span, :] = first + arrived[step - 1, span, :].astype(jnp.float32)


def share_rows(parts, tps):
    _, rows, width = parts.shape
    vmem = pl.BlockSpec(memory_space=pltpu.VMEM)
    return pl.pallas_call(
        lambda *refs: share_kernel(tps, *refs),
        name="share_rows",
        out_shape=jax.ShapeDtypeStruct((rows, width), jnp.float32),
        in_specs=[vmem],
        out_specs=vmem,
        scratch_shapes=[
            pltpu.VMEM((tps - 1, rows, width), parts.dtype),
            pltpu.SemaphoreType.DMA((tps - 1,)),
            pltpu.SemaphoreType.DMA((tps - 1,)),
        ],
        compiler_params=pltpu.CompilerParams(collective_id=4, has_side_effects=True),
    )(parts)


def spread_pairs(queries, heads):
    rows = queries.shape[0]
    pairs = queries.reshape(rows, 2 * heads // 2, 1, 2, DB)
    keep = jnp.eye(2, dtype=queries.dtype).reshape(1, 1, 2, 2, 1)
    return (pairs * keep).reshape(rows, 2 * heads * 2 * DB)


def expert_parts(gathered, expert, experts, capacity, width, weights):
    gate, up, down = weights
    blocks, rows, _ = gathered.shape
    shares = lax.dynamic_slice_in_dim(gathered[:, :, width:], expert, 1, 2)[:, :, 0]
    named = shares > 0
    order = jnp.arange(rows, dtype=jnp.int32)
    slots = jnp.dot(
        named.astype(jnp.bfloat16),
        (order[:, None] < order[None, :]).astype(jnp.bfloat16),
        preferred_element_type=jnp.float32,
    ).astype(jnp.int32)
    picks = (slots[:, None, :] == jnp.arange(capacity, dtype=jnp.int32)[None, :, None]) & named[:, None, :]
    rows_in = jnp.einsum(
        "bct,btd->bcd",
        picks.astype(jnp.bfloat16),
        gathered[:, :, :width],
        preferred_element_type=jnp.float32,
    ).astype(jnp.bfloat16)
    rows_in = rows_in.reshape(blocks * capacity, width)
    gate_pre = jnp.dot(rows_in, gate, preferred_element_type=jnp.float32)
    up_pre = jnp.dot(rows_in, up, preferred_element_type=jnp.float32)
    glu_part = jnp.minimum(gate_pre, 7.0)
    lin_part = jnp.clip(up_pre, -7.0, 7.0)
    hidden = (glu_part * jax.nn.sigmoid(1.702 * glu_part) * (lin_part + 1.0)).astype(jnp.bfloat16)
    outs = jnp.dot(hidden, down, preferred_element_type=jnp.float32).astype(jnp.bfloat16)
    back = jnp.where(picks, shares[:, None, :], 0).astype(jnp.bfloat16)
    return jnp.einsum(
        "bct,bcd->btd",
        back,
        outs.reshape(blocks, capacity, width),
        preferred_element_type=jnp.float32,
    ).astype(jnp.bfloat16)


def meet(chips, tps):
    chip, core, tp = place()
    barrier = pltpu.get_barrier_semaphore()
    others = 0
    for chip_step in range(chips):
        for core_step in range(CORES):
            for tp_step in range(tps):
                if chip_step + core_step + tp_step > 0:
                    others += 1
                    pl.semaphore_signal(
                        barrier,
                        inc=1,
                        device_id={
                            "sp": (chip + chip_step) % chips * CORES + (core + core_step) % CORES,
                            "tp": (tp + tp_step) % tps,
                        },
                        device_id_type=MESH,
                    )
    pl.semaphore_wait(barrier, others)


def group_at(chip, chips, step):
    near = jnp.minimum(chip, chips - 1 - chip)
    both = jnp.where(step % 2 == 1, chip - (step + 1) // 2, chip + step // 2)
    past = jnp.where(chip <= chips - 1 - chip, chip + step - near, chip - step + near)
    return jnp.where(step <= 2 * near, both, past)


def experts_kernel(
    chips, tps, capacity,
    own_ref, meta_ref, gate_ref, up_ref, down_ref, base_ref, gain_ref, out_ref,
    rows_all, meta_all, gate, up, down, rows_in, hidden, back, part, core_in, x_in, z_in,
    z_other, sums,
    load_sem, weight_sem, row_sem, meta_send, meta_recv, up_sem, dn_sem, x_sem, side_sem,
    core_send, core_recv, xs_send, xs_recv, zs_send, zs_recv,
    zo_send, zo_recv,
):
    chip, core, tp = place()
    experts = meta_ref.shape[0] // 2
    piece_rows, width = rows_all.shape[2], rows_all.shape[3]
    rows = piece_rows * CUTS
    ff = gate.shape[1]
    members = CORES * tps
    side_sp = chip * CORES + 1 - core

    def blk(chip_of, core_of, tp_of):
        return (chip_of * CORES + core_of) * tps + tp_of

    def remote(src, dst, send, recv, sp_to, tp_to):
        return pltpu.make_async_remote_copy(
            src_ref=src, dst_ref=dst, send_sem=send, recv_sem=recv,
            device_id={"sp": sp_to, "tp": tp_to}, device_id_type=MESH,
        )

    def rows_copy(block, piece, send, sp_to, tp_to):
        ref = rows_all.at[block, piece]
        return remote(ref, ref, send, row_sem.at[block, piece], sp_to, tp_to)

    def go_up(chip_of, piece):
        return rows_copy(blk(chip_of, core, tp), piece, up_sem.at[chip_of, piece],
                         (chip + 1) * CORES + core, tp)

    def go_dn(chip_of, piece):
        return rows_copy(blk(chip_of, core, tp), piece, dn_sem.at[chip_of, piece],
                         (chip - 1) * CORES + core, tp)

    def go_x(chip_of, step, piece):
        return rows_copy(blk(chip_of, core, tp), piece, x_sem.at[chip_of, step - 1, piece],
                         chip * CORES + core, (tp + step) % tps)

    def go_side(chip_of, tp_of, piece):
        return rows_copy(blk(chip_of, core, tp_of), piece, side_sem.at[chip_of, tp_of, piece],
                         side_sp, tp)

    def wait_rows(block, piece):
        ref = rows_all.at[block, piece]
        pltpu.make_async_copy(ref, ref, row_sem.at[block, piece]).wait()

    mine = blk(chip, core, tp)
    loads = [
        pltpu.make_async_copy(own_ref.at[piece], rows_all.at[mine, piece], load_sem.at[piece])
        for piece in range(CUTS)
    ]
    weights = [
        pltpu.make_async_copy(src, dst, weight_sem.at[number])
        for number, (src, dst) in enumerate(((gate_ref, gate), (up_ref, up), (down_ref, down)))
    ]
    for copy in loads + weights:
        copy.start()
    meta_all[mine] = meta_ref[...]
    meet(chips, tps)

    for piece in range(CUTS):
        loads[piece].wait()
        for step in range(1, tps):
            go_x(chip, step, piece).start()

        @pl.when(chip < chips - 1)
        def _():
            go_up(chip, piece).start()

        @pl.when(chip > 0)
        def _():
            go_dn(chip, piece).start()

        go_side(chip, tp, piece).start()

    def meta_copy(number, chip_step, core_step, tp_step):
        return remote(
            meta_ref, meta_all.at[mine], meta_send.at[number], meta_recv.at[mine],
            (chip + chip_step) % chips * CORES + (core + core_step) % CORES, (tp + tp_step) % tps,
        )

    meta_steps = [
        (chip_step, core_step, tp_step)
        for chip_step in range(chips) for core_step in range(CORES) for tp_step in range(tps)
        if chip_step + core_step + tp_step > 0
    ]
    for number, steps in enumerate(meta_steps):
        meta_copy(number, *steps).start()

    def relay(chip_of, piece, upward):
        wait_rows(blk(chip_of, core, tp), piece)
        for step in range(1, tps):
            go_x(chip_of, step, piece).start()
        if upward:
            @pl.when(chip < chips - 1)
            def _():
                go_up(chip_of, piece).start()
        else:
            @pl.when(chip > 0)
            def _():
                go_dn(chip_of, piece).start()
        go_side(chip_of, tp, piece).start()

    def compute(group):
        order = lax.broadcasted_iota(jnp.int32, (capacity, rows), 0).astype(jnp.float32)
        expert = chip * CORES + core
        for member in range(members):
            block = group * members + member
            slot = meta_all[block, pl.ds(expert, 1), :]
            share = meta_all[block, pl.ds(experts + expert, 1), :]
            hit = slot == order
            picks = jnp.where(hit, 1.0, 0.0).astype(jnp.bfloat16)
            back[member] = jnp.where(hit, share, 0.0).astype(jnp.bfloat16)
            values = rows_all[block].reshape(rows, width)
            rows_in[member * capacity : (member + 1) * capacity, :] = jnp.dot(
                picks, values, preferred_element_type=jnp.float32
            ).astype(jnp.bfloat16)
        cut = min(ff, 256)

        @pl.loop(0, ff // cut)
        def _(number):
            cols = pl.ds(pl.multiple_of(number * cut, cut), cut)
            gate_pre = jnp.dot(rows_in[...], gate[:, cols], preferred_element_type=jnp.float32)
            up_pre = jnp.dot(rows_in[...], up[:, cols], preferred_element_type=jnp.float32)
            glu_part = jnp.minimum(gate_pre, 7.0)
            lin_part = jnp.clip(up_pre, -7.0, 7.0)
            hidden[:, cols] = (
                glu_part * jax.nn.sigmoid(1.702 * glu_part) * (lin_part + 1.0)
            ).astype(jnp.bfloat16)

        wide = min(width, 256)

        @pl.loop(0, width // wide)
        def _(number):
            cols = pl.ds(pl.multiple_of(number * wide, wide), wide)
            outs = jnp.dot(
                hidden[...], down[:, cols], preferred_element_type=jnp.float32
            ).astype(jnp.bfloat16)
            for member in range(members):
                spread = lax.dot_general(
                    back[member], outs[member * capacity : (member + 1) * capacity],
                    (((0,), (0,)), ((), ())), preferred_element_type=jnp.float32,
                ).astype(jnp.bfloat16)
                part[group * members + member, :, :, cols] = spread.reshape(
                    CUTS, piece_rows, wide
                )

    def add(target, index, source, source_index):
        chunk = min(piece_rows, 16)

        @pl.loop(0, piece_rows // chunk)
        def _(number):
            span = pl.ds(pl.multiple_of(number * chunk, chunk), chunk)
            target[index + (span,)] = (
                target[index + (span,)].astype(jnp.float32)
                + source[source_index + (span,)].astype(jnp.float32)
            ).astype(target.dtype)

    def core_copy(group, tp_of):
        return remote(part.at[blk(group, 1 - core, tp_of)], core_in.at[group, tp_of],
                      core_send.at[group, tp_of], core_recv.at[group, tp_of], side_sp, tp)

    def part_x(group, step, piece):
        return remote(part.at[blk(group, core, (tp + step) % tps), piece],
                      x_in.at[group, step - 1, piece], xs_send.at[group, step - 1, piece],
                      xs_recv.at[group, step - 1, piece], chip * CORES + core, (tp + step) % tps)

    def part_z(way, group, piece):
        return remote(part.at[blk(group, core, tp), piece], z_in.at[way, group, piece],
                      zs_send.at[way, group, piece], zs_recv.at[way, group, piece],
                      (chip + 1 - 2 * way) * CORES + core, tp)

    def other_z(way, step, piece):
        group = chip + 1 - 2 * way
        return remote(part.at[blk(group, core, (tp + step) % tps), piece],
                      z_other.at[way, step - 1, piece], zo_send.at[way, step - 1, piece],
                      zo_recv.at[way, step - 1, piece], group * CORES + core, tp)

    def far(group):
        return (group - chip >= 2) | (chip - group >= 2)

    def arrived(ref, sem):
        pltpu.make_async_copy(ref, ref, sem).wait()

    def cross(group):
        for tp_of in range(tps):
            core_copy(group, tp_of).start()
        for step in list(range(1, tps)) + [0]:
            tp_of = (tp + step) % tps
            arrived(core_in.at[group, tp_of], core_recv.at[group, tp_of])
            for piece in range(CUTS):
                add(part, (blk(group, core, tp_of), piece), core_in, (group, tp_of, piece))
                if step > 0:
                    @pl.when(far(group))
                    def _():
                        part_x(group, step, piece).start()

                    for way in range(2):
                        @pl.when(group == chip + 1 - 2 * way)
                        def _():
                            other_z(way, step, piece).start()

    def settle(group):
        for piece in range(CUTS):
            @pl.when(far(group))
            def _():
                for step in range(1, tps):
                    arrived(x_in.at[group, step - 1, piece], xs_recv.at[group, step - 1, piece])
                    add(part, (blk(group, core, tp), piece), x_in, (group, step - 1, piece))

            @pl.when((chip == 0) & (group > 0))
            def _():
                part_z(0, group, piece).start()

            @pl.when((chip == chips - 1) & (group < chips - 1))
            def _():
                part_z(1, group, piece).start()

    def wave(step, carry):
        @pl.when(step < chips)
        def _():
            for piece in range(CUTS):
                @pl.when(chip - step >= 0)
                def _():
                    relay(chip - step, piece, True)

                @pl.when(chip + step < chips)
                def _():
                    relay(chip + step, piece, False)

        group = group_at(chip, chips, step - 1)
        for piece in range(CUTS):
            for tp_step in range(1, tps):
                tp_of = (tp + tp_step) % tps
                wait_rows(blk(group, core, tp_of), piece)
                go_side(group, tp_of, piece).start()

        @pl.when(step == 1)
        def _():
            for steps in meta_steps:
                block = blk((chip + steps[0]) % chips, (core + steps[1]) % CORES, (tp + steps[2]) % tps)
                arrived(meta_all.at[block], meta_recv.at[block])
            for copy in weights:
                copy.wait()

        for piece in range(CUTS):
            for tp_of in range(tps):
                wait_rows(blk(group, 1 - core, tp_of), piece)
        compute(group)
        cross(group)

        @pl.when(step > 1)
        def _():
            settle(group_at(chip, chips, step - 2))

        return carry

    lax.fori_loop(1, chips + 1, wave, 0)
    for piece in range(CUTS):
        for step in range(1, tps):
            for way in range(2):
                @pl.when(chip > 0 if way == 0 else chip < chips - 1)
                def _():
                    arrived(z_other.at[way, step - 1, piece], zo_recv.at[way, step - 1, piece])
                    add(part, (blk(chip, core, (tp + step) % tps), piece), z_other,
                        (way, step - 1, piece))

            part_x(chip, step, piece).start()

    settle(group_at(chip, chips, chips - 1))

    def chain(number, carry):
        for way in range(2):
            group = number if way == 0 else chips - 1 - number
            if way == 0:
                passes = (chip > 0) & (chip < group)
            else:
                passes = (chip < chips - 1) & (chip > group)

            @pl.when(passes)
            def _():
                for piece in range(CUTS):
                    arrived(z_in.at[way, group, piece], zs_recv.at[way, group, piece])
                    add(part, (blk(group, core, tp), piece), z_in, (way, group, piece))
                    part_z(way, group, piece).start()

        return carry

    lax.fori_loop(1, chips, chain, 0)

    chunk = min(piece_rows, 16)

    def each_chunk(body):
        @pl.loop(0, piece_rows // chunk)
        def _(number):
            body(pl.ds(pl.multiple_of(number * chunk, chunk), chunk))

    for piece in range(CUTS):
        for step in range(1, tps):
            arrived(x_in.at[chip, step - 1, piece], xs_recv.at[chip, step - 1, piece])

        def begin(span):
            start = part[mine, piece, span, :].astype(jnp.float32)
            for step in range(1, tps):
                start = start + x_in[chip, step - 1, piece, span, :].astype(jnp.float32)
            sums[span, :] = start

        each_chunk(begin)
        for way in range(2):
            def more(span):
                sums[span, :] = sums[span, :] + z_in[way, chip, piece, span, :].astype(jnp.float32)

            @pl.when(chip > 0 if way == 0 else chip < chips - 1)
            def _():
                arrived(z_in.at[way, chip, piece], zs_recv.at[way, chip, piece])
                each_chunk(more)

        def close(span):
            out_ref[piece, span, :] = (
                base_ref[piece, span, :].astype(jnp.float32) + rms_norm(sums[span, :], gain_ref[...])
            ).astype(out_ref.dtype)

        each_chunk(close)

    for number, steps in enumerate(meta_steps):
        meta_copy(number, *steps).wait_send()

    def finish(group, carry):
        for piece in range(CUTS):
            for step in range(1, tps):
                go_x(group, step, piece).wait_send()

                @pl.when(far(group) | (group == chip))
                def _():
                    part_x(group, step, piece).wait_send()

            for tp_of in range(tps):
                go_side(group, tp_of, piece).wait_send()

            @pl.when((group <= chip) & (chip < chips - 1))
            def _():
                go_up(group, piece).wait_send()

            @pl.when((group >= chip) & (chip > 0))
            def _():
                go_dn(group, piece).wait_send()

            @pl.when(group > chip)
            def _():
                part_z(0, group, piece).wait_send()

            @pl.when(group < chip)
            def _():
                part_z(1, group, piece).wait_send()

        for tp_of in range(tps):
            core_copy(group, tp_of).wait_send()
        return carry

    lax.fori_loop(0, chips, finish, 0)
    for piece in range(CUTS):
        for step in range(1, tps):
            for way in range(2):
                @pl.when(chip < chips - 1 if way == 0 else chip > 0)
                def _():
                    other_z(way, step, piece).wait_send()


def experts_bytes(rows, width, ff, chips, tps, capacity):
    blocks = chips * CORES * tps
    members = CORES * tps
    buffers = blocks * 2 + chips * (2 * tps - 1 + 2) + 2 * tps + 4
    return 2 * (
        rows * width * buffers + 3 * width * ff + members * capacity * (width + ff) + 2 * rows * width
    )


def run_experts(normed, meta, gate, up, down, base, gain, chips, tps, capacity):
    rows, width = normed.shape
    ff = gate.shape[1]
    blocks = chips * CORES * tps
    members = CORES * tps
    piece_rows = rows // CUTS
    vmem = pl.BlockSpec(memory_space=pltpu.VMEM)
    any_space = pl.BlockSpec(memory_space=pl.ANY)
    dma = pltpu.SemaphoreType.DMA
    bf16 = jnp.bfloat16
    return pl.pallas_call(
        lambda *refs: experts_kernel(chips, tps, capacity, *refs),
        name="run_experts",
        out_shape=jax.ShapeDtypeStruct((CUTS, piece_rows, width), bf16),
        in_specs=[any_space, vmem, any_space, any_space, any_space, vmem, vmem],
        out_specs=vmem,
        scratch_shapes=[
            pltpu.VMEM((blocks, CUTS, piece_rows, width), bf16),
            pltpu.VMEM((blocks,) + meta.shape, meta.dtype),
            pltpu.VMEM(gate.shape, bf16),
            pltpu.VMEM(up.shape, bf16),
            pltpu.VMEM(down.shape, bf16),
            pltpu.VMEM((members * capacity, width), bf16),
            pltpu.VMEM((members * capacity, ff), bf16),
            pltpu.VMEM((members, capacity, rows), bf16),
            pltpu.VMEM((blocks, CUTS, piece_rows, width), bf16),
            pltpu.VMEM((chips, tps, CUTS, piece_rows, width), bf16),
            pltpu.VMEM((chips, tps - 1, CUTS, piece_rows, width), bf16),
            pltpu.VMEM((2, chips, CUTS, piece_rows, width), bf16),
            pltpu.VMEM((2, tps - 1, CUTS, piece_rows, width), bf16),
            pltpu.VMEM((piece_rows, width), jnp.float32),
            dma((CUTS,)),
            dma((3,)),
            dma((blocks, CUTS)),
            dma((blocks - 1,)),
            dma((blocks,)),
            dma((chips, CUTS)),
            dma((chips, CUTS)),
            dma((chips, tps - 1, CUTS)),
            dma((chips, tps, CUTS)),
            dma((chips, tps)),
            dma((chips, tps)),
            dma((chips, tps - 1, CUTS)),
            dma((chips, tps - 1, CUTS)),
            dma((2, chips, CUTS)),
            dma((2, chips, CUTS)),
            dma((2, tps - 1, CUTS)),
            dma((2, tps - 1, CUTS)),
        ],
        compiler_params=pltpu.CompilerParams(
            collective_id=5, has_side_effects=True, vmem_limit_bytes=VMEM_BYTES
        ),
    )(
        normed.reshape(CUTS, piece_rows, width), meta, gate, up, down,
        base.reshape(CUTS, piece_rows, width), gain,
    ).reshape(rows, width)


def slot_table(routes, route_weights, experts):
    rows = routes.shape[0]
    chosen = routes[None, :, :] == jnp.arange(experts, dtype=jnp.int32)[:, None, None]
    shares = jnp.sum(jnp.where(chosen, route_weights[None], 0.0), 2)
    named = jnp.any(chosen, 2)
    order = jnp.arange(rows, dtype=jnp.int32)
    slots = jnp.dot(
        named.astype(jnp.bfloat16),
        (order[:, None] < order[None, :]).astype(jnp.bfloat16),
        preferred_element_type=jnp.float32,
    )
    return jnp.concatenate([jnp.where(named, slots, -1.0), shares], 0)


def spread_experts(normed, routes, route_weights, seq_slot, experts, capacity, chips, tps, weights):
    width = normed.shape[1]
    extra = -(-experts // 128) * 128
    shares = jnp.sum(
        jnp.where(
            routes[:, :, None] == jnp.arange(extra, dtype=jnp.int32)[None, None, :],
            route_weights[:, :, None],
            0.0,
        ),
        1,
    ).astype(jnp.bfloat16)
    gathered = gather_rows(jnp.concatenate([normed, shares], 1), chips, tps)
    parts = expert_parts(gathered, seq_slot, experts, capacity, width, weights)
    return scatter_rows(parts, chips, tps)


def per_device(
    queries_a,
    keys_a,
    values_a,
    queries_b,
    keys_b,
    values_b,
    lambdas,
    head_gain_a,
    head_gain_b,
    out_a,
    out_b,
    residual,
    gain_mix,
    gain_pre,
    gain_post,
    routes,
    route_weights,
    expert_gate,
    expert_up,
    expert_down,
):
    length = queries_a.shape[0]
    heads_a = queries_a.shape[2] // DA
    heads_b = queries_b.shape[2] // DB
    head_slot = lax.axis_index("tp")
    seq_slot = lax.axis_index("sp")
    experts, tps = lax.axis_size("sp"), lax.axis_size("tp")
    chips = experts // CORES
    pivots = pivots_of(chips, heads_a + heads_b // 2)
    own = jnp.concatenate(
        [keys_a.reshape(length, -1), values_a, keys_b.reshape(length, -1), values_b], 1
    )
    if pivots is not None:
        heads_out = attend_sliced(
            jnp.concatenate([queries_a.reshape(length, -1), queries_b.reshape(length, -1)], 1),
            own, lambdas[None], head_gain_a[None], head_gain_b[None], chips, tps, heads_a, heads_b,
            pivots,
        )
    else:
        lambda_a = lax.dynamic_slice_in_dim(lambdas, head_slot * heads_a, heads_a)
        lambda_b = lax.dynamic_slice_in_dim(lambdas, HA + head_slot * heads_b, heads_b)
        queries = jnp.concatenate(
            [queries_a.reshape(length, -1), spread_pairs(queries_b, heads_b)], 1
        )
        heads_out = attend_blocks(
            queries,
            own,
            jnp.concatenate([lambda_a, lambda_b])[None],
            head_gain_a[None],
            head_gain_b[None],
            chips,
            heads_a,
            heads_b,
        )
    cut = heads_a * 2 * DA
    mixed = (
        jnp.dot(heads_out[:, :cut], out_a, preferred_element_type=jnp.float32)
        + jnp.dot(heads_out[:, cut:], out_b, preferred_element_type=jnp.float32)
    ).astype(jnp.bfloat16)
    mixed_rows = share_rows(mixed.reshape(tps, length // tps, -1), tps)
    after_mix = (residual.astype(jnp.float32) + rms_norm(mixed_rows, gain_mix)).astype(jnp.bfloat16)
    normed = rms_norm(after_mix.astype(jnp.float32), gain_pre).astype(jnp.bfloat16)
    sub_rows = residual.shape[0]
    top_count = routes.shape[1]
    capacity = min(sub_rows, (5 * sub_rows * top_count + 4 * experts - 1) // (4 * experts))
    width = residual.shape[1]
    slots = -(-capacity // 16) * 16
    if experts_bytes(sub_rows, width, expert_gate.shape[2], chips, tps, slots) < VMEM_BYTES * 9 // 10:
        return run_experts(
            normed, slot_table(routes, route_weights, experts), expert_gate[0], expert_up[0],
            expert_down[0], after_mix, gain_post[None], chips, tps, slots,
        )
    routed = spread_experts(
        normed, routes, route_weights, seq_slot, experts, capacity, chips, tps,
        (expert_gate[0], expert_up[0], expert_down[0]),
    )
    return (after_mix.astype(jnp.float32) + rms_norm(routed, gain_post)).astype(jnp.bfloat16)


def solution(mesh):
    in_specs = (
        P(("grp", "sp"), None, "tp"),
        P(("grp", "sp"), None, "tp"),
        P(("grp", "sp"), "tp"),
        P(("grp", "sp"), None, "tp"),
        P(("grp", "sp"), None, "tp"),
        P(("grp", "sp"), "tp"),
        P(),
        P(),
        P(),
        P("tp", None),
        P("tp", None),
        P(("grp", "sp", "tp"), None),
        P(),
        P(),
        P(),
        P(("grp", "sp", "tp"), None),
        P(("grp", "sp", "tp"), None),
        P("sp", None, "tp"),
        P("sp", None, "tp"),
        P("sp", "tp", None),
    )
    out_specs = P(("grp", "sp", "tp"), None)
    return jax.shard_map(
        per_device, mesh=mesh, in_specs=in_specs, out_specs=out_specs, check_vma=False
    )
```

```python
import jax
import jax.numpy as jnp
from jax import lax
from jax.experimental import pallas as pl
from jax.experimental.pallas import tpu as pltpu
from jax.sharding import PartitionSpec as P

HA = 4
DA = 128
DB = 64


def rms_norm(values, gain_vec):
    return values * lax.rsqrt(jnp.mean(values * values, -1, keepdims=True) + 1e-06) * gain_vec


MESH = pl.DeviceIdType.MESH
CORES = 2
PIECES = 2
CUTS = 4
LOG2E = 1.4426950408889634
VMEM_BYTES = 60 * 1024 * 1024


def place():
    sp = lax.axis_index("sp")
    return sp // CORES, sp % CORES, lax.axis_index("tp")


def greet(chips, tps):
    chip, core, tp = place()
    barrier = pltpu.get_barrier_semaphore()
    for step in range(1, chips):
        other = (chip + step) % chips
        pl.semaphore_signal(
            barrier, inc=1, device_id={"sp": other * CORES + core, "tp": tp}, device_id_type=MESH
        )
    for step in range(1, tps):
        pl.semaphore_signal(
            barrier,
            inc=1,
            device_id={"sp": chip * CORES + core, "tp": (tp + step) % tps},
            device_id_type=MESH,
        )
    pl.semaphore_signal(
        barrier, inc=1, device_id={"sp": chip * CORES + 1 - core, "tp": tp}, device_id_type=MESH
    )
    pl.semaphore_wait(barrier, chips - 1 + tps - 1 + 1)


def gather_kernel(chips, tps, own_ref, all_ref, send_sem, recv_sem, own_sem):
    chip, core, tp = place()
    greet(chips, tps)
    started = []

    def block(chip_of, core_of, tp_of, piece):
        return ((chip_of * CORES + core_of) * tps + tp_of) * PIECES + piece

    def send(source, index, sp_to, tp_to):
        copy = pltpu.make_async_remote_copy(
            src_ref=source,
            dst_ref=all_ref.at[index],
            send_sem=send_sem.at[len(started)],
            recv_sem=recv_sem.at[index],
            device_id={"sp": sp_to, "tp": tp_to},
            device_id_type=MESH,
        )
        copy.start()
        started.append(copy)

    def arrived(index):
        pltpu.make_async_copy(all_ref.at[index], all_ref.at[index], recv_sem.at[index]).wait()

    for piece in range(PIECES):
        own = block(chip, core, tp, piece)
        for step in range(1, tps):
            send(own_ref.at[piece], own, chip * CORES + core, (tp + step) % tps)
        for step in range(1, chips):
            send(own_ref.at[piece], own, (chip + step) % chips * CORES + core, tp)
        send(own_ref.at[piece], own, chip * CORES + 1 - core, tp)
    mine = pltpu.make_async_copy(
        own_ref, all_ref.at[pl.ds(block(chip, core, tp, 0), PIECES)], own_sem
    )
    mine.start()

    def from_tp(chip_of, piece):
        for step in range(1, tps):
            index = block(chip_of, core, (tp + step) % tps, piece)
            arrived(index)
            send(all_ref.at[index], index, chip * CORES + 1 - core, tp)

    order = [(step, piece) for step in range(chips) for piece in range(PIECES)]
    for place_in, (step, piece) in enumerate(order):
        if step > 0:
            index = block((chip - step + chips) % chips, core, tp, piece)
            arrived(index)
            for tp_step in range(1, tps):
                send(all_ref.at[index], index, chip * CORES + core, (tp + tp_step) % tps)
            send(all_ref.at[index], index, chip * CORES + 1 - core, tp)
            done, done_piece = order[place_in - PIECES]
            from_tp((chip - done + chips) % chips, done_piece)
    for piece in range(PIECES):
        from_tp((chip + 1) % chips, piece)
    for step, piece in order:
        for tp_of in range(tps):
            arrived(block((chip - step + chips) % chips, 1 - core, (tp + tp_of) % tps, piece))
    mine.wait()
    for copy in started:
        copy.wait_send()


def gather_rows(own, chips, tps):
    blocks = chips * CORES * tps * PIECES
    sends = (chips - 1 + tps - 1 + 1 + (chips - 1) * tps + chips * (tps - 1)) * PIECES
    rows, width = own.shape
    own = own.reshape(PIECES, rows // PIECES, width)
    return pl.pallas_call(
        lambda *refs: gather_kernel(chips, tps, *refs),
        name="gather_rows",
        out_shape=jax.ShapeDtypeStruct((blocks,) + own.shape[1:], own.dtype),
        in_specs=[pl.BlockSpec(memory_space=pl.ANY)],
        out_specs=pl.BlockSpec(memory_space=pl.ANY),
        scratch_shapes=[
            pltpu.SemaphoreType.DMA((sends,)),
            pltpu.SemaphoreType.DMA((blocks,)),
            pltpu.SemaphoreType.DMA,
        ],
        compiler_params=pltpu.CompilerParams(collective_id=1, has_side_effects=True),
    )(own).reshape(-1, rows, width)


def add_rows(target, index, source, source_index):
    rows = target.shape[1]
    chunk = min(rows, 16)

    @pl.loop(0, rows // chunk)
    def _(part):
        span = pl.ds(pl.multiple_of(part * chunk, chunk), chunk)
        target[index, span, :] = (
            target[index, span, :].astype(jnp.float32)
            + source[source_index, span, :].astype(jnp.float32)
        ).astype(target.dtype)


def scatter_kernel(
    chips, tps, part_ref, out_ref, acc, core_in, tp_in, chip_in, load_sem, send_sem, core_sem, tp_sem, chip_sem
):
    chip, core, tp = place()
    load = []
    started = []
    order = [(step, piece) for step in range(chips) for piece in range(PIECES)]
    for step, piece in order:
        for tp_step in range(tps):
            chip_of, tp_of = (chip + 1 + step) % chips, (tp + 1 + tp_step) % tps
            copy = pltpu.make_async_copy(
                part_ref.at[((chip_of * CORES + core) * tps + tp_of) * PIECES + piece],
                acc.at[(chip_of * tps + tp_of) * PIECES + piece],
                load_sem.at[len(load)],
            )
            copy.start()
            load.append(copy)
    greet(chips, tps)

    def send(source, target, recv_sem, sp_to, tp_to):
        copy = pltpu.make_async_remote_copy(
            src_ref=source,
            dst_ref=target,
            send_sem=send_sem.at[len(started)],
            recv_sem=recv_sem,
            device_id={"sp": sp_to, "tp": tp_to},
            device_id_type=MESH,
        )
        copy.start()
        started.append(copy)

    def arrived(target, index, sem):
        pltpu.make_async_copy(target.at[index], target.at[index], sem).wait()

    for step, piece in order:
        chip_of = (chip + 1 + step) % chips
        for tp_step in range(tps):
            tp_of = (tp + 1 + tp_step) % tps
            index = (chip_of * tps + tp_of) * PIECES + piece
            send(
                part_ref.at[((chip_of * CORES + 1 - core) * tps + tp_of) * PIECES + piece],
                core_in.at[index],
                core_sem.at[index],
                chip * CORES + 1 - core,
                tp,
            )

    def chip_stage(step, piece):
        chip_of = (chip + 1 + step) % chips
        kept = (chip_of * tps + tp) * PIECES + piece
        for tp_step in range(1, tps):
            index = (chip_of * tps + (tp + tp_step) % tps) * PIECES + piece
            arrived(tp_in, index, tp_sem.at[index])
            add_rows(acc, kept, tp_in, index)
        if step < chips - 1:
            slot = chip * PIECES + piece
            send(acc.at[kept], chip_in.at[slot], chip_sem.at[slot], chip_of * CORES + core, tp)

    for number, (step, piece) in enumerate(order):
        chip_of = (chip + 1 + step) % chips
        for tp_step in range(tps):
            tp_of = (tp + 1 + tp_step) % tps
            index = (chip_of * tps + tp_of) * PIECES + piece
            load[number * tps + tp_step].wait()
            arrived(core_in, index, core_sem.at[index])
            add_rows(acc, index, core_in, index)
            if tp_step < tps - 1:
                slot = (chip_of * tps + tp) * PIECES + piece
                send(
                    acc.at[index], tp_in.at[slot], tp_sem.at[slot], chip * CORES + core, tp_of
                )
        if number > 0:
            chip_stage(*order[number - 1])
    chip_stage(*order[-1])
    rows = out_ref.shape[1]
    chunk = min(rows, 16)
    for step in range(1, chips):
        for piece in range(PIECES):
            source = (chip - step + chips) % chips * PIECES + piece
            kept = (chip * tps + tp) * PIECES + piece
            arrived(chip_in, source, chip_sem.at[source])
            if step < chips - 1:
                add_rows(acc, kept, chip_in, source)
            else:

                @pl.loop(0, rows // chunk)
                def _(part):
                    span = pl.ds(pl.multiple_of(part * chunk, chunk), chunk)
                    out_ref[piece, span, :] = acc[kept, span, :].astype(jnp.float32) + chip_in[
                        source, span, :
                    ].astype(jnp.float32)

    for copy in started:
        copy.wait_send()


def scatter_rows(parts, chips, tps):
    blocks, rows, width = parts.shape
    half = chips * tps * PIECES
    sends = half + (chips * (tps - 1) + chips - 1) * PIECES
    rows = rows // PIECES
    return pl.pallas_call(
        lambda *refs: scatter_kernel(chips, tps, *refs),
        name="scatter_rows",
        out_shape=jax.ShapeDtypeStruct((PIECES, rows, width), jnp.float32),
        in_specs=[pl.BlockSpec(memory_space=pl.ANY)],
        out_specs=pl.BlockSpec(memory_space=pltpu.VMEM),
        scratch_shapes=[
            pltpu.VMEM((half, rows, width), parts.dtype),
            pltpu.VMEM((half, rows, width), parts.dtype),
            pltpu.VMEM((half, rows, width), parts.dtype),
            pltpu.VMEM((chips * PIECES, rows, width), parts.dtype),
            pltpu.SemaphoreType.DMA((half,)),
            pltpu.SemaphoreType.DMA((sends,)),
            pltpu.SemaphoreType.DMA((half,)),
            pltpu.SemaphoreType.DMA((half,)),
            pltpu.SemaphoreType.DMA((chips * PIECES,)),
        ],
        compiler_params=pltpu.CompilerParams(
            collective_id=2, has_side_effects=True, vmem_limit_bytes=VMEM_BYTES
        ),
    )(parts.reshape(-1, rows, width)).reshape(PIECES * rows, width)


def attend_kernel(
    chips, heads_a, heads_b, query_ref, own_ref, lambda_ref, gain_a_ref, gain_b_ref, out_ref,
    held, top, total, accum_a, accum_b, own_sem, up_sem, side_sem, recv_sem,
):
    chip, core, tp = place()
    me = chip * CORES + core
    rows = own_ref.shape[0]
    mine = pltpu.make_async_copy(own_ref, held.at[me], own_sem)
    mine.start()
    barrier = pltpu.get_barrier_semaphore()

    def hello(sp_to):
        pl.semaphore_signal(barrier, inc=1, device_id={"sp": sp_to, "tp": tp}, device_id_type=MESH)

    hello(chip * CORES + 1 - core)

    @pl.when(chip > 0)
    def _():
        hello(me - CORES)

    @pl.when(chip < chips - 1)
    def _():
        hello(me + CORES)

    pl.semaphore_wait(
        barrier, 1 + jnp.where(chip > 0, 1, 0) + jnp.where(chip < chips - 1, 1, 0)
    )

    top[...] = jnp.full_like(top, -1e30)
    total[...] = jnp.zeros_like(total)
    accum_a[...] = jnp.zeros_like(accum_a)
    accum_b[...] = jnp.zeros_like(accum_b)
    mine.wait()

    def copy_up(back, index):
        return pltpu.make_async_remote_copy(
            src_ref=held.at[index], dst_ref=held.at[index], send_sem=up_sem.at[back],
            recv_sem=recv_sem.at[index], device_id={"sp": me + CORES, "tp": tp}, device_id_type=MESH,
        )

    def copy_side(back, index):
        return pltpu.make_async_remote_copy(
            src_ref=held.at[index], dst_ref=held.at[index], send_sem=side_sem.at[back],
            recv_sem=recv_sem.at[index], device_id={"sp": chip * CORES + 1 - core, "tp": tp},
            device_id_type=MESH,
        )

    base_va = 2 * heads_a * DA
    base_kb = base_va + heads_a * 2 * DA
    base_vb = base_kb + 2 * heads_b * DB
    base_qb = 2 * heads_a * DA
    ahead = lax.broadcasted_iota(jnp.int32, (rows, rows), 0) - lax.broadcasted_iota(
        jnp.int32, (rows, rows), 1
    )

    def flash(index):
        shown = ahead + (me - index) * rows >= 0

        def one(slot, query, key, value, accum, part, size):
            scores = lax.dot_general(
                query, key, (((1,), (1,)), ((), ())), preferred_element_type=jnp.float32
            )
            scores = jnp.where(shown, scores, -1e30)
            before = top[slot]
            after = jnp.maximum(before, jnp.max(scores, -1, keepdims=True))
            factor = size ** (-0.5) * LOG2E
            terms = jnp.exp2((scores - after) * factor)
            rescale = jnp.exp2((before - after) * factor)
            top[slot] = after
            total[slot] = total[slot] * rescale + jnp.sum(terms, -1, keepdims=True)
            accum[part] = accum[part] * rescale + jnp.dot(
                terms.astype(jnp.bfloat16), value, preferred_element_type=jnp.float32
            )

        for head in range(heads_a):
            value = held[index, :, base_va + head * 2 * DA : base_va + (head + 1) * 2 * DA]
            for pair in range(2):
                at = (pair * heads_a + head) * DA
                part = pair * heads_a + head
                one(
                    part, query_ref[:, at : at + DA], held[index, :, at : at + DA], value,
                    accum_a, part, DA,
                )
        for head in range(heads_b):
            value = held[index, :, base_vb + head * 2 * DB : base_vb + (head + 1) * 2 * DB]
            for pair in range(2):
                part = pair * heads_b + head
                at = base_qb + part * 2 * DB
                key_at = base_kb + part // 2 * 2 * DB
                one(
                    2 * heads_a + part, query_ref[:, at : at + 2 * DB],
                    held[index, :, key_at : key_at + 2 * DB], value, accum_b, part, DB,
                )

    def step(number, carry):
        back = number // 2
        side = number % 2
        source = chip - back

        @pl.when(source >= 0)
        def _():
            index = source * CORES + jnp.where(side == 0, core, 1 - core)

            @pl.when(number > 0)
            def _():
                pltpu.make_async_copy(held.at[index], held.at[index], recv_sem.at[index]).wait()

            @pl.when(side == 0)
            def _():
                @pl.when(chip < chips - 1)
                def _():
                    copy_up(back, index).start()

                copy_side(back, index).start()

            @pl.when(index <= me)
            def _():
                flash(index)

        return carry

    lax.fori_loop(0, 2 * chips, step, 0)

    def finish(head, parts, accum, slots, lam, gain_ref, at, wide):
        mixture = accum[parts[0]] / total[slots[0]] - lam * accum[parts[1]] / total[slots[1]]
        out_ref[:, at : at + wide] = rms_norm(mixture, gain_ref[...]).astype(out_ref.dtype)

    for head in range(heads_a):
        parts = (head, heads_a + head)
        finish(head, parts, accum_a, parts, lambda_ref[0:1, head : head + 1], gain_a_ref,
               head * 2 * DA, 2 * DA)
    for head in range(heads_b):
        parts = (head, heads_b + head)
        slots = (2 * heads_a + head, 2 * heads_a + heads_b + head)
        finish(head, parts, accum_b, slots, lambda_ref[0:1, heads_a + head : heads_a + head + 1],
               gain_b_ref, heads_a * 2 * DA + head * 2 * DB, 2 * DB)

    def settle(back, carry):
        @pl.when(chip - back >= 0)
        def _():
            index = (chip - back) * CORES + core

            @pl.when(chip < chips - 1)
            def _():
                copy_up(back, index).wait_send()

            copy_side(back, index).wait_send()

        return carry

    lax.fori_loop(0, chips, settle, 0)


def attend_blocks(queries, own, lambdas, gain_a, gain_b, chips, heads_a, heads_b):
    rows, width = own.shape
    vmem = pl.BlockSpec(memory_space=pltpu.VMEM)
    return pl.pallas_call(
        lambda *refs: attend_kernel(chips, heads_a, heads_b, *refs),
        name="attend_blocks",
        out_shape=jax.ShapeDtypeStruct((rows, heads_a * 2 * DA + heads_b * 2 * DB), jnp.bfloat16),
        in_specs=[vmem, pl.BlockSpec(memory_space=pl.ANY), vmem, vmem, vmem],
        out_specs=vmem,
        scratch_shapes=[
            pltpu.VMEM((chips * CORES, rows, width), own.dtype),
            pltpu.VMEM((2 * (heads_a + heads_b), rows, 1), jnp.float32),
            pltpu.VMEM((2 * (heads_a + heads_b), rows, 1), jnp.float32),
            pltpu.VMEM((2 * heads_a, rows, 2 * DA), jnp.float32),
            pltpu.VMEM((2 * heads_b, rows, 2 * DB), jnp.float32),
            pltpu.SemaphoreType.DMA,
            pltpu.SemaphoreType.DMA((chips,)),
            pltpu.SemaphoreType.DMA((chips,)),
            pltpu.SemaphoreType.DMA((chips * CORES,)),
        ],
        compiler_params=pltpu.CompilerParams(
            collective_id=3, has_side_effects=True, vmem_limit_bytes=VMEM_BYTES
        ),
    )(queries, own, lambdas, gain_a, gain_b)


def pivots_of(chips, slices):
    return [1, chips - 2, 0, chips - 2] if slices == chips == 4 else None


def sliced_kernel(
    chips, tps, heads_a, heads_b, pivots,
    q_ref, own_ref, lambda_ref, gain_a_ref, gain_b_ref, out_ref,
    kvs, qs, accum, top, total, o_out, o_all,
    load_sem, q_send, q_recv, dn_send, up_send, kv_recv, side_send, o_send, o_recv,
):
    chip, core, tp = place()
    rows = out_ref.shape[0]
    slices = len(pivots)
    key_width = 2 * DA
    me = chip * CORES + core

    def pivot(number):
        if isinstance(number, int):
            return pivots[number]
        return sum(jnp.where(number == n, pivots[n], 0) for n in range(slices))

    loads = []
    for number in range(slices):
        if number < heads_a:
            head, stride, q_at, k_at = number, heads_a * DA, 0, 0
        else:
            head, stride = number - heads_a, heads_b * DB
            q_at, k_at = 2 * heads_a * DA, 4 * heads_a * DA
        v_at = k_at + 2 * stride + head * 2 * DA
        moves = []
        for pair in range(2):
            at = pair * stride + head * DA
            spot = pl.ds(pair * DA, DA)
            moves.append((q_ref.at[:, pl.ds(q_at + at, DA)], qs.at[chip, number, :, spot]))
            moves.append((own_ref.at[:, pl.ds(k_at + at, DA)], kvs.at[me, number, :, spot]))
        moves.append(
            (own_ref.at[:, pl.ds(v_at, 2 * DA)], kvs.at[me, number, :, pl.ds(key_width, 2 * DA)])
        )
        loads.append([
            pltpu.make_async_copy(src, dst, load_sem.at[number, place_in])
            for place_in, (src, dst) in enumerate(moves)
        ])
    order = sorted(range(slices), key=lambda n: pivots[n])
    for number in order:
        for copy in loads[number]:
            copy.start()
    greet(chips, 1)

    def remote(src, dst, send, recv, sp_to):
        return pltpu.make_async_remote_copy(
            src_ref=src, dst_ref=dst, send_sem=send, recv_sem=recv,
            device_id={"sp": sp_to, "tp": tp}, device_id_type=MESH,
        )

    def send_q(number):
        ref = qs.at[chip, number]
        return remote(ref, ref, q_send.at[number], q_recv.at[chip, number],
                      pivot(number) * CORES + core)

    def send_kv(number, chip_to, sem):
        ref = kvs.at[me, number]
        return remote(ref, ref, sem, kv_recv.at[me, number], chip_to * CORES + core)

    def send_dn(number):
        return send_kv(number, pivot(number), dn_send.at[number])

    def send_up(number, step):
        return send_kv(number, chip + step, up_send.at[number, step - 1])

    def send_side(chip_of, number):
        ref = kvs.at[chip_of * CORES + core, number]
        return remote(ref, ref, side_send.at[chip_of, number],
                      kv_recv.at[chip_of * CORES + core, number], chip * CORES + 1 - core)

    def send_out(query, number):
        return remote(o_out.at[query, number], o_all.at[number], o_send.at[query, number],
                      o_recv.at[number], query * CORES + core)

    def arrived(ref, sem):
        pltpu.make_async_copy(ref, ref, sem).wait()

    for number in order:
        for copy in loads[number]:
            copy.wait()

        @pl.when(chip > pivots[number])
        def _():
            send_q(number).start()

        @pl.when(chip <= pivots[number])
        def _():
            send_side(chip, number).start()

    for number in reversed(order):
        @pl.when(chip > pivots[number])
        def _():
            send_dn(number).start()

    for step in reversed(range(1, chips)):
        for number in order:
            @pl.when(chip + step <= pivots[number])
            def _():
                send_up(number, step).start()

    ahead = lax.broadcasted_iota(jnp.int32, (rows, rows), 0) - lax.broadcasted_iota(
        jnp.int32, (rows, rows), 1
    )
    low_half = lax.broadcasted_iota(jnp.int32, (rows, DA), 1) < DB

    def step_one(query, number, slot, q, kv_chip, pair, v_at, wide, acc_at, size, masked):
        tiles = []
        for side in range(CORES):
            key = kvs[kv_chip * CORES + side, number, :, pair * DA : (pair + 1) * DA]
            scores = lax.dot_general(
                q, key, (((1,), (1,)), ((), ())), preferred_element_type=jnp.float32
            )
            if masked:
                scores = jnp.where(ahead + (core - side) * rows >= 0, scores, -1e30)
            tiles.append(scores)
        before = top[query, number, slot]
        after = jnp.maximum(
            before, jnp.max(jnp.maximum(tiles[0], tiles[1]), -1, keepdims=True)
        )
        factor = size ** (-0.5) * LOG2E
        terms = [jnp.exp2((scores - after) * factor) for scores in tiles]
        rescale = jnp.exp2((before - after) * factor)
        top[query, number, slot] = after
        total[query, number, slot] = total[query, number, slot] * rescale + jnp.sum(
            terms[0] + terms[1], -1, keepdims=True
        )
        fresh = sum(
            jnp.dot(
                terms[side].astype(jnp.bfloat16),
                kvs[kv_chip * CORES + side, number, :, v_at : v_at + wide],
                preferred_element_type=jnp.float32,
            )
            for side in range(CORES)
        )
        span = slice(acc_at, acc_at + wide)
        accum[query, number, pair, :, span] = accum[query, number, pair, :, span] * rescale + fresh

    def flash_a(query, kv_chip, number, masked):
        for pair in range(2):
            step_one(query, number, pair, qs[query, number, :, pair * DA : (pair + 1) * DA],
                     kv_chip, pair, key_width, 2 * DA, 0, DA, masked)

    def flash_b(query, kv_chip, number, masked):
        for pair in range(2):
            both = qs[query, number, :, pair * DA : (pair + 1) * DA]
            for head in range(2):
                keep = low_half if head == 0 else jnp.logical_not(low_half)
                q = jnp.where(keep, both, jnp.zeros_like(both))
                step_one(query, number, pair * 2 + head, q, kv_chip, pair,
                         key_width + head * 2 * DB, 2 * DB, head * 2 * DB, DB, masked)

    def relevant(query, number):
        return jnp.where(query == chip, pivot(number) >= chip, pivot(number) == chip)

    def over(body):
        def run_a(number, carry):
            body(number, flash_a)
            return carry

        def run_b(number, carry):
            body(number, flash_b)
            return carry

        lax.fori_loop(0, heads_a, run_a, 0)
        lax.fori_loop(heads_a, slices, run_b, 0)

    def pair_up(query, kv_chip, first):
        def body(number, flash):
            @pl.when(relevant(query, number))
            def _():
                @pl.when(first)
                def _():
                    top[query, number] = jnp.full(top.shape[2:], -1e30, jnp.float32)
                    total[query, number] = jnp.zeros(total.shape[2:], jnp.float32)
                    accum[query, number] = jnp.zeros(accum.shape[2:], jnp.float32)

                @pl.when(query == kv_chip)
                def _():
                    flash(query, kv_chip, number, True)

                @pl.when(query != kv_chip)
                def _():
                    flash(query, kv_chip, number, False)

        over(body)

    def mix(query, number, slots, spans, lam, gain_ref):
        mixture = (
            accum[query, number, 0, :, spans] / total[query, number, slots[0]]
            - lam * accum[query, number, 1, :, spans] / total[query, number, slots[1]]
        )
        return rms_norm(mixture, gain_ref[...]).astype(jnp.bfloat16)

    def finish(query):
        def body(number, flash):
            @pl.when(relevant(query, number))
            def _():
                if flash is flash_a:
                    lam = lambda_ref[0, tp * heads_a + number]
                    made = [mix(query, number, (0, 1), slice(0, 2 * DA), lam, gain_a_ref)]
                else:
                    made = []
                    for head in range(2):
                        lam = lambda_ref[
                            0, tps * heads_a + tp * heads_b + (number - heads_a) * 2 + head
                        ]
                        made.append(
                            mix(query, number, (head, 2 + head),
                                slice(head * 2 * DB, (head + 1) * 2 * DB), lam, gain_b_ref)
                        )
                wide = 2 * DA // len(made)
                for place_in, values in enumerate(made):
                    span = slice(place_in * wide, (place_in + 1) * wide)

                    @pl.when(query == chip)
                    def _():
                        o_all[number, :, span] = values

                    @pl.when(query != chip)
                    def _():
                        o_out[query, number, :, span] = values

                @pl.when(query != chip)
                def _():
                    send_out(query, number).start()

        over(body)

    above = chips - 1 - chip

    def event(number_of, carry):
        is_own = number_of == 0
        is_query = (number_of > 0) & (number_of <= above)
        is_below = (number_of > above) & (number_of <= above + chip)
        is_above = number_of > above + chip
        source = jnp.where(
            number_of <= above,
            chip + number_of,
            jnp.where(is_below, chip - (number_of - above), number_of - above),
        )
        kv_chip = jnp.where(number_of <= above, chip, source)
        low = jnp.where(is_below, chip, source)
        high = jnp.where(number_of <= above, source, chips - 1)

        def wait_q(number, carry):
            @pl.when(is_query & (pivot(number) == chip))
            def _():
                arrived(qs.at[source, number], q_recv.at[source, number])

            return carry

        def needs(number):
            return jnp.where(source > chip, pivot(number) == chip, pivot(number) >= chip)

        def wait_kv(number, carry):
            @pl.when((is_below | is_above) & needs(number))
            def _():
                index = source * CORES + core
                arrived(kvs.at[index, number], kv_recv.at[index, number])
                send_side(source, number).start()

            return carry

        def wait_side(number, carry):
            @pl.when((is_own | is_below | is_above) & needs(number))
            def _():
                index = source * CORES + 1 - core
                arrived(kvs.at[index, number], kv_recv.at[index, number])

            return carry

        lax.fori_loop(0, slices, wait_q, 0)
        lax.fori_loop(0, slices, wait_kv, 0)
        lax.fori_loop(0, slices, wait_side, 0)

        def queries(query, carry):
            pair_up(query, kv_chip, kv_chip == chip)

            @pl.when(
                ((query == chip) & (number_of == jnp.where(chip > 0, above + chip, 0)))
                | (is_above & (query == source))
            )
            def _():
                finish(query)

            return carry

        lax.fori_loop(low, high + 1, queries, 0)
        return carry

    lax.fori_loop(0, 1 + above + chips - 1, event, 0)

    for number in range(slices):
        @pl.when(chip > pivots[number])
        def _():
            arrived(o_all.at[number], o_recv.at[number])

        out_ref[:, number * 2 * DA : (number + 1) * 2 * DA] = o_all[number]

    for number in range(slices):
        @pl.when(chip > pivots[number])
        def _():
            send_q(number).wait_send()
            send_dn(number).wait_send()

        for step in range(1, chips):
            @pl.when(chip + step <= pivots[number])
            def _():
                send_up(number, step).wait_send()

        for chip_of in range(chips):
            @pl.when(jnp.where(chip_of > chip, pivots[number] == chip, pivots[number] >= chip))
            def _():
                send_side(chip_of, number).wait_send()

            @pl.when((chip_of > chip) & (pivots[number] == chip))
            def _():
                send_out(chip_of, number).wait_send()


def attend_sliced(queries, own, lambdas, gain_a, gain_b, chips, tps, heads_a, heads_b, pivots):
    rows = own.shape[0]
    slices = len(pivots)
    vmem = pl.BlockSpec(memory_space=pltpu.VMEM)
    any_space = pl.BlockSpec(memory_space=pl.ANY)
    dma = pltpu.SemaphoreType.DMA
    return pl.pallas_call(
        lambda *refs: sliced_kernel(chips, tps, heads_a, heads_b, pivots, *refs),
        name="attend_sliced",
        out_shape=jax.ShapeDtypeStruct((rows, slices * 2 * DA), jnp.bfloat16),
        in_specs=[any_space] * 2 + [pl.BlockSpec(memory_space=pltpu.SMEM), vmem, vmem],
        out_specs=vmem,
        scratch_shapes=[
            pltpu.VMEM((chips * CORES, slices, rows, 4 * DA), jnp.bfloat16),
            pltpu.VMEM((chips, slices, rows, 2 * DA), jnp.bfloat16),
            pltpu.VMEM((chips, slices, 2, rows, 2 * DA), jnp.float32),
            pltpu.VMEM((chips, slices, 4, rows, 1), jnp.float32),
            pltpu.VMEM((chips, slices, 4, rows, 1), jnp.float32),
            pltpu.VMEM((chips, slices, rows, 2 * DA), jnp.bfloat16),
            pltpu.VMEM((slices, rows, 2 * DA), jnp.bfloat16),
            dma((slices, 5)),
            dma((slices,)),
            dma((chips, slices)),
            dma((slices,)),
            dma((slices, chips - 1)),
            dma((chips * CORES, slices)),
            dma((chips, slices)),
            dma((chips, slices)),
            dma((slices,)),
        ],
        compiler_params=pltpu.CompilerParams(
            collective_id=6, has_side_effects=True, vmem_limit_bytes=VMEM_BYTES
        ),
    )(queries, own, lambdas, gain_a, gain_b)


def share_kernel(tps, part_ref, out_ref, arrived, send_sem, recv_sem):
    tp = lax.axis_index("tp")
    barrier = pltpu.get_barrier_semaphore()
    for step in range(1, tps):
        pl.semaphore_signal(barrier, inc=1, device_id={"tp": (tp + step) % tps}, device_id_type=MESH)
    pl.semaphore_wait(barrier, tps - 1)
    started = []
    for step in range(1, tps):
        other = (tp + step) % tps
        copy = pltpu.make_async_remote_copy(
            src_ref=part_ref.at[other], dst_ref=arrived.at[step - 1], send_sem=send_sem.at[step - 1],
            recv_sem=recv_sem.at[step - 1], device_id={"tp": other}, device_id_type=MESH,
        )
        copy.start()
        started.append(copy)
    rows = out_ref.shape[0]
    chunk = min(rows, 16)
    for step in range(1, tps):
        started[step - 1].wait()

        @pl.loop(0, rows // chunk)
        def _(part):
            span = pl.ds(pl.multiple_of(part * chunk, chunk), chunk)
            first = part_ref[tp, span, :].astype(jnp.float32) if step == 1 else out_ref[span, :]
            out_ref[span, :] = first + arrived[step - 1, span, :].astype(jnp.float32)


def share_rows(parts, tps):
    _, rows, width = parts.shape
    vmem = pl.BlockSpec(memory_space=pltpu.VMEM)
    return pl.pallas_call(
        lambda *refs: share_kernel(tps, *refs),
        name="share_rows",
        out_shape=jax.ShapeDtypeStruct((rows, width), jnp.float32),
        in_specs=[vmem],
        out_specs=vmem,
        scratch_shapes=[
            pltpu.VMEM((tps - 1, rows, width), parts.dtype),
            pltpu.SemaphoreType.DMA((tps - 1,)),
            pltpu.SemaphoreType.DMA((tps - 1,)),
        ],
        compiler_params=pltpu.CompilerParams(collective_id=4, has_side_effects=True),
    )(parts)


def spread_pairs(queries, heads):
    rows = queries.shape[0]
    pairs = queries.reshape(rows, 2 * heads // 2, 1, 2, DB)
    keep = jnp.eye(2, dtype=queries.dtype).reshape(1, 1, 2, 2, 1)
    return (pairs * keep).reshape(rows, 2 * heads * 2 * DB)


def expert_parts(gathered, expert, experts, capacity, width, weights):
    gate, up, down = weights
    blocks, rows, _ = gathered.shape
    shares = lax.dynamic_slice_in_dim(gathered[:, :, width:], expert, 1, 2)[:, :, 0]
    named = shares > 0
    order = jnp.arange(rows, dtype=jnp.int32)
    slots = jnp.dot(
        named.astype(jnp.bfloat16),
        (order[:, None] < order[None, :]).astype(jnp.bfloat16),
        preferred_element_type=jnp.float32,
    ).astype(jnp.int32)
    picks = (slots[:, None, :] == jnp.arange(capacity, dtype=jnp.int32)[None, :, None]) & named[:, None, :]
    rows_in = jnp.einsum(
        "bct,btd->bcd",
        picks.astype(jnp.bfloat16),
        gathered[:, :, :width],
        preferred_element_type=jnp.float32,
    ).astype(jnp.bfloat16)
    rows_in = rows_in.reshape(blocks * capacity, width)
    gate_pre = jnp.dot(rows_in, gate, preferred_element_type=jnp.float32)
    up_pre = jnp.dot(rows_in, up, preferred_element_type=jnp.float32)
    glu_part = jnp.minimum(gate_pre, 7.0)
    lin_part = jnp.clip(up_pre, -7.0, 7.0)
    hidden = (glu_part * jax.nn.sigmoid(1.702 * glu_part) * (lin_part + 1.0)).astype(jnp.bfloat16)
    outs = jnp.dot(hidden, down, preferred_element_type=jnp.float32).astype(jnp.bfloat16)
    back = jnp.where(picks, shares[:, None, :], 0).astype(jnp.bfloat16)
    return jnp.einsum(
        "bct,bcd->btd",
        back,
        outs.reshape(blocks, capacity, width),
        preferred_element_type=jnp.float32,
    ).astype(jnp.bfloat16)


def meet(chips, tps):
    chip, core, tp = place()
    barrier = pltpu.get_barrier_semaphore()
    others = 0
    for chip_step in range(chips):
        for core_step in range(CORES):
            for tp_step in range(tps):
                if chip_step + core_step + tp_step > 0:
                    others += 1
                    pl.semaphore_signal(
                        barrier,
                        inc=1,
                        device_id={
                            "sp": (chip + chip_step) % chips * CORES + (core + core_step) % CORES,
                            "tp": (tp + tp_step) % tps,
                        },
                        device_id_type=MESH,
                    )
    pl.semaphore_wait(barrier, others)


def group_at(chip, chips, step):
    near = jnp.minimum(chip, chips - 1 - chip)
    both = jnp.where(step % 2 == 1, chip - (step + 1) // 2, chip + step // 2)
    past = jnp.where(chip <= chips - 1 - chip, chip + step - near, chip - step + near)
    return jnp.where(step <= 2 * near, both, past)


def experts_kernel(
    chips, tps, capacity,
    heads_ref, out_a_ref, out_b_ref, residual_ref, gain_mix_ref, gain_pre_ref,
    meta_ref, gate_ref, up_ref, down_ref, gain_ref, out_ref,
    mixers, mix_out, mix_own, mix_in, base_ref, mix_send, mix_recv,
    rows_all, meta_all, gate, up, down, rows_in, hidden, outs, back, part, core_in, x_in, z_in,
    z_near, z_far, sums,
    load_sem, weight_sem, row_sem, meta_send, meta_recv, up_sem, dn_sem, x_sem, side_sem,
    core_send, core_recv, xs_send, xs_recv, zs_send, zs_recv,
    zn_send, zn_recv, zf_recv,
):
    chip, core, tp = place()
    experts = meta_ref.shape[0] // 2
    piece_rows, width = rows_all.shape[2], rows_all.shape[3]
    rows = piece_rows * CUTS
    ff = gate.shape[1]
    members = CORES * tps
    side_sp = chip * CORES + 1 - core

    def blk(chip_of, core_of, tp_of):
        return (chip_of * CORES + core_of) * tps + tp_of

    def remote(src, dst, send, recv, sp_to, tp_to):
        return pltpu.make_async_remote_copy(
            src_ref=src, dst_ref=dst, send_sem=send, recv_sem=recv,
            device_id={"sp": sp_to, "tp": tp_to}, device_id_type=MESH,
        )

    def rows_copy(block, piece, send, sp_to, tp_to):
        ref = rows_all.at[block, piece]
        return remote(ref, ref, send, row_sem.at[block, piece], sp_to, tp_to)

    def go_up(chip_of, piece):
        return rows_copy(blk(chip_of, core, tp), piece, up_sem.at[chip_of, piece],
                         (chip + 1) * CORES + core, tp)

    def go_dn(chip_of, piece):
        return rows_copy(blk(chip_of, core, tp), piece, dn_sem.at[chip_of, piece],
                         (chip - 1) * CORES + core, tp)

    def go_x(chip_of, step, piece):
        return rows_copy(blk(chip_of, core, tp), piece, x_sem.at[chip_of, step - 1, piece],
                         chip * CORES + core, (tp + step) % tps)

    def go_side(chip_of, tp_of, piece):
        return rows_copy(blk(chip_of, core, tp_of), piece, side_sem.at[chip_of, tp_of, piece],
                         side_sp, tp)

    def wait_rows(block, piece):
        ref = rows_all.at[block, piece]
        pltpu.make_async_copy(ref, ref, row_sem.at[block, piece]).wait()

    mine = blk(chip, core, tp)
    deep = out_a_ref.shape[0]
    loads = [
        pltpu.make_async_copy(src, mixers.at[number], load_sem.at[number])
        for number, src in enumerate((out_a_ref, out_b_ref))
    ]
    weights = [
        pltpu.make_async_copy(src, dst, weight_sem.at[number])
        for number, (src, dst) in enumerate(((gate_ref, gate), (up_ref, up), (down_ref, down)))
    ]
    for copy in loads + weights:
        copy.start()
    meta_all[mine] = meta_ref[...]
    meet(chips, tps)

    def meta_copy(number, chip_step, core_step, tp_step):
        return remote(
            meta_ref, meta_all.at[mine], meta_send.at[number], meta_recv.at[mine],
            (chip + chip_step) % chips * CORES + (core + core_step) % CORES, (tp + tp_step) % tps,
        )

    meta_steps = [
        (chip_step, core_step, tp_step)
        for chip_step in range(chips) for core_step in range(CORES) for tp_step in range(tps)
        if chip_step + core_step + tp_step > 0
    ]
    for number, steps in enumerate(meta_steps):
        meta_copy(number, *steps).start()

    def project(tp_of, store):
        wide = min(width, 512)
        span = pl.ds(pl.multiple_of(tp_of * rows, rows), rows)

        @pl.loop(0, width // wide)
        def _(number):
            cols = pl.ds(pl.multiple_of(number * wide, wide), wide)
            made = sum(
                jnp.dot(
                    heads_ref[span, half * deep : (half + 1) * deep], mixers[half, :, cols],
                    preferred_element_type=jnp.float32,
                )
                for half in range(2)
            )
            store(cols, made.astype(jnp.bfloat16).reshape(CUTS, piece_rows, wide))

    def mix_copy(step, piece):
        return remote(mix_out.at[step - 1, piece], mix_in.at[step - 1, piece],
                      mix_send.at[step - 1, piece], mix_recv.at[step - 1, piece],
                      chip * CORES + core, (tp + step) % tps)

    for copy in loads:
        copy.wait()
    for step in range(1, tps):
        def keep_other(cols, values):
            mix_out[step - 1, :, :, cols] = values

        project((tp + step) % tps, keep_other)
        for piece in range(CUTS):
            mix_copy(step, piece).start()

    def keep_own(cols, values):
        mix_own[:, :, cols] = values

    project(tp, keep_own)
    for piece in range(CUTS):
        for step in range(1, tps):
            ref = mix_in.at[step - 1, piece]
            pltpu.make_async_copy(ref, ref, mix_recv.at[step - 1, piece]).wait()

        @pl.loop(0, piece_rows // 16)
        def _(number):
            span = pl.ds(pl.multiple_of(number * 16, 16), 16)
            mixed = mix_own[piece, span, :].astype(jnp.float32)
            for step in range(1, tps):
                mixed = mixed + mix_in[step - 1, piece, span, :].astype(jnp.float32)
            after = (
                residual_ref[piece, span, :].astype(jnp.float32) + rms_norm(mixed, gain_mix_ref[...])
            ).astype(jnp.bfloat16)
            base_ref[piece, span, :] = after
            rows_all[mine, piece, span, :] = rms_norm(
                after.astype(jnp.float32), gain_pre_ref[...]
            ).astype(jnp.bfloat16)

        for step in range(1, tps):
            go_x(chip, step, piece).start()

        @pl.when(chip < chips - 1)
        def _():
            go_up(chip, piece).start()

        @pl.when(chip > 0)
        def _():
            go_dn(chip, piece).start()

        go_side(chip, tp, piece).start()

    def relay(chip_of, piece, upward):
        wait_rows(blk(chip_of, core, tp), piece)
        for step in range(1, tps):
            go_x(chip_of, step, piece).start()
        if upward:
            @pl.when(chip < chips - 1)
            def _():
                go_up(chip_of, piece).start()
        else:
            @pl.when(chip > 0)
            def _():
                go_dn(chip_of, piece).start()
        go_side(chip_of, tp, piece).start()

    def compute(group, between):
        order = lax.broadcasted_iota(jnp.int32, (rows, rows), 0).astype(jnp.float32)
        expert = chip * CORES + core
        between(0)
        for member in range(members):
            block = group * members + member
            slot = meta_all[block, pl.ds(expert, 1), :]
            share = meta_all[block, pl.ds(experts + expert, 1), :]
            hit = slot == order
            picks = jnp.where(hit[:capacity], 1.0, 0.0).astype(jnp.bfloat16)
            back[member] = jnp.where(hit, share, 0.0).T.astype(jnp.bfloat16)
            values = rows_all[block].reshape(rows, width)
            rows_in[member * capacity : (member + 1) * capacity, :] = jnp.dot(
                picks, values, preferred_element_type=jnp.float32
            ).astype(jnp.bfloat16)
        cut = min(ff, 512)
        wide = min(width, 512)
        split = min(CUTS // 2, ff // cut)

        @pl.loop(0, ff // cut)
        def _(number):
            @pl.when((number > 0) & (number < split))
            def _():
                between(number)

            cols = pl.ds(pl.multiple_of(number * cut, cut), cut)
            gate_pre = jnp.dot(rows_in[...], gate[:, cols], preferred_element_type=jnp.float32)
            up_pre = jnp.dot(rows_in[...], up[:, cols], preferred_element_type=jnp.float32)
            glu_part = jnp.minimum(gate_pre, 7.0)
            lin_part = jnp.clip(up_pre, -7.0, 7.0)
            hidden[:, cols] = (
                glu_part * jax.nn.sigmoid(1.702 * glu_part) * (lin_part + 1.0)
            ).astype(jnp.bfloat16)

        @pl.loop(0, width // wide)
        def _(number):
            @pl.when(number + split < CUTS)
            def _():
                between(number + split)

            cols = pl.ds(pl.multiple_of(number * wide, wide), wide)
            outs[:, cols] = jnp.dot(
                hidden[...], down[:, cols], preferred_element_type=jnp.float32
            ).astype(jnp.bfloat16)

        for piece in range(split + width // wide, CUTS):
            between(piece)

        @pl.loop(0, members)
        def _(member):
            span = pl.ds(pl.multiple_of(member * capacity, 16), capacity)
            spread = jnp.dot(
                back[member, :, :capacity], outs[span, :], preferred_element_type=jnp.float32
            ).astype(jnp.bfloat16)
            part[group * members + member] = spread.reshape(CUTS, piece_rows, width)

    def add(target, index, source, source_index):
        chunk = min(piece_rows, 16)

        @pl.loop(0, piece_rows // chunk)
        def _(number):
            span = pl.ds(pl.multiple_of(number * chunk, chunk), chunk)
            target[index + (span,)] = (
                target[index + (span,)].astype(jnp.float32)
                + source[source_index + (span,)].astype(jnp.float32)
            ).astype(target.dtype)

    def core_copy(group, tp_of, piece):
        return remote(part.at[blk(group, 1 - core, tp_of), piece], core_in.at[group, tp_of, piece],
                      core_send.at[group, tp_of, piece], core_recv.at[group, tp_of, piece],
                      side_sp, tp)

    def part_x(group, step, piece):
        return remote(part.at[blk(group, core, (tp + step) % tps), piece],
                      x_in.at[group, step - 1, piece], xs_send.at[group, step - 1, piece],
                      xs_recv.at[group, step - 1, piece], chip * CORES + core, (tp + step) % tps)

    def far_z(way, group, piece, last):
        dst, recv, chip_to = (
            (z_far.at[way, piece], zf_recv.at[way, piece], group) if last
            else (z_in.at[way, group, piece], zs_recv.at[way, group, piece], chip + 1 - 2 * way)
        )
        return remote(part.at[blk(group, core, tp), piece], dst, zs_send.at[way, group, piece], recv,
                      chip_to * CORES + core, tp)

    def near_z(way, step, piece):
        group = chip + 1 - 2 * way
        return remote(part.at[blk(group, core, (tp + step) % tps), piece],
                      z_near.at[way, step, piece], zn_send.at[way, step, piece],
                      zn_recv.at[way, step, piece], group * CORES + core, tp)

    def distance(way, group):
        return group - chip if way == 0 else chip - group

    def far(group):
        return (group - chip >= 2) | (chip - group >= 2)

    def go_far(way, group, piece):
        @pl.when(distance(way, group) == 2)
        def _():
            far_z(way, group, piece, True).start()

        @pl.when(distance(way, group) > 2)
        def _():
            far_z(way, group, piece, False).start()

    def arrived(ref, sem):
        pltpu.make_async_copy(ref, ref, sem).wait()

    steps_x = list(range(1, tps)) + [0]

    def hand_over(group):
        for step in steps_x:
            for piece in range(CUTS):
                core_copy(group, (tp + step) % tps, piece).start()

    def cross(group):
        for step in steps_x:
            tp_of = (tp + step) % tps
            for piece in range(CUTS):
                arrived(core_in.at[group, tp_of, piece], core_recv.at[group, tp_of, piece])
                add(part, (blk(group, core, tp_of), piece), core_in, (group, tp_of, piece))
                if step > 0:
                    @pl.when(far(group))
                    def _():
                        part_x(group, step, piece).start()

                for way in range(2):
                    @pl.when(distance(way, group) == 1)
                    def _():
                        near_z(way, step, piece).start()

    def settle(group):
        @pl.when(far(group))
        def _():
            for piece in range(CUTS):
                for step in range(1, tps):
                    arrived(x_in.at[group, step - 1, piece], xs_recv.at[group, step - 1, piece])
                    add(part, (blk(group, core, tp), piece), x_in, (group, step - 1, piece))

                @pl.when((chip == 0) & (group > 0))
                def _():
                    go_far(0, group, piece)

                @pl.when((chip == chips - 1) & (group < chips - 1))
                def _():
                    go_far(1, group, piece)

    def relays(step, piece):
        @pl.when((step < chips) & (chip - step >= 0))
        def _():
            relay(chip - step, piece, True)

        @pl.when((step < chips) & (chip + step < chips))
        def _():
            relay(chip + step, piece, False)

    def wave(step, carry):
        group = group_at(chip, chips, step - 1)
        for piece in range(CUTS):
            for tp_step in range(1, tps):
                tp_of = (tp + tp_step) % tps
                wait_rows(blk(group, core, tp_of), piece)
                go_side(group, tp_of, piece).start()

        @pl.when(step == 1)
        def _():
            for steps in meta_steps:
                block = blk((chip + steps[0]) % chips, (core + steps[1]) % CORES, (tp + steps[2]) % tps)
                arrived(meta_all.at[block], meta_recv.at[block])
            for copy in weights:
                copy.wait()

        for piece in range(CUTS):
            for tp_of in range(tps):
                wait_rows(blk(group, 1 - core, tp_of), piece)
        compute(group, lambda piece: relays(step + 1, piece))
        hand_over(group)
        before = group_at(chip, chips, step - 2)

        @pl.when((step > 1) & jnp.logical_not(far(before)))
        def _():
            cross(before)

        @pl.when(far(group) | (step == chips))
        def _():
            cross(group)

        @pl.when((step > 1) & far(before))
        def _():
            settle(before)

        return carry

    for piece in range(CUTS):
        relays(1, piece)
    lax.fori_loop(1, chips + 1, wave, 0)
    for piece in range(CUTS):
        for step in range(1, tps):
            for way in range(2):
                @pl.when(chip > 0 if way == 0 else chip < chips - 1)
                def _():
                    arrived(z_near.at[way, step, piece], zn_recv.at[way, step, piece])
                    add(part, (blk(chip, core, (tp + step) % tps), piece), z_near,
                        (way, step, piece))

            part_x(chip, step, piece).start()

    settle(group_at(chip, chips, chips - 1))

    def chain(number, carry):
        for way in range(2):
            group = number if way == 0 else chips - 1 - number
            starts = chip == 0 if way == 0 else chip == chips - 1

            @pl.when((distance(way, group) >= 2) & jnp.logical_not(starts))
            def _():
                for piece in range(CUTS):
                    arrived(z_in.at[way, group, piece], zs_recv.at[way, group, piece])
                    add(part, (blk(group, core, tp), piece), z_in, (way, group, piece))
                    go_far(way, group, piece)

        return carry

    lax.fori_loop(1, chips, chain, 0)

    chunk = min(piece_rows, 16)

    def each_chunk(body):
        @pl.loop(0, piece_rows // chunk)
        def _(number):
            body(pl.ds(pl.multiple_of(number * chunk, chunk), chunk))

    for piece in range(CUTS):
        for step in range(1, tps):
            arrived(x_in.at[chip, step - 1, piece], xs_recv.at[chip, step - 1, piece])

        def begin(span):
            start = part[mine, piece, span, :].astype(jnp.float32)
            for step in range(1, tps):
                start = start + x_in[chip, step - 1, piece, span, :].astype(jnp.float32)
            sums[span, :] = start

        each_chunk(begin)
        for way in range(2):
            def more(span):
                sums[span, :] = sums[span, :] + z_near[way, 0, piece, span, :].astype(jnp.float32)

            def most(span):
                sums[span, :] = sums[span, :] + z_far[way, piece, span, :].astype(jnp.float32)

            behind = chip if way == 0 else chips - 1 - chip

            @pl.when(behind > 0)
            def _():
                arrived(z_near.at[way, 0, piece], zn_recv.at[way, 0, piece])
                each_chunk(more)

            @pl.when(behind > 1)
            def _():
                arrived(z_far.at[way, piece], zf_recv.at[way, piece])
                each_chunk(most)

        def close(span):
            out_ref[piece, span, :] = (
                base_ref[piece, span, :].astype(jnp.float32) + rms_norm(sums[span, :], gain_ref[...])
            ).astype(out_ref.dtype)

        each_chunk(close)

    for number, steps in enumerate(meta_steps):
        meta_copy(number, *steps).wait_send()
    for piece in range(CUTS):
        for step in range(1, tps):
            mix_copy(step, piece).wait_send()

    def finish(group, carry):
        for piece in range(CUTS):
            for step in range(1, tps):
                go_x(group, step, piece).wait_send()

                @pl.when(far(group) | (group == chip))
                def _():
                    part_x(group, step, piece).wait_send()

            for tp_of in range(tps):
                go_side(group, tp_of, piece).wait_send()

            @pl.when((group <= chip) & (chip < chips - 1))
            def _():
                go_up(group, piece).wait_send()

            @pl.when((group >= chip) & (chip > 0))
            def _():
                go_dn(group, piece).wait_send()

            for way in range(2):
                @pl.when(distance(way, group) >= 2)
                def _():
                    far_z(way, group, piece, True).wait_send()

            for tp_of in range(tps):
                core_copy(group, tp_of, piece).wait_send()

        return carry

    lax.fori_loop(0, chips, finish, 0)
    for piece in range(CUTS):
        for step in range(tps):
            for way in range(2):
                @pl.when(chip < chips - 1 if way == 0 else chip > 0)
                def _():
                    near_z(way, step, piece).wait_send()


def experts_bytes(rows, width, ff, deep, chips, tps, capacity):
    blocks = chips * CORES * tps
    members = CORES * tps
    buffers = blocks * 2 + chips * (2 * tps - 1 + 2) + 2 * tps + 8
    return 2 * (
        rows * width * buffers + 3 * width * ff + members * capacity * (2 * width + ff) + 4 * rows * width
        + 2 * deep * (width + rows * tps) + (2 * tps + 1) * rows * width
    )


def run_experts(heads_out, mixers, residual, gains, meta, weights, chips, tps, capacity):
    rows, width = residual.shape
    gate, up, down = weights
    ff = gate.shape[1]
    blocks = chips * CORES * tps
    members = CORES * tps
    piece_rows = rows // CUTS
    vmem = pl.BlockSpec(memory_space=pltpu.VMEM)
    any_space = pl.BlockSpec(memory_space=pl.ANY)
    dma = pltpu.SemaphoreType.DMA
    bf16 = jnp.bfloat16
    return pl.pallas_call(
        lambda *refs: experts_kernel(chips, tps, capacity, *refs),
        name="run_experts",
        out_shape=jax.ShapeDtypeStruct((CUTS, piece_rows, width), bf16),
        in_specs=[vmem, any_space, any_space] + [vmem] * 4 + [any_space] * 3 + [vmem],
        out_specs=vmem,
        scratch_shapes=[
            pltpu.VMEM((2,) + mixers[0].shape, bf16),
            pltpu.VMEM((tps - 1, CUTS, piece_rows, width), bf16),
            pltpu.VMEM((CUTS, piece_rows, width), bf16),
            pltpu.VMEM((tps - 1, CUTS, piece_rows, width), bf16),
            pltpu.VMEM((CUTS, piece_rows, width), bf16),
            dma((tps - 1, CUTS)),
            dma((tps - 1, CUTS)),
            pltpu.VMEM((blocks, CUTS, piece_rows, width), bf16),
            pltpu.VMEM((blocks,) + meta.shape, meta.dtype),
            pltpu.VMEM(gate.shape, bf16),
            pltpu.VMEM(up.shape, bf16),
            pltpu.VMEM(down.shape, bf16),
            pltpu.VMEM((members * capacity, width), bf16),
            pltpu.VMEM((members * capacity, ff), bf16),
            pltpu.VMEM((members * capacity, width), bf16),
            pltpu.VMEM((members, rows, rows), bf16),
            pltpu.VMEM((blocks, CUTS, piece_rows, width), bf16),
            pltpu.VMEM((chips, tps, CUTS, piece_rows, width), bf16),
            pltpu.VMEM((chips, tps - 1, CUTS, piece_rows, width), bf16),
            pltpu.VMEM((2, chips, CUTS, piece_rows, width), bf16),
            pltpu.VMEM((2, tps, CUTS, piece_rows, width), bf16),
            pltpu.VMEM((2, CUTS, piece_rows, width), bf16),
            pltpu.VMEM((piece_rows, width), jnp.float32),
            dma((2,)),
            dma((3,)),
            dma((blocks, CUTS)),
            dma((blocks - 1,)),
            dma((blocks,)),
            dma((chips, CUTS)),
            dma((chips, CUTS)),
            dma((chips, tps - 1, CUTS)),
            dma((chips, tps, CUTS)),
            dma((chips, tps, CUTS)),
            dma((chips, tps, CUTS)),
            dma((chips, tps - 1, CUTS)),
            dma((chips, tps - 1, CUTS)),
            dma((2, chips, CUTS)),
            dma((2, chips, CUTS)),
            dma((2, tps, CUTS)),
            dma((2, tps, CUTS)),
            dma((2, CUTS)),
        ],
        compiler_params=pltpu.CompilerParams(
            collective_id=5, has_side_effects=True, vmem_limit_bytes=VMEM_BYTES
        ),
    )(
        heads_out, *mixers, residual.reshape(CUTS, piece_rows, width), gains[0], gains[1], meta, gate, up,
        down, gains[2],
    ).reshape(rows, width)


def slot_table(routes, route_weights, experts):
    rows = routes.shape[0]
    chosen = routes[None, :, :] == jnp.arange(experts, dtype=jnp.int32)[:, None, None]
    shares = jnp.sum(jnp.where(chosen, route_weights[None], 0.0), 2)
    named = jnp.any(chosen, 2)
    order = jnp.arange(rows, dtype=jnp.int32)
    slots = jnp.dot(
        named.astype(jnp.bfloat16),
        (order[:, None] < order[None, :]).astype(jnp.bfloat16),
        preferred_element_type=jnp.float32,
    )
    return jnp.concatenate([jnp.where(named, slots, -1.0), shares], 0)


def spread_experts(normed, routes, route_weights, seq_slot, experts, capacity, chips, tps, weights):
    width = normed.shape[1]
    extra = -(-experts // 128) * 128
    shares = jnp.sum(
        jnp.where(
            routes[:, :, None] == jnp.arange(extra, dtype=jnp.int32)[None, None, :],
            route_weights[:, :, None],
            0.0,
        ),
        1,
    ).astype(jnp.bfloat16)
    gathered = gather_rows(jnp.concatenate([normed, shares], 1), chips, tps)
    parts = expert_parts(gathered, seq_slot, experts, capacity, width, weights)
    return scatter_rows(parts, chips, tps)


def per_device(
    queries_a,
    keys_a,
    values_a,
    queries_b,
    keys_b,
    values_b,
    lambdas,
    head_gain_a,
    head_gain_b,
    out_a,
    out_b,
    residual,
    gain_mix,
    gain_pre,
    gain_post,
    routes,
    route_weights,
    expert_gate,
    expert_up,
    expert_down,
):
    length = queries_a.shape[0]
    heads_a = queries_a.shape[2] // DA
    heads_b = queries_b.shape[2] // DB
    head_slot = lax.axis_index("tp")
    seq_slot = lax.axis_index("sp")
    experts, tps = lax.axis_size("sp"), lax.axis_size("tp")
    chips = experts // CORES
    pivots = pivots_of(chips, heads_a + heads_b // 2)
    own = jnp.concatenate(
        [keys_a.reshape(length, -1), values_a, keys_b.reshape(length, -1), values_b], 1
    )
    if pivots is not None:
        heads_out = attend_sliced(
            jnp.concatenate([queries_a.reshape(length, -1), queries_b.reshape(length, -1)], 1),
            own, lambdas[None], head_gain_a[None], head_gain_b[None], chips, tps, heads_a, heads_b,
            pivots,
        )
    else:
        lambda_a = lax.dynamic_slice_in_dim(lambdas, head_slot * heads_a, heads_a)
        lambda_b = lax.dynamic_slice_in_dim(lambdas, HA + head_slot * heads_b, heads_b)
        queries = jnp.concatenate(
            [queries_a.reshape(length, -1), spread_pairs(queries_b, heads_b)], 1
        )
        heads_out = attend_blocks(
            queries,
            own,
            jnp.concatenate([lambda_a, lambda_b])[None],
            head_gain_a[None],
            head_gain_b[None],
            chips,
            heads_a,
            heads_b,
        )
    sub_rows = residual.shape[0]
    top_count = routes.shape[1]
    capacity = min(sub_rows, (5 * sub_rows * top_count + 4 * experts - 1) // (4 * experts))
    width = residual.shape[1]
    slots = -(-capacity // 16) * 16
    weights = (expert_gate[0], expert_up[0], expert_down[0])
    cut = heads_a * 2 * DA
    need = experts_bytes(sub_rows, width, weights[0].shape[1], cut, chips, tps, slots)
    if out_a.shape == out_b.shape and need < VMEM_BYTES:
        return run_experts(
            heads_out, (out_a, out_b), residual, (gain_mix[None], gain_pre[None], gain_post[None]),
            slot_table(routes, route_weights, experts), weights, chips, tps, slots,
        )
    mixed = (
        jnp.dot(heads_out[:, :cut], out_a, preferred_element_type=jnp.float32)
        + jnp.dot(heads_out[:, cut:], out_b, preferred_element_type=jnp.float32)
    ).astype(jnp.bfloat16)
    mixed_rows = share_rows(mixed.reshape(tps, length // tps, -1), tps)
    after_mix = (residual.astype(jnp.float32) + rms_norm(mixed_rows, gain_mix)).astype(jnp.bfloat16)
    normed = rms_norm(after_mix.astype(jnp.float32), gain_pre).astype(jnp.bfloat16)
    routed = spread_experts(
        normed, routes, route_weights, seq_slot, experts, capacity, chips, tps,
        weights,
    )
    return (after_mix.astype(jnp.float32) + rms_norm(routed, gain_post)).astype(jnp.bfloat16)


def solution(mesh):
    in_specs = (
        P(("grp", "sp"), None, "tp"),
        P(("grp", "sp"), None, "tp"),
        P(("grp", "sp"), "tp"),
        P(("grp", "sp"), None, "tp"),
        P(("grp", "sp"), None, "tp"),
        P(("grp", "sp"), "tp"),
        P(),
        P(),
        P(),
        P("tp", None),
        P("tp", None),
        P(("grp", "sp", "tp"), None),
        P(),
        P(),
        P(),
        P(("grp", "sp", "tp"), None),
        P(("grp", "sp", "tp"), None),
        P("sp", None, "tp"),
        P("sp", None, "tp"),
        P("sp", "tp", None),
    )
    out_specs = P(("grp", "sp", "tp"), None)
    return jax.shard_map(
        per_device, mesh=mesh, in_specs=in_specs, out_specs=out_specs, check_vma=False
    )
```

```python
import jax
import jax.numpy as jnp
from jax import lax
from jax.experimental import pallas as pl
from jax.experimental.pallas import tpu as pltpu
from jax.sharding import PartitionSpec as P

HA = 4
DA = 128
DB = 64


def rms_norm(values, gain_vec):
    return values * lax.rsqrt(jnp.mean(values * values, -1, keepdims=True) + 1e-06) * gain_vec


MESH = pl.DeviceIdType.MESH
CORES = 2
PIECES = 2
CUTS = 2
EARLY = ()
LOG2E = 1.4426950408889634
VMEM_BYTES = 60 * 1024 * 1024


def place():
    sp = lax.axis_index("sp")
    return sp // CORES, sp % CORES, lax.axis_index("tp")


def greet(chips, tps):
    chip, core, tp = place()
    barrier = pltpu.get_barrier_semaphore()
    for step in range(1, chips):
        other = (chip + step) % chips
        pl.semaphore_signal(
            barrier, inc=1, device_id={"sp": other * CORES + core, "tp": tp}, device_id_type=MESH
        )
    for step in range(1, tps):
        pl.semaphore_signal(
            barrier,
            inc=1,
            device_id={"sp": chip * CORES + core, "tp": (tp + step) % tps},
            device_id_type=MESH,
        )
    pl.semaphore_signal(
        barrier, inc=1, device_id={"sp": chip * CORES + 1 - core, "tp": tp}, device_id_type=MESH
    )
    pl.semaphore_wait(barrier, chips - 1 + tps - 1 + 1)


def gather_kernel(chips, tps, own_ref, all_ref, send_sem, recv_sem, own_sem):
    chip, core, tp = place()
    greet(chips, tps)
    started = []

    def block(chip_of, core_of, tp_of, piece):
        return ((chip_of * CORES + core_of) * tps + tp_of) * PIECES + piece

    def send(source, index, sp_to, tp_to):
        copy = pltpu.make_async_remote_copy(
            src_ref=source,
            dst_ref=all_ref.at[index],
            send_sem=send_sem.at[len(started)],
            recv_sem=recv_sem.at[index],
            device_id={"sp": sp_to, "tp": tp_to},
            device_id_type=MESH,
        )
        copy.start()
        started.append(copy)

    def arrived(index):
        pltpu.make_async_copy(all_ref.at[index], all_ref.at[index], recv_sem.at[index]).wait()

    for piece in range(PIECES):
        own = block(chip, core, tp, piece)
        for step in range(1, tps):
            send(own_ref.at[piece], own, chip * CORES + core, (tp + step) % tps)
        for step in range(1, chips):
            send(own_ref.at[piece], own, (chip + step) % chips * CORES + core, tp)
        send(own_ref.at[piece], own, chip * CORES + 1 - core, tp)
    mine = pltpu.make_async_copy(
        own_ref, all_ref.at[pl.ds(block(chip, core, tp, 0), PIECES)], own_sem
    )
    mine.start()

    def from_tp(chip_of, piece):
        for step in range(1, tps):
            index = block(chip_of, core, (tp + step) % tps, piece)
            arrived(index)
            send(all_ref.at[index], index, chip * CORES + 1 - core, tp)

    order = [(step, piece) for step in range(chips) for piece in range(PIECES)]
    for place_in, (step, piece) in enumerate(order):
        if step > 0:
            index = block((chip - step + chips) % chips, core, tp, piece)
            arrived(index)
            for tp_step in range(1, tps):
                send(all_ref.at[index], index, chip * CORES + core, (tp + tp_step) % tps)
            send(all_ref.at[index], index, chip * CORES + 1 - core, tp)
            done, done_piece = order[place_in - PIECES]
            from_tp((chip - done + chips) % chips, done_piece)
    for piece in range(PIECES):
        from_tp((chip + 1) % chips, piece)
    for step, piece in order:
        for tp_of in range(tps):
            arrived(block((chip - step + chips) % chips, 1 - core, (tp + tp_of) % tps, piece))
    mine.wait()
    for copy in started:
        copy.wait_send()


def gather_rows(own, chips, tps):
    blocks = chips * CORES * tps * PIECES
    sends = (chips - 1 + tps - 1 + 1 + (chips - 1) * tps + chips * (tps - 1)) * PIECES
    rows, width = own.shape
    own = own.reshape(PIECES, rows // PIECES, width)
    return pl.pallas_call(
        lambda *refs: gather_kernel(chips, tps, *refs),
        name="gather_rows",
        out_shape=jax.ShapeDtypeStruct((blocks,) + own.shape[1:], own.dtype),
        in_specs=[pl.BlockSpec(memory_space=pl.ANY)],
        out_specs=pl.BlockSpec(memory_space=pl.ANY),
        scratch_shapes=[
            pltpu.SemaphoreType.DMA((sends,)),
            pltpu.SemaphoreType.DMA((blocks,)),
            pltpu.SemaphoreType.DMA,
        ],
        compiler_params=pltpu.CompilerParams(collective_id=1, has_side_effects=True),
    )(own).reshape(-1, rows, width)


def add_rows(target, index, source, source_index):
    rows = target.shape[1]
    chunk = min(rows, 16)

    @pl.loop(0, rows // chunk)
    def _(part):
        span = pl.ds(pl.multiple_of(part * chunk, chunk), chunk)
        target[index, span, :] = (
            target[index, span, :].astype(jnp.float32)
            + source[source_index, span, :].astype(jnp.float32)
        ).astype(target.dtype)


def scatter_kernel(
    chips, tps, part_ref, out_ref, acc, core_in, tp_in, chip_in, load_sem, send_sem, core_sem, tp_sem, chip_sem
):
    chip, core, tp = place()
    load = []
    started = []
    order = [(step, piece) for step in range(chips) for piece in range(PIECES)]
    for step, piece in order:
        for tp_step in range(tps):
            chip_of, tp_of = (chip + 1 + step) % chips, (tp + 1 + tp_step) % tps
            copy = pltpu.make_async_copy(
                part_ref.at[((chip_of * CORES + core) * tps + tp_of) * PIECES + piece],
                acc.at[(chip_of * tps + tp_of) * PIECES + piece],
                load_sem.at[len(load)],
            )
            copy.start()
            load.append(copy)
    greet(chips, tps)

    def send(source, target, recv_sem, sp_to, tp_to):
        copy = pltpu.make_async_remote_copy(
            src_ref=source,
            dst_ref=target,
            send_sem=send_sem.at[len(started)],
            recv_sem=recv_sem,
            device_id={"sp": sp_to, "tp": tp_to},
            device_id_type=MESH,
        )
        copy.start()
        started.append(copy)

    def arrived(target, index, sem):
        pltpu.make_async_copy(target.at[index], target.at[index], sem).wait()

    for step, piece in order:
        chip_of = (chip + 1 + step) % chips
        for tp_step in range(tps):
            tp_of = (tp + 1 + tp_step) % tps
            index = (chip_of * tps + tp_of) * PIECES + piece
            send(
                part_ref.at[((chip_of * CORES + 1 - core) * tps + tp_of) * PIECES + piece],
                core_in.at[index],
                core_sem.at[index],
                chip * CORES + 1 - core,
                tp,
            )

    def chip_stage(step, piece):
        chip_of = (chip + 1 + step) % chips
        kept = (chip_of * tps + tp) * PIECES + piece
        for tp_step in range(1, tps):
            index = (chip_of * tps + (tp + tp_step) % tps) * PIECES + piece
            arrived(tp_in, index, tp_sem.at[index])
            add_rows(acc, kept, tp_in, index)
        if step < chips - 1:
            slot = chip * PIECES + piece
            send(acc.at[kept], chip_in.at[slot], chip_sem.at[slot], chip_of * CORES + core, tp)

    for number, (step, piece) in enumerate(order):
        chip_of = (chip + 1 + step) % chips
        for tp_step in range(tps):
            tp_of = (tp + 1 + tp_step) % tps
            index = (chip_of * tps + tp_of) * PIECES + piece
            load[number * tps + tp_step].wait()
            arrived(core_in, index, core_sem.at[index])
            add_rows(acc, index, core_in, index)
            if tp_step < tps - 1:
                slot = (chip_of * tps + tp) * PIECES + piece
                send(
                    acc.at[index], tp_in.at[slot], tp_sem.at[slot], chip * CORES + core, tp_of
                )
        if number > 0:
            chip_stage(*order[number - 1])
    chip_stage(*order[-1])
    rows = out_ref.shape[1]
    chunk = min(rows, 16)
    for step in range(1, chips):
        for piece in range(PIECES):
            source = (chip - step + chips) % chips * PIECES + piece
            kept = (chip * tps + tp) * PIECES + piece
            arrived(chip_in, source, chip_sem.at[source])
            if step < chips - 1:
                add_rows(acc, kept, chip_in, source)
            else:

                @pl.loop(0, rows // chunk)
                def _(part):
                    span = pl.ds(pl.multiple_of(part * chunk, chunk), chunk)
                    out_ref[piece, span, :] = acc[kept, span, :].astype(jnp.float32) + chip_in[
                        source, span, :
                    ].astype(jnp.float32)

    for copy in started:
        copy.wait_send()


def scatter_rows(parts, chips, tps):
    blocks, rows, width = parts.shape
    half = chips * tps * PIECES
    sends = half + (chips * (tps - 1) + chips - 1) * PIECES
    rows = rows // PIECES
    return pl.pallas_call(
        lambda *refs: scatter_kernel(chips, tps, *refs),
        name="scatter_rows",
        out_shape=jax.ShapeDtypeStruct((PIECES, rows, width), jnp.float32),
        in_specs=[pl.BlockSpec(memory_space=pl.ANY)],
        out_specs=pl.BlockSpec(memory_space=pltpu.VMEM),
        scratch_shapes=[
            pltpu.VMEM((half, rows, width), parts.dtype),
            pltpu.VMEM((half, rows, width), parts.dtype),
            pltpu.VMEM((half, rows, width), parts.dtype),
            pltpu.VMEM((chips * PIECES, rows, width), parts.dtype),
            pltpu.SemaphoreType.DMA((half,)),
            pltpu.SemaphoreType.DMA((sends,)),
            pltpu.SemaphoreType.DMA((half,)),
            pltpu.SemaphoreType.DMA((half,)),
            pltpu.SemaphoreType.DMA((chips * PIECES,)),
        ],
        compiler_params=pltpu.CompilerParams(
            collective_id=2, has_side_effects=True, vmem_limit_bytes=VMEM_BYTES
        ),
    )(parts.reshape(-1, rows, width)).reshape(PIECES * rows, width)


def attend_kernel(
    chips, heads_a, heads_b, query_ref, own_ref, lambda_ref, gain_a_ref, gain_b_ref, out_ref,
    held, top, total, accum_a, accum_b, own_sem, up_sem, side_sem, recv_sem,
):
    chip, core, tp = place()
    me = chip * CORES + core
    rows = own_ref.shape[0]
    mine = pltpu.make_async_copy(own_ref, held.at[me], own_sem)
    mine.start()
    barrier = pltpu.get_barrier_semaphore()

    def hello(sp_to):
        pl.semaphore_signal(barrier, inc=1, device_id={"sp": sp_to, "tp": tp}, device_id_type=MESH)

    hello(chip * CORES + 1 - core)

    @pl.when(chip > 0)
    def _():
        hello(me - CORES)

    @pl.when(chip < chips - 1)
    def _():
        hello(me + CORES)

    pl.semaphore_wait(
        barrier, 1 + jnp.where(chip > 0, 1, 0) + jnp.where(chip < chips - 1, 1, 0)
    )

    top[...] = jnp.full_like(top, -1e30)
    total[...] = jnp.zeros_like(total)
    accum_a[...] = jnp.zeros_like(accum_a)
    accum_b[...] = jnp.zeros_like(accum_b)
    mine.wait()

    def copy_up(back, index):
        return pltpu.make_async_remote_copy(
            src_ref=held.at[index], dst_ref=held.at[index], send_sem=up_sem.at[back],
            recv_sem=recv_sem.at[index], device_id={"sp": me + CORES, "tp": tp}, device_id_type=MESH,
        )

    def copy_side(back, index):
        return pltpu.make_async_remote_copy(
            src_ref=held.at[index], dst_ref=held.at[index], send_sem=side_sem.at[back],
            recv_sem=recv_sem.at[index], device_id={"sp": chip * CORES + 1 - core, "tp": tp},
            device_id_type=MESH,
        )

    base_va = 2 * heads_a * DA
    base_kb = base_va + heads_a * 2 * DA
    base_vb = base_kb + 2 * heads_b * DB
    base_qb = 2 * heads_a * DA
    ahead = lax.broadcasted_iota(jnp.int32, (rows, rows), 0) - lax.broadcasted_iota(
        jnp.int32, (rows, rows), 1
    )

    def flash(index):
        shown = ahead + (me - index) * rows >= 0

        def one(slot, query, key, value, accum, part, size):
            scores = lax.dot_general(
                query, key, (((1,), (1,)), ((), ())), preferred_element_type=jnp.float32
            )
            scores = jnp.where(shown, scores, -1e30)
            before = top[slot]
            after = jnp.maximum(before, jnp.max(scores, -1, keepdims=True))
            factor = size ** (-0.5) * LOG2E
            terms = jnp.exp2((scores - after) * factor)
            rescale = jnp.exp2((before - after) * factor)
            top[slot] = after
            total[slot] = total[slot] * rescale + jnp.sum(terms, -1, keepdims=True)
            accum[part] = accum[part] * rescale + jnp.dot(
                terms.astype(jnp.bfloat16), value, preferred_element_type=jnp.float32
            )

        for head in range(heads_a):
            value = held[index, :, base_va + head * 2 * DA : base_va + (head + 1) * 2 * DA]
            for pair in range(2):
                at = (pair * heads_a + head) * DA
                part = pair * heads_a + head
                one(
                    part, query_ref[:, at : at + DA], held[index, :, at : at + DA], value,
                    accum_a, part, DA,
                )
        for head in range(heads_b):
            value = held[index, :, base_vb + head * 2 * DB : base_vb + (head + 1) * 2 * DB]
            for pair in range(2):
                part = pair * heads_b + head
                at = base_qb + part * 2 * DB
                key_at = base_kb + part // 2 * 2 * DB
                one(
                    2 * heads_a + part, query_ref[:, at : at + 2 * DB],
                    held[index, :, key_at : key_at + 2 * DB], value, accum_b, part, DB,
                )

    def step(number, carry):
        back = number // 2
        side = number % 2
        source = chip - back

        @pl.when(source >= 0)
        def _():
            index = source * CORES + jnp.where(side == 0, core, 1 - core)

            @pl.when(number > 0)
            def _():
                pltpu.make_async_copy(held.at[index], held.at[index], recv_sem.at[index]).wait()

            @pl.when(side == 0)
            def _():
                @pl.when(chip < chips - 1)
                def _():
                    copy_up(back, index).start()

                copy_side(back, index).start()

            @pl.when(index <= me)
            def _():
                flash(index)

        return carry

    lax.fori_loop(0, 2 * chips, step, 0)

    def finish(head, parts, accum, slots, lam, gain_ref, at, wide):
        mixture = accum[parts[0]] / total[slots[0]] - lam * accum[parts[1]] / total[slots[1]]
        out_ref[:, at : at + wide] = rms_norm(mixture, gain_ref[...]).astype(out_ref.dtype)

    for head in range(heads_a):
        parts = (head, heads_a + head)
        finish(head, parts, accum_a, parts, lambda_ref[0:1, head : head + 1], gain_a_ref,
               head * 2 * DA, 2 * DA)
    for head in range(heads_b):
        parts = (head, heads_b + head)
        slots = (2 * heads_a + head, 2 * heads_a + heads_b + head)
        finish(head, parts, accum_b, slots, lambda_ref[0:1, heads_a + head : heads_a + head + 1],
               gain_b_ref, heads_a * 2 * DA + head * 2 * DB, 2 * DB)

    def settle(back, carry):
        @pl.when(chip - back >= 0)
        def _():
            index = (chip - back) * CORES + core

            @pl.when(chip < chips - 1)
            def _():
                copy_up(back, index).wait_send()

            copy_side(back, index).wait_send()

        return carry

    lax.fori_loop(0, chips, settle, 0)


def attend_blocks(queries, own, lambdas, gain_a, gain_b, chips, heads_a, heads_b):
    rows, width = own.shape
    vmem = pl.BlockSpec(memory_space=pltpu.VMEM)
    return pl.pallas_call(
        lambda *refs: attend_kernel(chips, heads_a, heads_b, *refs),
        name="attend_blocks",
        out_shape=jax.ShapeDtypeStruct((rows, heads_a * 2 * DA + heads_b * 2 * DB), jnp.bfloat16),
        in_specs=[vmem, pl.BlockSpec(memory_space=pl.ANY), vmem, vmem, vmem],
        out_specs=vmem,
        scratch_shapes=[
            pltpu.VMEM((chips * CORES, rows, width), own.dtype),
            pltpu.VMEM((2 * (heads_a + heads_b), rows, 1), jnp.float32),
            pltpu.VMEM((2 * (heads_a + heads_b), rows, 1), jnp.float32),
            pltpu.VMEM((2 * heads_a, rows, 2 * DA), jnp.float32),
            pltpu.VMEM((2 * heads_b, rows, 2 * DB), jnp.float32),
            pltpu.SemaphoreType.DMA,
            pltpu.SemaphoreType.DMA((chips,)),
            pltpu.SemaphoreType.DMA((chips,)),
            pltpu.SemaphoreType.DMA((chips * CORES,)),
        ],
        compiler_params=pltpu.CompilerParams(
            collective_id=3, has_side_effects=True, vmem_limit_bytes=VMEM_BYTES
        ),
    )(queries, own, lambdas, gain_a, gain_b)


def pivots_of(chips, slices):
    return [1, chips - 2, 0, chips - 2] if slices == chips == 4 else None


def sliced_kernel(
    chips, tps, heads_a, heads_b, pivots,
    q_ref, k_ref, va_ref, vb_ref, lambda_ref, gain_a_ref, gain_b_ref, out_ref,
    kvs, qs, accum, top, total, o_out, o_all,
    load_sem, q_send, q_recv, dn_send, up_send, kv_recv, side_send, o_send, o_recv,
):
    chip, core, tp = place()
    rows = out_ref.shape[0]
    slices = len(pivots)
    key_width = 2 * DA
    me = chip * CORES + core

    def pivot(number):
        if isinstance(number, int):
            return pivots[number]
        return sum(jnp.where(number == n, pivots[n], 0) for n in range(slices))

    loads = []
    for number in range(slices):
        if number < heads_a:
            head, stride, base, v_ref = number, heads_a * DA, 0, va_ref
        else:
            head, stride, base, v_ref = number - heads_a, heads_b * DB, 2 * heads_a * DA, vb_ref
        moves = []
        for pair in range(2):
            cols = pl.ds(base + pair * stride + head * DA, DA)
            spot = pl.ds(pair * DA, DA)
            moves.append((q_ref.at[:, cols], qs.at[chip, number, :, spot]))
            moves.append((k_ref.at[:, cols], kvs.at[me, number, :, spot]))
        moves.append(
            (v_ref.at[:, pl.ds(head * 2 * DA, 2 * DA)], kvs.at[me, number, :, pl.ds(key_width, 2 * DA)])
        )
        loads.append([
            pltpu.make_async_copy(src, dst, load_sem.at[number, place_in])
            for place_in, (src, dst) in enumerate(moves)
        ])
    order = sorted(range(slices), key=lambda n: pivots[n])
    for number in order:
        for copy in loads[number]:
            copy.start()
    greet(chips, 1)

    def remote(src, dst, send, recv, sp_to):
        return pltpu.make_async_remote_copy(
            src_ref=src, dst_ref=dst, send_sem=send, recv_sem=recv,
            device_id={"sp": sp_to, "tp": tp}, device_id_type=MESH,
        )

    def send_q(number):
        ref = qs.at[chip, number]
        return remote(ref, ref, q_send.at[number], q_recv.at[chip, number],
                      pivot(number) * CORES + core)

    def send_kv(number, chip_to, sem):
        ref = kvs.at[me, number]
        return remote(ref, ref, sem, kv_recv.at[me, number], chip_to * CORES + core)

    def send_dn(number):
        return send_kv(number, pivot(number), dn_send.at[number])

    def send_up(number, step):
        return send_kv(number, chip + step, up_send.at[number, step - 1])

    def send_side(chip_of, number):
        ref = kvs.at[chip_of * CORES + core, number]
        return remote(ref, ref, side_send.at[chip_of, number],
                      kv_recv.at[chip_of * CORES + core, number], chip * CORES + 1 - core)

    def send_out(query, number):
        return remote(o_out.at[query, number], o_all.at[number], o_send.at[query, number],
                      o_recv.at[number], query * CORES + core)

    def arrived(ref, sem):
        pltpu.make_async_copy(ref, ref, sem).wait()

    for number in order:
        for copy in loads[number]:
            copy.wait()

        @pl.when(chip > pivots[number])
        def _():
            send_q(number).start()

        @pl.when(chip <= pivots[number])
        def _():
            send_side(chip, number).start()

    for number in order:
        @pl.when(chip > pivots[number])
        def _():
            send_dn(number).start()

    for step in reversed(range(1, chips)):
        for number in order:
            @pl.when(chip + step <= pivots[number])
            def _():
                send_up(number, step).start()

    ahead = lax.broadcasted_iota(jnp.int32, (rows, rows), 0) - lax.broadcasted_iota(
        jnp.int32, (rows, rows), 1
    )
    low_half = lax.broadcasted_iota(jnp.int32, (rows, DA), 1) < DB

    def step_one(query, number, slot, q, kv_chip, pair, v_at, wide, acc_at, size, masked):
        tiles = []
        for side in range(CORES):
            key = kvs[kv_chip * CORES + side, number, :, pair * DA : (pair + 1) * DA]
            scores = lax.dot_general(
                q, key, (((1,), (1,)), ((), ())), preferred_element_type=jnp.float32
            )
            if masked:
                scores = jnp.where(ahead + (core - side) * rows >= 0, scores, -1e30)
            tiles.append(scores)
        before = top[query, number, slot]
        after = jnp.maximum(
            before, jnp.max(jnp.maximum(tiles[0], tiles[1]), -1, keepdims=True)
        )
        factor = size ** (-0.5) * LOG2E
        terms = [jnp.exp2((scores - after) * factor) for scores in tiles]
        rescale = jnp.exp2((before - after) * factor)
        top[query, number, slot] = after
        total[query, number, slot] = total[query, number, slot] * rescale + jnp.sum(
            terms[0] + terms[1], -1, keepdims=True
        )
        fresh = sum(
            jnp.dot(
                terms[side].astype(jnp.bfloat16),
                kvs[kv_chip * CORES + side, number, :, v_at : v_at + wide],
                preferred_element_type=jnp.float32,
            )
            for side in range(CORES)
        )
        span = slice(acc_at, acc_at + wide)
        accum[query, number, pair, :, span] = accum[query, number, pair, :, span] * rescale + fresh

    def flash_a(query, kv_chip, number, masked):
        for pair in range(2):
            step_one(query, number, pair, qs[query, number, :, pair * DA : (pair + 1) * DA],
                     kv_chip, pair, key_width, 2 * DA, 0, DA, masked)

    def flash_b(query, kv_chip, number, masked):
        for pair in range(2):
            both = qs[query, number, :, pair * DA : (pair + 1) * DA]
            for head in range(2):
                keep = low_half if head == 0 else jnp.logical_not(low_half)
                q = jnp.where(keep, both, jnp.zeros_like(both))
                step_one(query, number, pair * 2 + head, q, kv_chip, pair,
                         key_width + head * 2 * DB, 2 * DB, head * 2 * DB, DB, masked)

    def relevant(query, number):
        return jnp.where(query == chip, pivot(number) >= chip, pivot(number) == chip)

    def over(body):
        def run_a(number, carry):
            body(number, flash_a)
            return carry

        def run_b(number, carry):
            body(number, flash_b)
            return carry

        lax.fori_loop(0, heads_a, run_a, 0)
        lax.fori_loop(heads_a, slices, run_b, 0)

    def pair_up(query, kv_chip, first, number, flash):
        @pl.when(relevant(query, number))
        def _():
            @pl.when(first)
            def _():
                top[query, number] = jnp.full(top.shape[2:], -1e30, jnp.float32)
                total[query, number] = jnp.zeros(total.shape[2:], jnp.float32)
                accum[query, number] = jnp.zeros(accum.shape[2:], jnp.float32)

            @pl.when(query == kv_chip)
            def _():
                flash(query, kv_chip, number, True)

            @pl.when(query != kv_chip)
            def _():
                flash(query, kv_chip, number, False)

    def mix(query, number, slots, spans, lam, gain_ref):
        mixture = (
            accum[query, number, 0, :, spans] / total[query, number, slots[0]]
            - lam * accum[query, number, 1, :, spans] / total[query, number, slots[1]]
        )
        return rms_norm(mixture, gain_ref[...]).astype(jnp.bfloat16)

    def finish(query, number, flash):
        @pl.when(relevant(query, number))
        def _():
            if flash is flash_a:
                lam = lambda_ref[0, tp * heads_a + number]
                made = [mix(query, number, (0, 1), slice(0, 2 * DA), lam, gain_a_ref)]
            else:
                made = []
                for head in range(2):
                    lam = lambda_ref[
                        0, tps * heads_a + tp * heads_b + (number - heads_a) * 2 + head
                    ]
                    made.append(
                        mix(query, number, (head, 2 + head),
                            slice(head * 2 * DB, (head + 1) * 2 * DB), lam, gain_b_ref)
                    )
            wide = 2 * DA // len(made)
            for place_in, values in enumerate(made):
                span = slice(place_in * wide, (place_in + 1) * wide)

                @pl.when(query == chip)
                def _():
                    o_all[number, :, span] = values

                @pl.when(query != chip)
                def _():
                    o_out[query, number, :, span] = values

            @pl.when(query != chip)
            def _():
                send_out(query, number).start()

    above = chips - 1 - chip

    def event(number_of, carry):
        is_own = number_of == 0
        is_query = (number_of > 0) & (number_of <= above)
        is_below = (number_of > above) & (number_of <= above + chip)
        is_above = number_of > above + chip
        source = jnp.where(
            number_of <= above,
            chip + number_of,
            jnp.where(is_below, chip - (number_of - above), number_of - above),
        )
        kv_chip = jnp.where(number_of <= above, chip, source)
        low = jnp.where(is_below, chip, source)
        high = jnp.where(number_of <= above, source, chips - 1)

        def wait_q(number, carry):
            @pl.when(is_query & (pivot(number) == chip))
            def _():
                arrived(qs.at[source, number], q_recv.at[source, number])

            return carry

        def needs(number):
            return jnp.where(source > chip, pivot(number) == chip, pivot(number) >= chip)

        def wait_kv(number, carry):
            @pl.when((is_below | is_above) & needs(number))
            def _():
                index = source * CORES + core
                arrived(kvs.at[index, number], kv_recv.at[index, number])
                send_side(source, number).start()

            return carry

        def wait_side(number, carry):
            @pl.when((is_own | is_below | is_above) & needs(number))
            def _():
                index = source * CORES + 1 - core
                arrived(kvs.at[index, number], kv_recv.at[index, number])

            return carry

        def body(number, flash):
            wait_q(number, 0)
            wait_kv(number, 0)
            wait_side(number, 0)

            def queries(query, carry):
                pair_up(query, kv_chip, kv_chip == chip, number, flash)

                @pl.when(
                    ((query == chip) & (number_of == jnp.where(chip > 0, above + chip, 0)))
                    | (is_above & (query == source))
                )
                def _():
                    finish(query, number, flash)

                return carry

            lax.fori_loop(low, high + 1, queries, 0)

        over(body)
        return carry

    lax.fori_loop(0, 1 + above + chips - 1, event, 0)

    for number in range(slices):
        @pl.when(chip > pivots[number])
        def _():
            arrived(o_all.at[number], o_recv.at[number])

        out_ref[:, number * 2 * DA : (number + 1) * 2 * DA] = o_all[number]

    for number in range(slices):
        @pl.when(chip > pivots[number])
        def _():
            send_q(number).wait_send()
            send_dn(number).wait_send()

        for step in range(1, chips):
            @pl.when(chip + step <= pivots[number])
            def _():
                send_up(number, step).wait_send()

        for chip_of in range(chips):
            @pl.when(jnp.where(chip_of > chip, pivots[number] == chip, pivots[number] >= chip))
            def _():
                send_side(chip_of, number).wait_send()

            @pl.when((chip_of > chip) & (pivots[number] == chip))
            def _():
                send_out(chip_of, number).wait_send()


def attend_sliced(queries, keys, values, lambdas, gain_a, gain_b, chips, tps, heads_a, heads_b, pivots):
    rows = keys.shape[0]
    slices = len(pivots)
    vmem = pl.BlockSpec(memory_space=pltpu.VMEM)
    any_space = pl.BlockSpec(memory_space=pl.ANY)
    dma = pltpu.SemaphoreType.DMA
    return pl.pallas_call(
        lambda *refs: sliced_kernel(chips, tps, heads_a, heads_b, pivots, *refs),
        name="attend_sliced",
        out_shape=jax.ShapeDtypeStruct((rows, slices * 2 * DA), jnp.bfloat16),
        in_specs=[any_space] * 4 + [pl.BlockSpec(memory_space=pltpu.SMEM), vmem, vmem],
        out_specs=vmem,
        scratch_shapes=[
            pltpu.VMEM((chips * CORES, slices, rows, 4 * DA), jnp.bfloat16),
            pltpu.VMEM((chips, slices, rows, 2 * DA), jnp.bfloat16),
            pltpu.VMEM((chips, slices, 2, rows, 2 * DA), jnp.float32),
            pltpu.VMEM((chips, slices, 4, rows, 1), jnp.float32),
            pltpu.VMEM((chips, slices, 4, rows, 1), jnp.float32),
            pltpu.VMEM((chips, slices, rows, 2 * DA), jnp.bfloat16),
            pltpu.VMEM((slices, rows, 2 * DA), jnp.bfloat16),
            dma((slices, 5)),
            dma((slices,)),
            dma((chips, slices)),
            dma((slices,)),
            dma((slices, chips - 1)),
            dma((chips * CORES, slices)),
            dma((chips, slices)),
            dma((chips, slices)),
            dma((slices,)),
        ],
        compiler_params=pltpu.CompilerParams(
            collective_id=6, has_side_effects=True, vmem_limit_bytes=VMEM_BYTES
        ),
    )(queries, keys, *values, lambdas, gain_a, gain_b)


def share_kernel(tps, part_ref, out_ref, arrived, send_sem, recv_sem):
    tp = lax.axis_index("tp")
    barrier = pltpu.get_barrier_semaphore()
    for step in range(1, tps):
        pl.semaphore_signal(barrier, inc=1, device_id={"tp": (tp + step) % tps}, device_id_type=MESH)
    pl.semaphore_wait(barrier, tps - 1)
    started = []
    for step in range(1, tps):
        other = (tp + step) % tps
        copy = pltpu.make_async_remote_copy(
            src_ref=part_ref.at[other], dst_ref=arrived.at[step - 1], send_sem=send_sem.at[step - 1],
            recv_sem=recv_sem.at[step - 1], device_id={"tp": other}, device_id_type=MESH,
        )
        copy.start()
        started.append(copy)
    rows = out_ref.shape[0]
    chunk = min(rows, 16)
    for step in range(1, tps):
        started[step - 1].wait()

        @pl.loop(0, rows // chunk)
        def _(part):
            span = pl.ds(pl.multiple_of(part * chunk, chunk), chunk)
            first = part_ref[tp, span, :].astype(jnp.float32) if step == 1 else out_ref[span, :]
            out_ref[span, :] = first + arrived[step - 1, span, :].astype(jnp.float32)


def share_rows(parts, tps):
    _, rows, width = parts.shape
    vmem = pl.BlockSpec(memory_space=pltpu.VMEM)
    return pl.pallas_call(
        lambda *refs: share_kernel(tps, *refs),
        name="share_rows",
        out_shape=jax.ShapeDtypeStruct((rows, width), jnp.float32),
        in_specs=[vmem],
        out_specs=vmem,
        scratch_shapes=[
            pltpu.VMEM((tps - 1, rows, width), parts.dtype),
            pltpu.SemaphoreType.DMA((tps - 1,)),
            pltpu.SemaphoreType.DMA((tps - 1,)),
        ],
        compiler_params=pltpu.CompilerParams(collective_id=4, has_side_effects=True),
    )(parts)


def spread_pairs(queries, heads):
    rows = queries.shape[0]
    pairs = queries.reshape(rows, 2 * heads // 2, 1, 2, DB)
    keep = jnp.eye(2, dtype=queries.dtype).reshape(1, 1, 2, 2, 1)
    return (pairs * keep).reshape(rows, 2 * heads * 2 * DB)


def expert_parts(gathered, expert, experts, capacity, width, weights):
    gate, up, down = weights
    blocks, rows, _ = gathered.shape
    shares = lax.dynamic_slice_in_dim(gathered[:, :, width:], expert, 1, 2)[:, :, 0]
    named = shares > 0
    order = jnp.arange(rows, dtype=jnp.int32)
    slots = jnp.dot(
        named.astype(jnp.bfloat16),
        (order[:, None] < order[None, :]).astype(jnp.bfloat16),
        preferred_element_type=jnp.float32,
    ).astype(jnp.int32)
    picks = (slots[:, None, :] == jnp.arange(capacity, dtype=jnp.int32)[None, :, None]) & named[:, None, :]
    rows_in = jnp.einsum(
        "bct,btd->bcd",
        picks.astype(jnp.bfloat16),
        gathered[:, :, :width],
        preferred_element_type=jnp.float32,
    ).astype(jnp.bfloat16)
    rows_in = rows_in.reshape(blocks * capacity, width)
    gate_pre = jnp.dot(rows_in, gate, preferred_element_type=jnp.float32)
    up_pre = jnp.dot(rows_in, up, preferred_element_type=jnp.float32)
    glu_part = jnp.minimum(gate_pre, 7.0)
    lin_part = jnp.clip(up_pre, -7.0, 7.0)
    hidden = (glu_part * jax.nn.sigmoid(1.702 * glu_part) * (lin_part + 1.0)).astype(jnp.bfloat16)
    outs = jnp.dot(hidden, down, preferred_element_type=jnp.float32).astype(jnp.bfloat16)
    back = jnp.where(picks, shares[:, None, :], 0).astype(jnp.bfloat16)
    return jnp.einsum(
        "bct,bcd->btd",
        back,
        outs.reshape(blocks, capacity, width),
        preferred_element_type=jnp.float32,
    ).astype(jnp.bfloat16)


def meet(chips, tps):
    chip, core, tp = place()
    barrier = pltpu.get_barrier_semaphore()
    others = 0
    for chip_step in range(chips):
        for core_step in range(CORES):
            for tp_step in range(tps):
                if chip_step + core_step + tp_step > 0:
                    others += 1
                    pl.semaphore_signal(
                        barrier,
                        inc=1,
                        device_id={
                            "sp": (chip + chip_step) % chips * CORES + (core + core_step) % CORES,
                            "tp": (tp + tp_step) % tps,
                        },
                        device_id_type=MESH,
                    )
    pl.semaphore_wait(barrier, others)


def group_at(chip, chips, step):
    near = jnp.minimum(chip, chips - 1 - chip)
    both = jnp.where(step % 2 == 1, chip - (step + 1) // 2, chip + step // 2)
    past = jnp.where(chip <= chips - 1 - chip, chip + step - near, chip - step + near)
    return jnp.where(step <= 2 * near, both, past)


def experts_kernel(
    chips, tps, capacity,
    heads_ref, out_a_ref, out_b_ref, residual_ref, gain_mix_ref, gain_pre_ref,
    meta_ref, gate_ref, up_ref, down_ref, gain_ref, out_ref,
    mixers, mix_out, mix_own, mix_in, base_ref, mix_send, mix_recv,
    rows_all, meta_all, gate, up, down, rows_in, hidden, outs, back, part, core_in, x_in, z_in,
    z_near, z_far, sums,
    load_sem, weight_sem, row_sem, meta_send, meta_recv, up_sem, dn_sem, x_sem, side_sem,
    core_send, core_recv, xs_send, xs_recv, zs_send, zs_recv,
    zn_send, zn_recv, zf_recv,
):
    chip, core, tp = place()
    experts = meta_ref.shape[0] // 2
    piece_rows, width = rows_all.shape[2], rows_all.shape[3]
    rows = piece_rows * CUTS
    ff = gate.shape[1]
    members = CORES * tps
    side_sp = chip * CORES + 1 - core

    def blk(chip_of, core_of, tp_of):
        return (chip_of * CORES + core_of) * tps + tp_of

    def remote(src, dst, send, recv, sp_to, tp_to):
        return pltpu.make_async_remote_copy(
            src_ref=src, dst_ref=dst, send_sem=send, recv_sem=recv,
            device_id={"sp": sp_to, "tp": tp_to}, device_id_type=MESH,
        )

    def rows_copy(block, piece, send, sp_to, tp_to):
        ref = rows_all.at[block, piece]
        return remote(ref, ref, send, row_sem.at[block, piece], sp_to, tp_to)

    def go_up(chip_of, step, piece):
        return rows_copy(blk(chip_of, core, (tp + step) % tps), piece,
                         up_sem.at[chip_of, step, piece], (chip + 1) * CORES + core, tp)

    def go_dn(chip_of, step, piece):
        return rows_copy(blk(chip_of, core, (tp + step) % tps), piece,
                         dn_sem.at[chip_of, step, piece], (chip - 1) * CORES + core, tp)

    def go_on(chip_of, step, piece, upward, downward):
        if upward:
            @pl.when(chip < chips - 1)
            def _():
                go_up(chip_of, step, piece).start()

        if downward:
            @pl.when(chip > 0)
            def _():
                go_dn(chip_of, step, piece).start()

        go_side(chip_of, (tp + step) % tps, piece).start()

    def go_x(chip_of, step, piece):
        return rows_copy(blk(chip_of, core, tp), piece, x_sem.at[chip_of, step - 1, piece],
                         chip * CORES + core, (tp + step) % tps)

    def go_side(chip_of, tp_of, piece):
        return rows_copy(blk(chip_of, core, tp_of), piece, side_sem.at[chip_of, tp_of, piece],
                         side_sp, tp)

    def wait_rows(block, piece):
        ref = rows_all.at[block, piece]
        pltpu.make_async_copy(ref, ref, row_sem.at[block, piece]).wait()

    mine = blk(chip, core, tp)
    deep = out_a_ref.shape[0]
    loads = [
        pltpu.make_async_copy(src, mixers.at[number], load_sem.at[number])
        for number, src in enumerate((out_a_ref, out_b_ref))
    ]
    weights = [
        pltpu.make_async_copy(src, dst, weight_sem.at[number])
        for number, (src, dst) in enumerate(((gate_ref, gate), (up_ref, up), (down_ref, down)))
    ]
    for copy in loads + weights:
        copy.start()
    meta_all[mine] = meta_ref[...]
    meet(chips, tps)

    def meta_copy(number, chip_step, core_step, tp_step):
        return remote(
            meta_ref, meta_all.at[mine], meta_send.at[number], meta_recv.at[mine],
            (chip + chip_step) % chips * CORES + (core + core_step) % CORES, (tp + tp_step) % tps,
        )

    meta_steps = [
        (chip_step, core_step, tp_step)
        for chip_step in range(chips) for core_step in range(CORES) for tp_step in range(tps)
        if chip_step + core_step + tp_step > 0
    ]
    for number, steps in enumerate(meta_steps):
        meta_copy(number, *steps).start()

    def project(tp_of, store):
        wide = min(width, 512)
        span = pl.ds(pl.multiple_of(tp_of * rows, rows), rows)

        @pl.loop(0, width // wide)
        def _(number):
            cols = pl.ds(pl.multiple_of(number * wide, wide), wide)
            made = sum(
                jnp.dot(
                    heads_ref[span, half * deep : (half + 1) * deep], mixers[half, :, cols],
                    preferred_element_type=jnp.float32,
                )
                for half in range(2)
            )
            store(cols, made.astype(jnp.bfloat16).reshape(CUTS, piece_rows, wide))

    def mix_copy(step, piece):
        return remote(mix_out.at[step - 1, piece], mix_in.at[step - 1, piece],
                      mix_send.at[step - 1, piece], mix_recv.at[step - 1, piece],
                      chip * CORES + core, (tp + step) % tps)

    for copy in loads:
        copy.wait()
    for step in range(1, tps):
        def keep_other(cols, values):
            mix_out[step - 1, :, :, cols] = values

        project((tp + step) % tps, keep_other)
        for piece in range(CUTS):
            mix_copy(step, piece).start()

    def keep_own(cols, values):
        mix_own[:, :, cols] = values

    project(tp, keep_own)
    for piece in range(CUTS):
        for step in range(1, tps):
            ref = mix_in.at[step - 1, piece]
            pltpu.make_async_copy(ref, ref, mix_recv.at[step - 1, piece]).wait()

        @pl.loop(0, piece_rows // 16)
        def _(number):
            span = pl.ds(pl.multiple_of(number * 16, 16), 16)
            mixed = mix_own[piece, span, :].astype(jnp.float32)
            for step in range(1, tps):
                mixed = mixed + mix_in[step - 1, piece, span, :].astype(jnp.float32)
            after = (
                residual_ref[piece, span, :].astype(jnp.float32) + rms_norm(mixed, gain_mix_ref[...])
            ).astype(jnp.bfloat16)
            base_ref[piece, span, :] = after
            rows_all[mine, piece, span, :] = rms_norm(
                after.astype(jnp.float32), gain_pre_ref[...]
            ).astype(jnp.bfloat16)

        for step in range(1, tps):
            go_x(chip, step, piece).start()

        go_on(chip, 0, piece, True, True)

    for piece in EARLY:
        for step in range(1, tps):
            wait_rows(blk(chip, core, (tp + step) % tps), piece)
            go_on(chip, step, piece, True, True)

    def relay(chip_of, piece, upward):
        for step in range(tps if piece in EARLY else 1):
            wait_rows(blk(chip_of, core, (tp + step) % tps), piece)
            if piece not in EARLY:
                for tp_step in range(1, tps):
                    go_x(chip_of, tp_step, piece).start()
            go_on(chip_of, step, piece, upward, not upward)

    def compute(group, between):
        order = lax.broadcasted_iota(jnp.int32, (rows, rows), 0).astype(jnp.float32)
        expert = chip * CORES + core
        between(0)
        for member in range(members):
            block = group * members + member
            slot = meta_all[block, pl.ds(expert, 1), :]
            share = meta_all[block, pl.ds(experts + expert, 1), :]
            hit = slot == order
            picks = jnp.where(hit[:capacity], 1.0, 0.0).astype(jnp.bfloat16)
            back[member] = jnp.where(hit, share, 0.0).T.astype(jnp.bfloat16)
            values = rows_all[block].reshape(rows, width)
            rows_in[member * capacity : (member + 1) * capacity, :] = jnp.dot(
                picks, values, preferred_element_type=jnp.float32
            ).astype(jnp.bfloat16)
        cut = min(ff, 512)
        wide = min(width, 512)
        split = min(CUTS // 2, ff // cut)

        @pl.loop(0, ff // cut)
        def _(number):
            for piece in range(1, split):
                @pl.when(number == piece)
                def _():
                    between(piece)

            cols = pl.ds(pl.multiple_of(number * cut, cut), cut)
            gate_pre = jnp.dot(rows_in[...], gate[:, cols], preferred_element_type=jnp.float32)
            up_pre = jnp.dot(rows_in[...], up[:, cols], preferred_element_type=jnp.float32)
            glu_part = jnp.minimum(gate_pre, 7.0)
            lin_part = jnp.clip(up_pre, -7.0, 7.0)
            hidden[:, cols] = (
                glu_part * jax.nn.sigmoid(1.702 * glu_part) * (lin_part + 1.0)
            ).astype(jnp.bfloat16)

        @pl.loop(0, width // wide)
        def _(number):
            for piece in range(split, min(CUTS, split + width // wide)):
                @pl.when(number + split == piece)
                def _():
                    between(piece)

            cols = pl.ds(pl.multiple_of(number * wide, wide), wide)
            outs[:, cols] = jnp.dot(
                hidden[...], down[:, cols], preferred_element_type=jnp.float32
            ).astype(jnp.bfloat16)

        for piece in range(split + width // wide, CUTS):
            between(piece)

        @pl.loop(0, members)
        def _(member):
            span = pl.ds(pl.multiple_of(member * capacity, 16), capacity)
            spread = jnp.dot(
                back[member, :, :capacity], outs[span, :], preferred_element_type=jnp.float32
            ).astype(jnp.bfloat16)
            part[group * members + member] = spread.reshape(CUTS, piece_rows, width)

    def add(target, index, source, source_index):
        chunk = min(piece_rows, 16)

        @pl.loop(0, piece_rows // chunk)
        def _(number):
            span = pl.ds(pl.multiple_of(number * chunk, chunk), chunk)
            target[index + (span,)] = (
                target[index + (span,)].astype(jnp.float32)
                + source[source_index + (span,)].astype(jnp.float32)
            ).astype(target.dtype)

    def core_copy(group, tp_of, piece):
        return remote(part.at[blk(group, 1 - core, tp_of), piece], core_in.at[group, tp_of, piece],
                      core_send.at[group, tp_of, piece], core_recv.at[group, tp_of, piece],
                      side_sp, tp)

    def part_x(group, step, piece):
        return remote(part.at[blk(group, core, (tp + step) % tps), piece],
                      x_in.at[group, step - 1, piece], xs_send.at[group, step - 1, piece],
                      xs_recv.at[group, step - 1, piece], chip * CORES + core, (tp + step) % tps)

    def far_z(way, group, piece, last):
        dst, recv, chip_to = (
            (z_far.at[way, piece], zf_recv.at[way, piece], group) if last
            else (z_in.at[way, group, piece], zs_recv.at[way, group, piece], chip + 1 - 2 * way)
        )
        return remote(part.at[blk(group, core, tp), piece], dst, zs_send.at[way, group, piece], recv,
                      chip_to * CORES + core, tp)

    def near_z(way, step, piece):
        group = chip + 1 - 2 * way
        return remote(part.at[blk(group, core, (tp + step) % tps), piece],
                      z_near.at[way, step, piece], zn_send.at[way, step, piece],
                      zn_recv.at[way, step, piece], group * CORES + core, tp)

    def distance(way, group):
        return group - chip if way == 0 else chip - group

    def far(group):
        return (group - chip >= 2) | (chip - group >= 2)

    def go_far(way, group, piece):
        @pl.when(distance(way, group) == 2)
        def _():
            far_z(way, group, piece, True).start()

        @pl.when(distance(way, group) > 2)
        def _():
            far_z(way, group, piece, False).start()

    def arrived(ref, sem):
        pltpu.make_async_copy(ref, ref, sem).wait()

    steps_x = list(range(1, tps)) + [0]

    def hand_over(group):
        for step in steps_x:
            for piece in range(CUTS):
                core_copy(group, (tp + step) % tps, piece).start()

    def cross(group):
        for step in steps_x:
            tp_of = (tp + step) % tps
            for piece in range(CUTS):
                arrived(core_in.at[group, tp_of, piece], core_recv.at[group, tp_of, piece])
                add(part, (blk(group, core, tp_of), piece), core_in, (group, tp_of, piece))
                if step > 0:
                    @pl.when(far(group))
                    def _():
                        part_x(group, step, piece).start()

                for way in range(2):
                    @pl.when(distance(way, group) == 1)
                    def _():
                        near_z(way, step, piece).start()

    def settle(group):
        @pl.when(far(group))
        def _():
            for piece in range(CUTS):
                for step in range(1, tps):
                    arrived(x_in.at[group, step - 1, piece], xs_recv.at[group, step - 1, piece])
                    add(part, (blk(group, core, tp), piece), x_in, (group, step - 1, piece))

                @pl.when((chip == 0) & (group > 0))
                def _():
                    go_far(0, group, piece)

                @pl.when((chip == chips - 1) & (group < chips - 1))
                def _():
                    go_far(1, group, piece)

    def relays(step, piece):
        @pl.when((step < chips) & (chip - step >= 0))
        def _():
            relay(chip - step, piece, True)

        @pl.when((step < chips) & (chip + step < chips))
        def _():
            relay(chip + step, piece, False)

    def wave(step, carry):
        group = group_at(chip, chips, step - 1)
        for piece in range(CUTS):
            if piece not in EARLY:
                for tp_step in range(1, tps):
                    tp_of = (tp + tp_step) % tps
                    wait_rows(blk(group, core, tp_of), piece)
                    go_side(group, tp_of, piece).start()

        @pl.when(step == 1)
        def _():
            for steps in meta_steps:
                block = blk((chip + steps[0]) % chips, (core + steps[1]) % CORES, (tp + steps[2]) % tps)
                arrived(meta_all.at[block], meta_recv.at[block])
            for copy in weights:
                copy.wait()

        for piece in range(CUTS):
            for tp_of in range(tps):
                wait_rows(blk(group, 1 - core, tp_of), piece)
        compute(group, lambda piece: relays(step + 1, piece))
        hand_over(group)
        cross(group)
        before = group_at(chip, chips, step - 2)

        @pl.when((step > 1) & far(before))
        def _():
            settle(before)

        return carry

    for piece in range(CUTS):
        relays(1, piece)
    lax.fori_loop(1, chips + 1, wave, 0)
    for piece in range(CUTS):
        for step in range(1, tps):
            for way in range(2):
                @pl.when(chip > 0 if way == 0 else chip < chips - 1)
                def _():
                    arrived(z_near.at[way, step, piece], zn_recv.at[way, step, piece])
                    add(part, (blk(chip, core, (tp + step) % tps), piece), z_near,
                        (way, step, piece))

            part_x(chip, step, piece).start()

    settle(group_at(chip, chips, chips - 1))

    def chain(number, carry):
        for way in range(2):
            group = number if way == 0 else chips - 1 - number
            starts = chip == 0 if way == 0 else chip == chips - 1

            @pl.when((distance(way, group) >= 2) & jnp.logical_not(starts))
            def _():
                for piece in range(CUTS):
                    arrived(z_in.at[way, group, piece], zs_recv.at[way, group, piece])
                    add(part, (blk(group, core, tp), piece), z_in, (way, group, piece))
                    go_far(way, group, piece)

        return carry

    lax.fori_loop(1, chips, chain, 0)

    chunk = min(piece_rows, 16)

    def each_chunk(body):
        @pl.loop(0, piece_rows // chunk)
        def _(number):
            body(pl.ds(pl.multiple_of(number * chunk, chunk), chunk))

    for piece in range(CUTS):
        for step in range(1, tps):
            arrived(x_in.at[chip, step - 1, piece], xs_recv.at[chip, step - 1, piece])

        def begin(span):
            start = part[mine, piece, span, :].astype(jnp.float32)
            for step in range(1, tps):
                start = start + x_in[chip, step - 1, piece, span, :].astype(jnp.float32)
            sums[span, :] = start

        each_chunk(begin)
        for way in range(2):
            def more(span):
                sums[span, :] = sums[span, :] + z_near[way, 0, piece, span, :].astype(jnp.float32)

            def most(span):
                sums[span, :] = sums[span, :] + z_far[way, piece, span, :].astype(jnp.float32)

            behind = chip if way == 0 else chips - 1 - chip

            @pl.when(behind > 0)
            def _():
                arrived(z_near.at[way, 0, piece], zn_recv.at[way, 0, piece])
                each_chunk(more)

            @pl.when(behind > 1)
            def _():
                arrived(z_far.at[way, piece], zf_recv.at[way, piece])
                each_chunk(most)

        def close(span):
            out_ref[piece, span, :] = (
                base_ref[piece, span, :].astype(jnp.float32) + rms_norm(sums[span, :], gain_ref[...])
            ).astype(out_ref.dtype)

        each_chunk(close)

    for number, steps in enumerate(meta_steps):
        meta_copy(number, *steps).wait_send()
    for piece in range(CUTS):
        for step in range(1, tps):
            mix_copy(step, piece).wait_send()

    def finish(group, carry):
        for piece in range(CUTS):
            for step in range(1, tps):
                @pl.when((group == chip) | (piece not in EARLY))
                def _():
                    go_x(group, step, piece).wait_send()

                @pl.when(far(group) | (group == chip))
                def _():
                    part_x(group, step, piece).wait_send()

            for tp_of in range(tps):
                go_side(group, tp_of, piece).wait_send()

            for step in range(tps if piece in EARLY else 1):
                @pl.when((group <= chip) & (chip < chips - 1))
                def _():
                    go_up(group, step, piece).wait_send()

                @pl.when((group >= chip) & (chip > 0))
                def _():
                    go_dn(group, step, piece).wait_send()

            for way in range(2):
                @pl.when(distance(way, group) >= 2)
                def _():
                    far_z(way, group, piece, True).wait_send()

            for tp_of in range(tps):
                core_copy(group, tp_of, piece).wait_send()

        return carry

    lax.fori_loop(0, chips, finish, 0)
    for piece in range(CUTS):
        for step in range(tps):
            for way in range(2):
                @pl.when(chip < chips - 1 if way == 0 else chip > 0)
                def _():
                    near_z(way, step, piece).wait_send()


def experts_bytes(rows, width, ff, deep, chips, tps, capacity):
    blocks = chips * CORES * tps
    members = CORES * tps
    buffers = blocks * 2 + chips * (2 * tps - 1 + 2) + 2 * tps + 8
    return 2 * (
        rows * width * buffers + 3 * width * ff + members * capacity * (2 * width + ff) + 4 * rows * width
        + 2 * deep * (width + rows * tps) + (2 * tps + 1) * rows * width
    )


def run_experts(heads_out, mixers, residual, gains, meta, weights, chips, tps, capacity):
    rows, width = residual.shape
    gate, up, down = weights
    ff = gate.shape[1]
    blocks = chips * CORES * tps
    members = CORES * tps
    piece_rows = rows // CUTS
    vmem = pl.BlockSpec(memory_space=pltpu.VMEM)
    any_space = pl.BlockSpec(memory_space=pl.ANY)
    dma = pltpu.SemaphoreType.DMA
    bf16 = jnp.bfloat16
    return pl.pallas_call(
        lambda *refs: experts_kernel(chips, tps, capacity, *refs),
        name="run_experts",
        out_shape=jax.ShapeDtypeStruct((CUTS, piece_rows, width), bf16),
        in_specs=[vmem, any_space, any_space] + [vmem] * 4 + [any_space] * 3 + [vmem],
        out_specs=vmem,
        scratch_shapes=[
            pltpu.VMEM((2,) + mixers[0].shape, bf16),
            pltpu.VMEM((tps - 1, CUTS, piece_rows, width), bf16),
            pltpu.VMEM((CUTS, piece_rows, width), bf16),
            pltpu.VMEM((tps - 1, CUTS, piece_rows, width), bf16),
            pltpu.VMEM((CUTS, piece_rows, width), bf16),
            dma((tps - 1, CUTS)),
            dma((tps - 1, CUTS)),
            pltpu.VMEM((blocks, CUTS, piece_rows, width), bf16),
            pltpu.VMEM((blocks,) + meta.shape, meta.dtype),
            pltpu.VMEM(gate.shape, bf16),
            pltpu.VMEM(up.shape, bf16),
            pltpu.VMEM(down.shape, bf16),
            pltpu.VMEM((members * capacity, width), bf16),
            pltpu.VMEM((members * capacity, ff), bf16),
            pltpu.VMEM((members * capacity, width), bf16),
            pltpu.VMEM((members, rows, rows), bf16),
            pltpu.VMEM((blocks, CUTS, piece_rows, width), bf16),
            pltpu.VMEM((chips, tps, CUTS, piece_rows, width), bf16),
            pltpu.VMEM((chips, tps - 1, CUTS, piece_rows, width), bf16),
            pltpu.VMEM((2, chips, CUTS, piece_rows, width), bf16),
            pltpu.VMEM((2, tps, CUTS, piece_rows, width), bf16),
            pltpu.VMEM((2, CUTS, piece_rows, width), bf16),
            pltpu.VMEM((piece_rows, width), jnp.float32),
            dma((2,)),
            dma((3,)),
            dma((blocks, CUTS)),
            dma((blocks - 1,)),
            dma((blocks,)),
            dma((chips, tps, CUTS)),
            dma((chips, tps, CUTS)),
            dma((chips, tps - 1, CUTS)),
            dma((chips, tps, CUTS)),
            dma((chips, tps, CUTS)),
            dma((chips, tps, CUTS)),
            dma((chips, tps - 1, CUTS)),
            dma((chips, tps - 1, CUTS)),
            dma((2, chips, CUTS)),
            dma((2, chips, CUTS)),
            dma((2, tps, CUTS)),
            dma((2, tps, CUTS)),
            dma((2, CUTS)),
        ],
        compiler_params=pltpu.CompilerParams(
            collective_id=5, has_side_effects=True, vmem_limit_bytes=VMEM_BYTES
        ),
    )(
        heads_out, *mixers, residual.reshape(CUTS, piece_rows, width), gains[0], gains[1], meta, gate, up,
        down, gains[2],
    ).reshape(rows, width)


def slot_table(routes, route_weights, experts):
    rows = routes.shape[0]
    chosen = routes[None, :, :] == jnp.arange(experts, dtype=jnp.int32)[:, None, None]
    shares = jnp.sum(jnp.where(chosen, route_weights[None], 0.0), 2)
    named = jnp.any(chosen, 2)
    order = jnp.arange(rows, dtype=jnp.int32)
    slots = jnp.dot(
        named.astype(jnp.bfloat16),
        (order[:, None] < order[None, :]).astype(jnp.bfloat16),
        preferred_element_type=jnp.float32,
    )
    return jnp.concatenate([jnp.where(named, slots, -1.0), shares], 0)


def spread_experts(normed, routes, route_weights, seq_slot, experts, capacity, chips, tps, weights):
    width = normed.shape[1]
    extra = -(-experts // 128) * 128
    shares = jnp.sum(
        jnp.where(
            routes[:, :, None] == jnp.arange(extra, dtype=jnp.int32)[None, None, :],
            route_weights[:, :, None],
            0.0,
        ),
        1,
    ).astype(jnp.bfloat16)
    gathered = gather_rows(jnp.concatenate([normed, shares], 1), chips, tps)
    parts = expert_parts(gathered, seq_slot, experts, capacity, width, weights)
    return scatter_rows(parts, chips, tps)


def per_device(
    queries_a,
    keys_a,
    values_a,
    queries_b,
    keys_b,
    values_b,
    lambdas,
    head_gain_a,
    head_gain_b,
    out_a,
    out_b,
    residual,
    gain_mix,
    gain_pre,
    gain_post,
    routes,
    route_weights,
    expert_gate,
    expert_up,
    expert_down,
):
    length = queries_a.shape[0]
    heads_a = queries_a.shape[2] // DA
    heads_b = queries_b.shape[2] // DB
    head_slot = lax.axis_index("tp")
    seq_slot = lax.axis_index("sp")
    experts, tps = lax.axis_size("sp"), lax.axis_size("tp")
    chips = experts // CORES
    pivots = pivots_of(chips, heads_a + heads_b // 2)
    if pivots is not None:
        heads_out = attend_sliced(
            jnp.concatenate([queries_a.reshape(length, -1), queries_b.reshape(length, -1)], 1),
            jnp.concatenate([keys_a.reshape(length, -1), keys_b.reshape(length, -1)], 1),
            (values_a, values_b), lambdas[None], head_gain_a[None], head_gain_b[None], chips, tps,
            heads_a, heads_b, pivots,
        )
    else:
        lambda_a = lax.dynamic_slice_in_dim(lambdas, head_slot * heads_a, heads_a)
        lambda_b = lax.dynamic_slice_in_dim(lambdas, HA + head_slot * heads_b, heads_b)
        own = jnp.concatenate(
            [keys_a.reshape(length, -1), values_a, keys_b.reshape(length, -1), values_b], 1
        )
        queries = jnp.concatenate(
            [queries_a.reshape(length, -1), spread_pairs(queries_b, heads_b)], 1
        )
        heads_out = attend_blocks(
            queries,
            own,
            jnp.concatenate([lambda_a, lambda_b])[None],
            head_gain_a[None],
            head_gain_b[None],
            chips,
            heads_a,
            heads_b,
        )
    sub_rows = residual.shape[0]
    top_count = routes.shape[1]
    capacity = min(sub_rows, (5 * sub_rows * top_count + 4 * experts - 1) // (4 * experts))
    width = residual.shape[1]
    slots = -(-capacity // 16) * 16
    weights = (expert_gate[0], expert_up[0], expert_down[0])
    cut = heads_a * 2 * DA
    need = experts_bytes(sub_rows, width, weights[0].shape[1], cut, chips, tps, slots)
    if out_a.shape == out_b.shape and need < VMEM_BYTES:
        return run_experts(
            heads_out, (out_a, out_b), residual, (gain_mix[None], gain_pre[None], gain_post[None]),
            slot_table(routes, route_weights, experts), weights, chips, tps, slots,
        )
    mixed = (
        jnp.dot(heads_out[:, :cut], out_a, preferred_element_type=jnp.float32)
        + jnp.dot(heads_out[:, cut:], out_b, preferred_element_type=jnp.float32)
    ).astype(jnp.bfloat16)
    mixed_rows = share_rows(mixed.reshape(tps, length // tps, -1), tps)
    after_mix = (residual.astype(jnp.float32) + rms_norm(mixed_rows, gain_mix)).astype(jnp.bfloat16)
    normed = rms_norm(after_mix.astype(jnp.float32), gain_pre).astype(jnp.bfloat16)
    routed = spread_experts(
        normed, routes, route_weights, seq_slot, experts, capacity, chips, tps,
        weights,
    )
    return (after_mix.astype(jnp.float32) + rms_norm(routed, gain_post)).astype(jnp.bfloat16)


def solution(mesh):
    in_specs = (
        P(("grp", "sp"), None, "tp"),
        P(("grp", "sp"), None, "tp"),
        P(("grp", "sp"), "tp"),
        P(("grp", "sp"), None, "tp"),
        P(("grp", "sp"), None, "tp"),
        P(("grp", "sp"), "tp"),
        P(),
        P(),
        P(),
        P("tp", None),
        P("tp", None),
        P(("grp", "sp", "tp"), None),
        P(),
        P(),
        P(),
        P(("grp", "sp", "tp"), None),
        P(("grp", "sp", "tp"), None),
        P("sp", None, "tp"),
        P("sp", None, "tp"),
        P("sp", "tp", None),
    )
    out_specs = P(("grp", "sp", "tp"), None)
    return jax.shard_map(
        per_device, mesh=mesh, in_specs=in_specs, out_specs=out_specs, check_vma=False
    )
```

```python
import jax
import jax.numpy as jnp
from jax import lax
from jax.experimental import pallas as pl
from jax.experimental.pallas import tpu as pltpu
from jax.sharding import PartitionSpec as P

HA = 4
DA = 128
DB = 64


def rms_norm(values, gain_vec):
    return values * lax.rsqrt(jnp.mean(values * values, -1, keepdims=True) + 1e-06) * gain_vec


MESH = pl.DeviceIdType.MESH
CORES = 2
PIECES = 2
CUTS = 2
EARLY = ()
LOG2E = 1.4426950408889634
VMEM_BYTES = 60 * 1024 * 1024


def place():
    sp = lax.axis_index("sp")
    return sp // CORES, sp % CORES, lax.axis_index("tp")


def greet(chips, tps):
    chip, core, tp = place()
    barrier = pltpu.get_barrier_semaphore()
    for step in range(1, chips):
        other = (chip + step) % chips
        pl.semaphore_signal(
            barrier, inc=1, device_id={"sp": other * CORES + core, "tp": tp}, device_id_type=MESH
        )
    for step in range(1, tps):
        pl.semaphore_signal(
            barrier,
            inc=1,
            device_id={"sp": chip * CORES + core, "tp": (tp + step) % tps},
            device_id_type=MESH,
        )
    pl.semaphore_signal(
        barrier, inc=1, device_id={"sp": chip * CORES + 1 - core, "tp": tp}, device_id_type=MESH
    )
    pl.semaphore_wait(barrier, chips - 1 + tps - 1 + 1)


def gather_kernel(chips, tps, own_ref, all_ref, send_sem, recv_sem, own_sem):
    chip, core, tp = place()
    greet(chips, tps)
    started = []

    def block(chip_of, core_of, tp_of, piece):
        return ((chip_of * CORES + core_of) * tps + tp_of) * PIECES + piece

    def send(source, index, sp_to, tp_to):
        copy = pltpu.make_async_remote_copy(
            src_ref=source,
            dst_ref=all_ref.at[index],
            send_sem=send_sem.at[len(started)],
            recv_sem=recv_sem.at[index],
            device_id={"sp": sp_to, "tp": tp_to},
            device_id_type=MESH,
        )
        copy.start()
        started.append(copy)

    def arrived(index):
        pltpu.make_async_copy(all_ref.at[index], all_ref.at[index], recv_sem.at[index]).wait()

    for piece in range(PIECES):
        own = block(chip, core, tp, piece)
        for step in range(1, tps):
            send(own_ref.at[piece], own, chip * CORES + core, (tp + step) % tps)
        for step in range(1, chips):
            send(own_ref.at[piece], own, (chip + step) % chips * CORES + core, tp)
        send(own_ref.at[piece], own, chip * CORES + 1 - core, tp)
    mine = pltpu.make_async_copy(
        own_ref, all_ref.at[pl.ds(block(chip, core, tp, 0), PIECES)], own_sem
    )
    mine.start()

    def from_tp(chip_of, piece):
        for step in range(1, tps):
            index = block(chip_of, core, (tp + step) % tps, piece)
            arrived(index)
            send(all_ref.at[index], index, chip * CORES + 1 - core, tp)

    order = [(step, piece) for step in range(chips) for piece in range(PIECES)]
    for place_in, (step, piece) in enumerate(order):
        if step > 0:
            index = block((chip - step + chips) % chips, core, tp, piece)
            arrived(index)
            for tp_step in range(1, tps):
                send(all_ref.at[index], index, chip * CORES + core, (tp + tp_step) % tps)
            send(all_ref.at[index], index, chip * CORES + 1 - core, tp)
            done, done_piece = order[place_in - PIECES]
            from_tp((chip - done + chips) % chips, done_piece)
    for piece in range(PIECES):
        from_tp((chip + 1) % chips, piece)
    for step, piece in order:
        for tp_of in range(tps):
            arrived(block((chip - step + chips) % chips, 1 - core, (tp + tp_of) % tps, piece))
    mine.wait()
    for copy in started:
        copy.wait_send()


def gather_rows(own, chips, tps):
    blocks = chips * CORES * tps * PIECES
    sends = (chips - 1 + tps - 1 + 1 + (chips - 1) * tps + chips * (tps - 1)) * PIECES
    rows, width = own.shape
    own = own.reshape(PIECES, rows // PIECES, width)
    return pl.pallas_call(
        lambda *refs: gather_kernel(chips, tps, *refs),
        name="gather_rows",
        out_shape=jax.ShapeDtypeStruct((blocks,) + own.shape[1:], own.dtype),
        in_specs=[pl.BlockSpec(memory_space=pl.ANY)],
        out_specs=pl.BlockSpec(memory_space=pl.ANY),
        scratch_shapes=[
            pltpu.SemaphoreType.DMA((sends,)),
            pltpu.SemaphoreType.DMA((blocks,)),
            pltpu.SemaphoreType.DMA,
        ],
        compiler_params=pltpu.CompilerParams(collective_id=1, has_side_effects=True),
    )(own).reshape(-1, rows, width)


def add_rows(target, index, source, source_index):
    rows = target.shape[1]
    chunk = min(rows, 16)

    @pl.loop(0, rows // chunk)
    def _(part):
        span = pl.ds(pl.multiple_of(part * chunk, chunk), chunk)
        target[index, span, :] = (
            target[index, span, :].astype(jnp.float32)
            + source[source_index, span, :].astype(jnp.float32)
        ).astype(target.dtype)


def scatter_kernel(
    chips, tps, part_ref, out_ref, acc, core_in, tp_in, chip_in, load_sem, send_sem, core_sem, tp_sem, chip_sem
):
    chip, core, tp = place()
    load = []
    started = []
    order = [(step, piece) for step in range(chips) for piece in range(PIECES)]
    for step, piece in order:
        for tp_step in range(tps):
            chip_of, tp_of = (chip + 1 + step) % chips, (tp + 1 + tp_step) % tps
            copy = pltpu.make_async_copy(
                part_ref.at[((chip_of * CORES + core) * tps + tp_of) * PIECES + piece],
                acc.at[(chip_of * tps + tp_of) * PIECES + piece],
                load_sem.at[len(load)],
            )
            copy.start()
            load.append(copy)
    greet(chips, tps)

    def send(source, target, recv_sem, sp_to, tp_to):
        copy = pltpu.make_async_remote_copy(
            src_ref=source,
            dst_ref=target,
            send_sem=send_sem.at[len(started)],
            recv_sem=recv_sem,
            device_id={"sp": sp_to, "tp": tp_to},
            device_id_type=MESH,
        )
        copy.start()
        started.append(copy)

    def arrived(target, index, sem):
        pltpu.make_async_copy(target.at[index], target.at[index], sem).wait()

    for step, piece in order:
        chip_of = (chip + 1 + step) % chips
        for tp_step in range(tps):
            tp_of = (tp + 1 + tp_step) % tps
            index = (chip_of * tps + tp_of) * PIECES + piece
            send(
                part_ref.at[((chip_of * CORES + 1 - core) * tps + tp_of) * PIECES + piece],
                core_in.at[index],
                core_sem.at[index],
                chip * CORES + 1 - core,
                tp,
            )

    def chip_stage(step, piece):
        chip_of = (chip + 1 + step) % chips
        kept = (chip_of * tps + tp) * PIECES + piece
        for tp_step in range(1, tps):
            index = (chip_of * tps + (tp + tp_step) % tps) * PIECES + piece
            arrived(tp_in, index, tp_sem.at[index])
            add_rows(acc, kept, tp_in, index)
        if step < chips - 1:
            slot = chip * PIECES + piece
            send(acc.at[kept], chip_in.at[slot], chip_sem.at[slot], chip_of * CORES + core, tp)

    for number, (step, piece) in enumerate(order):
        chip_of = (chip + 1 + step) % chips
        for tp_step in range(tps):
            tp_of = (tp + 1 + tp_step) % tps
            index = (chip_of * tps + tp_of) * PIECES + piece
            load[number * tps + tp_step].wait()
            arrived(core_in, index, core_sem.at[index])
            add_rows(acc, index, core_in, index)
            if tp_step < tps - 1:
                slot = (chip_of * tps + tp) * PIECES + piece
                send(
                    acc.at[index], tp_in.at[slot], tp_sem.at[slot], chip * CORES + core, tp_of
                )
        if number > 0:
            chip_stage(*order[number - 1])
    chip_stage(*order[-1])
    rows = out_ref.shape[1]
    chunk = min(rows, 16)
    for step in range(1, chips):
        for piece in range(PIECES):
            source = (chip - step + chips) % chips * PIECES + piece
            kept = (chip * tps + tp) * PIECES + piece
            arrived(chip_in, source, chip_sem.at[source])
            if step < chips - 1:
                add_rows(acc, kept, chip_in, source)
            else:

                @pl.loop(0, rows // chunk)
                def _(part):
                    span = pl.ds(pl.multiple_of(part * chunk, chunk), chunk)
                    out_ref[piece, span, :] = acc[kept, span, :].astype(jnp.float32) + chip_in[
                        source, span, :
                    ].astype(jnp.float32)

    for copy in started:
        copy.wait_send()


def scatter_rows(parts, chips, tps):
    blocks, rows, width = parts.shape
    half = chips * tps * PIECES
    sends = half + (chips * (tps - 1) + chips - 1) * PIECES
    rows = rows // PIECES
    return pl.pallas_call(
        lambda *refs: scatter_kernel(chips, tps, *refs),
        name="scatter_rows",
        out_shape=jax.ShapeDtypeStruct((PIECES, rows, width), jnp.float32),
        in_specs=[pl.BlockSpec(memory_space=pl.ANY)],
        out_specs=pl.BlockSpec(memory_space=pltpu.VMEM),
        scratch_shapes=[
            pltpu.VMEM((half, rows, width), parts.dtype),
            pltpu.VMEM((half, rows, width), parts.dtype),
            pltpu.VMEM((half, rows, width), parts.dtype),
            pltpu.VMEM((chips * PIECES, rows, width), parts.dtype),
            pltpu.SemaphoreType.DMA((half,)),
            pltpu.SemaphoreType.DMA((sends,)),
            pltpu.SemaphoreType.DMA((half,)),
            pltpu.SemaphoreType.DMA((half,)),
            pltpu.SemaphoreType.DMA((chips * PIECES,)),
        ],
        compiler_params=pltpu.CompilerParams(
            collective_id=2, has_side_effects=True, vmem_limit_bytes=VMEM_BYTES
        ),
    )(parts.reshape(-1, rows, width)).reshape(PIECES * rows, width)


def attend_kernel(
    chips, heads_a, heads_b, query_ref, own_ref, lambda_ref, gain_a_ref, gain_b_ref, out_ref,
    held, top, total, accum_a, accum_b, own_sem, up_sem, side_sem, recv_sem,
):
    chip, core, tp = place()
    me = chip * CORES + core
    rows = own_ref.shape[0]
    mine = pltpu.make_async_copy(own_ref, held.at[me], own_sem)
    mine.start()
    barrier = pltpu.get_barrier_semaphore()

    def hello(sp_to):
        pl.semaphore_signal(barrier, inc=1, device_id={"sp": sp_to, "tp": tp}, device_id_type=MESH)

    hello(chip * CORES + 1 - core)

    @pl.when(chip > 0)
    def _():
        hello(me - CORES)

    @pl.when(chip < chips - 1)
    def _():
        hello(me + CORES)

    pl.semaphore_wait(
        barrier, 1 + jnp.where(chip > 0, 1, 0) + jnp.where(chip < chips - 1, 1, 0)
    )

    top[...] = jnp.full_like(top, -1e30)
    total[...] = jnp.zeros_like(total)
    accum_a[...] = jnp.zeros_like(accum_a)
    accum_b[...] = jnp.zeros_like(accum_b)
    mine.wait()

    def copy_up(back, index):
        return pltpu.make_async_remote_copy(
            src_ref=held.at[index], dst_ref=held.at[index], send_sem=up_sem.at[back],
            recv_sem=recv_sem.at[index], device_id={"sp": me + CORES, "tp": tp}, device_id_type=MESH,
        )

    def copy_side(back, index):
        return pltpu.make_async_remote_copy(
            src_ref=held.at[index], dst_ref=held.at[index], send_sem=side_sem.at[back],
            recv_sem=recv_sem.at[index], device_id={"sp": chip * CORES + 1 - core, "tp": tp},
            device_id_type=MESH,
        )

    base_va = 2 * heads_a * DA
    base_kb = base_va + heads_a * 2 * DA
    base_vb = base_kb + 2 * heads_b * DB
    base_qb = 2 * heads_a * DA
    ahead = lax.broadcasted_iota(jnp.int32, (rows, rows), 0) - lax.broadcasted_iota(
        jnp.int32, (rows, rows), 1
    )

    def flash(index):
        shown = ahead + (me - index) * rows >= 0

        def one(slot, query, key, value, accum, part, size):
            scores = lax.dot_general(
                query, key, (((1,), (1,)), ((), ())), preferred_element_type=jnp.float32
            )
            scores = jnp.where(shown, scores, -1e30)
            before = top[slot]
            after = jnp.maximum(before, jnp.max(scores, -1, keepdims=True))
            factor = size ** (-0.5) * LOG2E
            terms = jnp.exp2((scores - after) * factor)
            rescale = jnp.exp2((before - after) * factor)
            top[slot] = after
            total[slot] = total[slot] * rescale + jnp.sum(terms, -1, keepdims=True)
            accum[part] = accum[part] * rescale + jnp.dot(
                terms.astype(jnp.bfloat16), value, preferred_element_type=jnp.float32
            )

        for head in range(heads_a):
            value = held[index, :, base_va + head * 2 * DA : base_va + (head + 1) * 2 * DA]
            for pair in range(2):
                at = (pair * heads_a + head) * DA
                part = pair * heads_a + head
                one(
                    part, query_ref[:, at : at + DA], held[index, :, at : at + DA], value,
                    accum_a, part, DA,
                )
        for head in range(heads_b):
            value = held[index, :, base_vb + head * 2 * DB : base_vb + (head + 1) * 2 * DB]
            for pair in range(2):
                part = pair * heads_b + head
                at = base_qb + part * 2 * DB
                key_at = base_kb + part // 2 * 2 * DB
                one(
                    2 * heads_a + part, query_ref[:, at : at + 2 * DB],
                    held[index, :, key_at : key_at + 2 * DB], value, accum_b, part, DB,
                )

    def step(number, carry):
        back = number // 2
        side = number % 2
        source = chip - back

        @pl.when(source >= 0)
        def _():
            index = source * CORES + jnp.where(side == 0, core, 1 - core)

            @pl.when(number > 0)
            def _():
                pltpu.make_async_copy(held.at[index], held.at[index], recv_sem.at[index]).wait()

            @pl.when(side == 0)
            def _():
                @pl.when(chip < chips - 1)
                def _():
                    copy_up(back, index).start()

                copy_side(back, index).start()

            @pl.when(index <= me)
            def _():
                flash(index)

        return carry

    lax.fori_loop(0, 2 * chips, step, 0)

    def finish(head, parts, accum, slots, lam, gain_ref, at, wide):
        mixture = accum[parts[0]] / total[slots[0]] - lam * accum[parts[1]] / total[slots[1]]
        out_ref[:, at : at + wide] = rms_norm(mixture, gain_ref[...]).astype(out_ref.dtype)

    for head in range(heads_a):
        parts = (head, heads_a + head)
        finish(head, parts, accum_a, parts, lambda_ref[0:1, head : head + 1], gain_a_ref,
               head * 2 * DA, 2 * DA)
    for head in range(heads_b):
        parts = (head, heads_b + head)
        slots = (2 * heads_a + head, 2 * heads_a + heads_b + head)
        finish(head, parts, accum_b, slots, lambda_ref[0:1, heads_a + head : heads_a + head + 1],
               gain_b_ref, heads_a * 2 * DA + head * 2 * DB, 2 * DB)

    def settle(back, carry):
        @pl.when(chip - back >= 0)
        def _():
            index = (chip - back) * CORES + core

            @pl.when(chip < chips - 1)
            def _():
                copy_up(back, index).wait_send()

            copy_side(back, index).wait_send()

        return carry

    lax.fori_loop(0, chips, settle, 0)


def attend_blocks(queries, own, lambdas, gain_a, gain_b, chips, heads_a, heads_b):
    rows, width = own.shape
    vmem = pl.BlockSpec(memory_space=pltpu.VMEM)
    return pl.pallas_call(
        lambda *refs: attend_kernel(chips, heads_a, heads_b, *refs),
        name="attend_blocks",
        out_shape=jax.ShapeDtypeStruct((rows, heads_a * 2 * DA + heads_b * 2 * DB), jnp.bfloat16),
        in_specs=[vmem, pl.BlockSpec(memory_space=pl.ANY), vmem, vmem, vmem],
        out_specs=vmem,
        scratch_shapes=[
            pltpu.VMEM((chips * CORES, rows, width), own.dtype),
            pltpu.VMEM((2 * (heads_a + heads_b), rows, 1), jnp.float32),
            pltpu.VMEM((2 * (heads_a + heads_b), rows, 1), jnp.float32),
            pltpu.VMEM((2 * heads_a, rows, 2 * DA), jnp.float32),
            pltpu.VMEM((2 * heads_b, rows, 2 * DB), jnp.float32),
            pltpu.SemaphoreType.DMA,
            pltpu.SemaphoreType.DMA((chips,)),
            pltpu.SemaphoreType.DMA((chips,)),
            pltpu.SemaphoreType.DMA((chips * CORES,)),
        ],
        compiler_params=pltpu.CompilerParams(
            collective_id=3, has_side_effects=True, vmem_limit_bytes=VMEM_BYTES
        ),
    )(queries, own, lambdas, gain_a, gain_b)


def pivots_of(chips, slices):
    return [1, chips - 2, 0, chips - 2] if slices == chips == 4 else None


def sliced_kernel(
    chips, tps, heads_a, heads_b, pivots,
    q_ref, k_ref, va_ref, vb_ref, lambda_ref, gain_a_ref, gain_b_ref, out_ref,
    kvs, qs, accum, top, total, o_out, o_all,
    load_sem, q_send, q_recv, dn_send, up_send, kv_recv, side_send, o_send, o_recv,
):
    chip, core, tp = place()
    rows = out_ref.shape[0]
    slices = len(pivots)
    key_width = 2 * DA
    me = chip * CORES + core

    def pivot(number):
        if isinstance(number, int):
            return pivots[number]
        return sum(jnp.where(number == n, pivots[n], 0) for n in range(slices))

    loads = []
    for number in range(slices):
        if number < heads_a:
            head, stride, base, v_ref = number, heads_a * DA, 0, va_ref
        else:
            head, stride, base, v_ref = number - heads_a, heads_b * DB, 2 * heads_a * DA, vb_ref
        moves = []
        for pair in range(2):
            cols = pl.ds(base + pair * stride + head * DA, DA)
            spot = pl.ds(pair * DA, DA)
            moves.append((q_ref.at[:, cols], qs.at[chip, number, :, spot]))
            moves.append((k_ref.at[:, cols], kvs.at[me, number, :, spot]))
        moves.append(
            (v_ref.at[:, pl.ds(head * 2 * DA, 2 * DA)], kvs.at[me, number, :, pl.ds(key_width, 2 * DA)])
        )
        loads.append([
            pltpu.make_async_copy(src, dst, load_sem.at[number, place_in])
            for place_in, (src, dst) in enumerate(moves)
        ])
    order = sorted(range(slices), key=lambda n: pivots[n])
    for number in order:
        for copy in loads[number]:
            copy.start()
    greet(chips, 1)

    def remote(src, dst, send, recv, sp_to):
        return pltpu.make_async_remote_copy(
            src_ref=src, dst_ref=dst, send_sem=send, recv_sem=recv,
            device_id={"sp": sp_to, "tp": tp}, device_id_type=MESH,
        )

    def send_q(number):
        ref = qs.at[chip, number]
        return remote(ref, ref, q_send.at[number], q_recv.at[chip, number],
                      pivot(number) * CORES + core)

    def send_kv(number, chip_to, sem):
        ref = kvs.at[me, number]
        return remote(ref, ref, sem, kv_recv.at[me, number], chip_to * CORES + core)

    def send_dn(number):
        return send_kv(number, pivot(number), dn_send.at[number])

    def send_up(number, step):
        return send_kv(number, chip + step, up_send.at[number, step - 1])

    def send_side(chip_of, number):
        ref = kvs.at[chip_of * CORES + core, number]
        return remote(ref, ref, side_send.at[chip_of, number],
                      kv_recv.at[chip_of * CORES + core, number], chip * CORES + 1 - core)

    def send_out(query, number):
        return remote(o_out.at[query, number], o_all.at[number], o_send.at[query, number],
                      o_recv.at[number], query * CORES + core)

    def arrived(ref, sem):
        pltpu.make_async_copy(ref, ref, sem).wait()

    for number in order:
        for copy in loads[number]:
            copy.wait()

        @pl.when(chip > pivots[number])
        def _():
            send_q(number).start()

        @pl.when(chip <= pivots[number])
        def _():
            send_side(chip, number).start()

    for number in order:
        @pl.when(chip > pivots[number])
        def _():
            send_dn(number).start()

    for step in reversed(range(1, chips)):
        for number in order:
            @pl.when(chip + step <= pivots[number])
            def _():
                send_up(number, step).start()

    ahead = lax.broadcasted_iota(jnp.int32, (rows, rows), 0) - lax.broadcasted_iota(
        jnp.int32, (rows, rows), 1
    )
    low_half = lax.broadcasted_iota(jnp.int32, (rows, DA), 1) < DB

    def step_one(query, number, slot, q, kv_chip, pair, v_at, wide, acc_at, size, masked):
        tiles = []
        for side in range(CORES):
            key = kvs[kv_chip * CORES + side, number, :, pair * DA : (pair + 1) * DA]
            scores = lax.dot_general(
                q, key, (((1,), (1,)), ((), ())), preferred_element_type=jnp.float32
            )
            if masked:
                scores = jnp.where(ahead + (core - side) * rows >= 0, scores, -1e30)
            tiles.append(scores)
        before = top[query, number, slot]
        after = jnp.maximum(
            before, jnp.max(jnp.maximum(tiles[0], tiles[1]), -1, keepdims=True)
        )
        factor = size ** (-0.5) * LOG2E
        terms = [jnp.exp2((scores - after) * factor) for scores in tiles]
        rescale = jnp.exp2((before - after) * factor)
        top[query, number, slot] = after
        total[query, number, slot] = total[query, number, slot] * rescale + jnp.sum(
            terms[0] + terms[1], -1, keepdims=True
        )
        fresh = sum(
            jnp.dot(
                terms[side].astype(jnp.bfloat16),
                kvs[kv_chip * CORES + side, number, :, v_at : v_at + wide],
                preferred_element_type=jnp.float32,
            )
            for side in range(CORES)
        )
        span = slice(acc_at, acc_at + wide)
        accum[query, number, pair, :, span] = accum[query, number, pair, :, span] * rescale + fresh

    def flash_a(query, kv_chip, number, masked):
        for pair in range(2):
            step_one(query, number, pair, qs[query, number, :, pair * DA : (pair + 1) * DA],
                     kv_chip, pair, key_width, 2 * DA, 0, DA, masked)

    def flash_b(query, kv_chip, number, masked):
        for pair in range(2):
            both = qs[query, number, :, pair * DA : (pair + 1) * DA]
            for head in range(2):
                keep = low_half if head == 0 else jnp.logical_not(low_half)
                q = jnp.where(keep, both, jnp.zeros_like(both))
                step_one(query, number, pair * 2 + head, q, kv_chip, pair,
                         key_width + head * 2 * DB, 2 * DB, head * 2 * DB, DB, masked)

    def relevant(query, number):
        return jnp.where(query == chip, pivot(number) >= chip, pivot(number) == chip)

    def over(body):
        def run_a(number, carry):
            body(number, flash_a)
            return carry

        def run_b(number, carry):
            body(number, flash_b)
            return carry

        lax.fori_loop(0, heads_a, run_a, 0)
        lax.fori_loop(heads_a, slices, run_b, 0)

    def pair_up(query, kv_chip, first, number, flash):
        @pl.when(relevant(query, number))
        def _():
            @pl.when(first)
            def _():
                top[query, number] = jnp.full(top.shape[2:], -1e30, jnp.float32)
                total[query, number] = jnp.zeros(total.shape[2:], jnp.float32)
                accum[query, number] = jnp.zeros(accum.shape[2:], jnp.float32)

            @pl.when(query == kv_chip)
            def _():
                flash(query, kv_chip, number, True)

            @pl.when(query != kv_chip)
            def _():
                flash(query, kv_chip, number, False)

    def mix(query, number, slots, spans, lam, gain_ref):
        mixture = (
            accum[query, number, 0, :, spans] / total[query, number, slots[0]]
            - lam * accum[query, number, 1, :, spans] / total[query, number, slots[1]]
        )
        return rms_norm(mixture, gain_ref[...]).astype(jnp.bfloat16)

    def finish(query, number, flash):
        @pl.when(relevant(query, number))
        def _():
            if flash is flash_a:
                lam = lambda_ref[0, tp * heads_a + number]
                made = [mix(query, number, (0, 1), slice(0, 2 * DA), lam, gain_a_ref)]
            else:
                made = []
                for head in range(2):
                    lam = lambda_ref[
                        0, tps * heads_a + tp * heads_b + (number - heads_a) * 2 + head
                    ]
                    made.append(
                        mix(query, number, (head, 2 + head),
                            slice(head * 2 * DB, (head + 1) * 2 * DB), lam, gain_b_ref)
                    )
            wide = 2 * DA // len(made)
            for place_in, values in enumerate(made):
                span = slice(place_in * wide, (place_in + 1) * wide)

                @pl.when(query == chip)
                def _():
                    o_all[number, :, span] = values

                @pl.when(query != chip)
                def _():
                    o_out[query, number, :, span] = values

            @pl.when(query != chip)
            def _():
                send_out(query, number).start()

    above = chips - 1 - chip

    def event(number_of, carry):
        is_own = number_of == 0
        is_query = (number_of > 0) & (number_of <= above)
        is_below = (number_of > above) & (number_of <= above + chip)
        is_above = number_of > above + chip
        source = jnp.where(
            number_of <= above,
            chip + number_of,
            jnp.where(is_below, chip - (number_of - above), number_of - above),
        )
        kv_chip = jnp.where(number_of <= above, chip, source)
        low = jnp.where(is_below, chip, source)
        high = jnp.where(number_of <= above, source, chips - 1)

        def wait_q(number, carry):
            @pl.when(is_query & (pivot(number) == chip))
            def _():
                arrived(qs.at[source, number], q_recv.at[source, number])

            return carry

        def needs(number):
            return jnp.where(source > chip, pivot(number) == chip, pivot(number) >= chip)

        def wait_kv(number, carry):
            @pl.when((is_below | is_above) & needs(number))
            def _():
                index = source * CORES + core
                arrived(kvs.at[index, number], kv_recv.at[index, number])
                send_side(source, number).start()

            return carry

        def wait_side(number, carry):
            @pl.when((is_own | is_below | is_above) & needs(number))
            def _():
                index = source * CORES + 1 - core
                arrived(kvs.at[index, number], kv_recv.at[index, number])

            return carry

        def body(number, flash):
            wait_q(number, 0)
            wait_kv(number, 0)
            wait_side(number, 0)

            def queries(query, carry):
                pair_up(query, kv_chip, kv_chip == chip, number, flash)

                @pl.when(
                    ((query == chip) & (number_of == jnp.where(chip > 0, above + chip, 0)))
                    | (is_above & (query == source))
                )
                def _():
                    finish(query, number, flash)

                return carry

            lax.fori_loop(low, high + 1, queries, 0)

        over(body)
        return carry

    lax.fori_loop(0, 1 + above + chips - 1, event, 0)

    for number in range(slices):
        @pl.when(chip > pivots[number])
        def _():
            arrived(o_all.at[number], o_recv.at[number])

        out_ref[:, number * 2 * DA : (number + 1) * 2 * DA] = o_all[number]

    for number in range(slices):
        @pl.when(chip > pivots[number])
        def _():
            send_q(number).wait_send()
            send_dn(number).wait_send()

        for step in range(1, chips):
            @pl.when(chip + step <= pivots[number])
            def _():
                send_up(number, step).wait_send()

        for chip_of in range(chips):
            @pl.when(jnp.where(chip_of > chip, pivots[number] == chip, pivots[number] >= chip))
            def _():
                send_side(chip_of, number).wait_send()

            @pl.when((chip_of > chip) & (pivots[number] == chip))
            def _():
                send_out(chip_of, number).wait_send()


def attend_sliced(queries, keys, values, lambdas, gain_a, gain_b, chips, tps, heads_a, heads_b, pivots):
    rows = keys.shape[0]
    slices = len(pivots)
    vmem = pl.BlockSpec(memory_space=pltpu.VMEM)
    any_space = pl.BlockSpec(memory_space=pl.ANY)
    dma = pltpu.SemaphoreType.DMA
    return pl.pallas_call(
        lambda *refs: sliced_kernel(chips, tps, heads_a, heads_b, pivots, *refs),
        name="attend_sliced",
        out_shape=jax.ShapeDtypeStruct((rows, slices * 2 * DA), jnp.bfloat16),
        in_specs=[any_space] * 4 + [pl.BlockSpec(memory_space=pltpu.SMEM), vmem, vmem],
        out_specs=vmem,
        scratch_shapes=[
            pltpu.VMEM((chips * CORES, slices, rows, 4 * DA), jnp.bfloat16),
            pltpu.VMEM((chips, slices, rows, 2 * DA), jnp.bfloat16),
            pltpu.VMEM((chips, slices, 2, rows, 2 * DA), jnp.float32),
            pltpu.VMEM((chips, slices, 4, rows, 1), jnp.float32),
            pltpu.VMEM((chips, slices, 4, rows, 1), jnp.float32),
            pltpu.VMEM((chips, slices, rows, 2 * DA), jnp.bfloat16),
            pltpu.VMEM((slices, rows, 2 * DA), jnp.bfloat16),
            dma((slices, 5)),
            dma((slices,)),
            dma((chips, slices)),
            dma((slices,)),
            dma((slices, chips - 1)),
            dma((chips * CORES, slices)),
            dma((chips, slices)),
            dma((chips, slices)),
            dma((slices,)),
        ],
        compiler_params=pltpu.CompilerParams(
            collective_id=6, has_side_effects=True, vmem_limit_bytes=VMEM_BYTES
        ),
    )(queries, keys, *values, lambdas, gain_a, gain_b)


def share_kernel(tps, part_ref, out_ref, arrived, send_sem, recv_sem):
    tp = lax.axis_index("tp")
    barrier = pltpu.get_barrier_semaphore()
    for step in range(1, tps):
        pl.semaphore_signal(barrier, inc=1, device_id={"tp": (tp + step) % tps}, device_id_type=MESH)
    pl.semaphore_wait(barrier, tps - 1)
    started = []
    for step in range(1, tps):
        other = (tp + step) % tps
        copy = pltpu.make_async_remote_copy(
            src_ref=part_ref.at[other], dst_ref=arrived.at[step - 1], send_sem=send_sem.at[step - 1],
            recv_sem=recv_sem.at[step - 1], device_id={"tp": other}, device_id_type=MESH,
        )
        copy.start()
        started.append(copy)
    rows = out_ref.shape[0]
    chunk = min(rows, 16)
    for step in range(1, tps):
        started[step - 1].wait()

        @pl.loop(0, rows // chunk)
        def _(part):
            span = pl.ds(pl.multiple_of(part * chunk, chunk), chunk)
            first = part_ref[tp, span, :].astype(jnp.float32) if step == 1 else out_ref[span, :]
            out_ref[span, :] = first + arrived[step - 1, span, :].astype(jnp.float32)


def share_rows(parts, tps):
    _, rows, width = parts.shape
    vmem = pl.BlockSpec(memory_space=pltpu.VMEM)
    return pl.pallas_call(
        lambda *refs: share_kernel(tps, *refs),
        name="share_rows",
        out_shape=jax.ShapeDtypeStruct((rows, width), jnp.float32),
        in_specs=[vmem],
        out_specs=vmem,
        scratch_shapes=[
            pltpu.VMEM((tps - 1, rows, width), parts.dtype),
            pltpu.SemaphoreType.DMA((tps - 1,)),
            pltpu.SemaphoreType.DMA((tps - 1,)),
        ],
        compiler_params=pltpu.CompilerParams(collective_id=4, has_side_effects=True),
    )(parts)


def spread_pairs(queries, heads):
    rows = queries.shape[0]
    pairs = queries.reshape(rows, 2 * heads // 2, 1, 2, DB)
    keep = jnp.eye(2, dtype=queries.dtype).reshape(1, 1, 2, 2, 1)
    return (pairs * keep).reshape(rows, 2 * heads * 2 * DB)


def expert_parts(gathered, expert, experts, capacity, width, weights):
    gate, up, down = weights
    blocks, rows, _ = gathered.shape
    shares = lax.dynamic_slice_in_dim(gathered[:, :, width:], expert, 1, 2)[:, :, 0]
    named = shares > 0
    order = jnp.arange(rows, dtype=jnp.int32)
    slots = jnp.dot(
        named.astype(jnp.bfloat16),
        (order[:, None] < order[None, :]).astype(jnp.bfloat16),
        preferred_element_type=jnp.float32,
    ).astype(jnp.int32)
    picks = (slots[:, None, :] == jnp.arange(capacity, dtype=jnp.int32)[None, :, None]) & named[:, None, :]
    rows_in = jnp.einsum(
        "bct,btd->bcd",
        picks.astype(jnp.bfloat16),
        gathered[:, :, :width],
        preferred_element_type=jnp.float32,
    ).astype(jnp.bfloat16)
    rows_in = rows_in.reshape(blocks * capacity, width)
    gate_pre = jnp.dot(rows_in, gate, preferred_element_type=jnp.float32)
    up_pre = jnp.dot(rows_in, up, preferred_element_type=jnp.float32)
    glu_part = jnp.minimum(gate_pre, 7.0)
    lin_part = jnp.clip(up_pre, -7.0, 7.0)
    hidden = (glu_part * jax.nn.sigmoid(1.702 * glu_part) * (lin_part + 1.0)).astype(jnp.bfloat16)
    outs = jnp.dot(hidden, down, preferred_element_type=jnp.float32).astype(jnp.bfloat16)
    back = jnp.where(picks, shares[:, None, :], 0).astype(jnp.bfloat16)
    return jnp.einsum(
        "bct,bcd->btd",
        back,
        outs.reshape(blocks, capacity, width),
        preferred_element_type=jnp.float32,
    ).astype(jnp.bfloat16)


def meet(chips, tps):
    chip, core, tp = place()
    barrier = pltpu.get_barrier_semaphore()
    others = 0
    for chip_step in range(chips):
        for core_step in range(CORES):
            for tp_step in range(tps):
                if chip_step + core_step + tp_step > 0:
                    others += 1
                    pl.semaphore_signal(
                        barrier,
                        inc=1,
                        device_id={
                            "sp": (chip + chip_step) % chips * CORES + (core + core_step) % CORES,
                            "tp": (tp + tp_step) % tps,
                        },
                        device_id_type=MESH,
                    )
    pl.semaphore_wait(barrier, others)


def group_at(chip, chips, step):
    near = jnp.minimum(chip, chips - 1 - chip)
    both = jnp.where(step % 2 == 1, chip - (step + 1) // 2, chip + step // 2)
    past = jnp.where(chip <= chips - 1 - chip, chip + step - near, chip - step + near)
    return jnp.where(step <= 2 * near, both, past)


def experts_kernel(
    chips, tps, capacity,
    heads_ref, out_a_ref, out_b_ref, residual_ref, gain_mix_ref, gain_pre_ref,
    meta_ref, gate_ref, up_ref, down_ref, gain_ref, out_ref,
    mixers, mix_out, mix_own, mix_in, base_ref, mix_send, mix_recv,
    rows_all, meta_all, gate, up, down, rows_in, hidden, outs, back, part, core_in, x_in, z_in,
    z_near, z_far, sums,
    load_sem, weight_sem, row_sem, meta_send, meta_recv, up_sem, dn_sem, x_sem, side_sem,
    core_send, core_recv, xs_send, xs_recv, zs_send, zs_recv,
    zn_send, zn_recv, zf_recv,
):
    chip, core, tp = place()
    experts = meta_ref.shape[0] // 2
    piece_rows, width = rows_all.shape[2], rows_all.shape[3]
    rows = piece_rows * CUTS
    ff = gate.shape[1]
    members = CORES * tps
    side_sp = chip * CORES + 1 - core

    def blk(chip_of, core_of, tp_of):
        return (chip_of * CORES + core_of) * tps + tp_of

    def remote(src, dst, send, recv, sp_to, tp_to):
        return pltpu.make_async_remote_copy(
            src_ref=src, dst_ref=dst, send_sem=send, recv_sem=recv,
            device_id={"sp": sp_to, "tp": tp_to}, device_id_type=MESH,
        )

    def rows_copy(block, piece, send, sp_to, tp_to):
        ref = rows_all.at[block, piece]
        return remote(ref, ref, send, row_sem.at[block, piece], sp_to, tp_to)

    def go_up(chip_of, step, piece):
        return rows_copy(blk(chip_of, core, (tp + step) % tps), piece,
                         up_sem.at[chip_of, step, piece], (chip + 1) * CORES + core, tp)

    def go_dn(chip_of, step, piece):
        return rows_copy(blk(chip_of, core, (tp + step) % tps), piece,
                         dn_sem.at[chip_of, step, piece], (chip - 1) * CORES + core, tp)

    def go_on(chip_of, step, piece, upward, downward):
        if upward:
            @pl.when(chip < chips - 1)
            def _():
                go_up(chip_of, step, piece).start()

        if downward:
            @pl.when(chip > 0)
            def _():
                go_dn(chip_of, step, piece).start()

        go_side(chip_of, (tp + step) % tps, piece).start()

    def go_x(chip_of, step, piece):
        return rows_copy(blk(chip_of, core, tp), piece, x_sem.at[chip_of, step - 1, piece],
                         chip * CORES + core, (tp + step) % tps)

    def go_side(chip_of, tp_of, piece):
        return rows_copy(blk(chip_of, core, tp_of), piece, side_sem.at[chip_of, tp_of, piece],
                         side_sp, tp)

    def wait_rows(block, piece):
        ref = rows_all.at[block, piece]
        pltpu.make_async_copy(ref, ref, row_sem.at[block, piece]).wait()

    mine = blk(chip, core, tp)
    deep = out_a_ref.shape[0]
    loads = [
        pltpu.make_async_copy(src, mixers.at[number], load_sem.at[number])
        for number, src in enumerate((out_a_ref, out_b_ref))
    ]
    weights = [
        pltpu.make_async_copy(src, dst, weight_sem.at[number])
        for number, (src, dst) in enumerate(((gate_ref, gate), (up_ref, up), (down_ref, down)))
    ]
    for copy in loads:
        copy.start()
    meta_all[mine] = meta_ref[...]
    meet(chips, tps)

    def meta_copy(number, chip_step, core_step, tp_step):
        return remote(
            meta_ref, meta_all.at[mine], meta_send.at[number], meta_recv.at[mine],
            (chip + chip_step) % chips * CORES + (core + core_step) % CORES, (tp + tp_step) % tps,
        )

    meta_steps = [
        (chip_step, core_step, tp_step)
        for chip_step in range(chips) for core_step in range(CORES) for tp_step in range(tps)
        if chip_step + core_step + tp_step > 0
    ]
    for number, steps in enumerate(meta_steps):
        meta_copy(number, *steps).start()

    def project(tp_of, store):
        wide = min(width, 512)
        span = pl.ds(pl.multiple_of(tp_of * rows, rows), rows)

        @pl.loop(0, width // wide)
        def _(number):
            cols = pl.ds(pl.multiple_of(number * wide, wide), wide)
            made = sum(
                jnp.dot(
                    heads_ref[span, half * deep : (half + 1) * deep], mixers[half, :, cols],
                    preferred_element_type=jnp.float32,
                )
                for half in range(2)
            )
            store(cols, made.astype(jnp.bfloat16).reshape(CUTS, piece_rows, wide))

    def mix_copy(step, piece):
        return remote(mix_out.at[step - 1, piece], mix_in.at[step - 1, piece],
                      mix_send.at[step - 1, piece], mix_recv.at[step - 1, piece],
                      chip * CORES + core, (tp + step) % tps)

    for copy in loads:
        copy.wait()
    for copy in weights:
        copy.start()
    for step in range(1, tps):
        def keep_other(cols, values):
            mix_out[step - 1, :, :, cols] = values

        project((tp + step) % tps, keep_other)
        for piece in range(CUTS):
            mix_copy(step, piece).start()

    def keep_own(cols, values):
        mix_own[:, :, cols] = values

    project(tp, keep_own)
    for piece in range(CUTS):
        for step in range(1, tps):
            ref = mix_in.at[step - 1, piece]
            pltpu.make_async_copy(ref, ref, mix_recv.at[step - 1, piece]).wait()

        @pl.loop(0, piece_rows // 16)
        def _(number):
            span = pl.ds(pl.multiple_of(number * 16, 16), 16)
            mixed = mix_own[piece, span, :].astype(jnp.float32)
            for step in range(1, tps):
                mixed = mixed + mix_in[step - 1, piece, span, :].astype(jnp.float32)
            after = (
                residual_ref[piece, span, :].astype(jnp.float32) + rms_norm(mixed, gain_mix_ref[...])
            ).astype(jnp.bfloat16)
            base_ref[piece, span, :] = after
            rows_all[mine, piece, span, :] = rms_norm(
                after.astype(jnp.float32), gain_pre_ref[...]
            ).astype(jnp.bfloat16)

        for step in range(1, tps):
            go_x(chip, step, piece).start()

        go_on(chip, 0, piece, True, True)

    for piece in EARLY:
        for step in range(1, tps):
            wait_rows(blk(chip, core, (tp + step) % tps), piece)
            go_on(chip, step, piece, True, True)

    def relay(chip_of, piece, upward):
        for step in range(tps if piece in EARLY else 1):
            wait_rows(blk(chip_of, core, (tp + step) % tps), piece)
            if piece not in EARLY:
                for tp_step in range(1, tps):
                    go_x(chip_of, tp_step, piece).start()
            go_on(chip_of, step, piece, upward, not upward)

    def compute(group, between):
        order = lax.broadcasted_iota(jnp.int32, (rows, rows), 0).astype(jnp.float32)
        expert = chip * CORES + core
        between(0)
        for member in range(members):
            block = group * members + member
            slot = meta_all[block, pl.ds(expert, 1), :]
            share = meta_all[block, pl.ds(experts + expert, 1), :]
            hit = slot == order
            picks = jnp.where(hit[:capacity], 1.0, 0.0).astype(jnp.bfloat16)
            back[member] = jnp.where(hit, share, 0.0).T.astype(jnp.bfloat16)
            values = rows_all[block].reshape(rows, width)
            rows_in[member * capacity : (member + 1) * capacity, :] = jnp.dot(
                picks, values, preferred_element_type=jnp.float32
            ).astype(jnp.bfloat16)
        cut = min(ff, 512)
        wide = min(width, 512)
        split = min(CUTS // 2, ff // cut)

        @pl.loop(0, ff // cut)
        def _(number):
            for piece in range(1, split):
                @pl.when(number == piece)
                def _():
                    between(piece)

            cols = pl.ds(pl.multiple_of(number * cut, cut), cut)
            gate_pre = jnp.dot(rows_in[...], gate[:, cols], preferred_element_type=jnp.float32)
            up_pre = jnp.dot(rows_in[...], up[:, cols], preferred_element_type=jnp.float32)
            glu_part = jnp.minimum(gate_pre, 7.0)
            lin_part = jnp.clip(up_pre, -7.0, 7.0)
            hidden[:, cols] = (
                glu_part * jax.nn.sigmoid(1.702 * glu_part) * (lin_part + 1.0)
            ).astype(jnp.bfloat16)

        @pl.loop(0, width // wide)
        def _(number):
            for piece in range(split, min(CUTS, split + width // wide)):
                @pl.when(number + split == piece)
                def _():
                    between(piece)

            cols = pl.ds(pl.multiple_of(number * wide, wide), wide)
            outs[:, cols] = jnp.dot(
                hidden[...], down[:, cols], preferred_element_type=jnp.float32
            ).astype(jnp.bfloat16)

        for piece in range(split + width // wide, CUTS):
            between(piece)

        @pl.loop(0, members)
        def _(member):
            span = pl.ds(pl.multiple_of(member * capacity, 16), capacity)
            spread = jnp.dot(
                back[member, :, :capacity], outs[span, :], preferred_element_type=jnp.float32
            ).astype(jnp.bfloat16)
            part[group * members + member] = spread.reshape(CUTS, piece_rows, width)

    def add(target, index, source, source_index):
        chunk = min(piece_rows, 16)

        @pl.loop(0, piece_rows // chunk)
        def _(number):
            span = pl.ds(pl.multiple_of(number * chunk, chunk), chunk)
            target[index + (span,)] = (
                target[index + (span,)].astype(jnp.float32)
                + source[source_index + (span,)].astype(jnp.float32)
            ).astype(target.dtype)

    def core_copy(group, tp_of, piece):
        return remote(part.at[blk(group, 1 - core, tp_of), piece], core_in.at[group, tp_of, piece],
                      core_send.at[group, tp_of, piece], core_recv.at[group, tp_of, piece],
                      side_sp, tp)

    def part_x(group, step, piece):
        return remote(part.at[blk(group, core, (tp + step) % tps), piece],
                      x_in.at[group, step - 1, piece], xs_send.at[group, step - 1, piece],
                      xs_recv.at[group, step - 1, piece], chip * CORES + core, (tp + step) % tps)

    def far_z(way, group, piece, last):
        dst, recv, chip_to = (
            (z_far.at[way, piece], zf_recv.at[way, piece], group) if last
            else (z_in.at[way, group, piece], zs_recv.at[way, group, piece], chip + 1 - 2 * way)
        )
        return remote(part.at[blk(group, core, tp), piece], dst, zs_send.at[way, group, piece], recv,
                      chip_to * CORES + core, tp)

    def near_z(way, step, piece):
        group = chip + 1 - 2 * way
        return remote(part.at[blk(group, core, (tp + step) % tps), piece],
                      z_near.at[way, step, piece], zn_send.at[way, step, piece],
                      zn_recv.at[way, step, piece], group * CORES + core, tp)

    def distance(way, group):
        return group - chip if way == 0 else chip - group

    def far(group):
        return (group - chip >= 2) | (chip - group >= 2)

    def go_far(way, group, piece):
        @pl.when(distance(way, group) == 2)
        def _():
            far_z(way, group, piece, True).start()

        @pl.when(distance(way, group) > 2)
        def _():
            far_z(way, group, piece, False).start()

    def arrived(ref, sem):
        pltpu.make_async_copy(ref, ref, sem).wait()

    steps_x = list(range(1, tps)) + [0]

    def hand_over(group):
        for step in steps_x:
            for piece in range(CUTS):
                core_copy(group, (tp + step) % tps, piece).start()

    def cross(group):
        for step in steps_x:
            tp_of = (tp + step) % tps
            for piece in range(CUTS):
                arrived(core_in.at[group, tp_of, piece], core_recv.at[group, tp_of, piece])
                add(part, (blk(group, core, tp_of), piece), core_in, (group, tp_of, piece))
                if step > 0:
                    @pl.when(far(group))
                    def _():
                        part_x(group, step, piece).start()

                for way in range(2):
                    @pl.when(distance(way, group) == 1)
                    def _():
                        near_z(way, step, piece).start()

    def settle(group):
        @pl.when(far(group))
        def _():
            for piece in range(CUTS):
                for step in range(1, tps):
                    arrived(x_in.at[group, step - 1, piece], xs_recv.at[group, step - 1, piece])
                    add(part, (blk(group, core, tp), piece), x_in, (group, step - 1, piece))

                @pl.when((chip == 0) & (group > 0))
                def _():
                    go_far(0, group, piece)

                @pl.when((chip == chips - 1) & (group < chips - 1))
                def _():
                    go_far(1, group, piece)

    def relays(step, piece):
        @pl.when((step < chips) & (chip - step >= 0))
        def _():
            relay(chip - step, piece, True)

        @pl.when((step < chips) & (chip + step < chips))
        def _():
            relay(chip + step, piece, False)

    def wave(step, carry):
        group = group_at(chip, chips, step - 1)
        for piece in range(CUTS):
            if piece not in EARLY:
                for tp_step in range(1, tps):
                    tp_of = (tp + tp_step) % tps
                    wait_rows(blk(group, core, tp_of), piece)
                    go_side(group, tp_of, piece).start()

        @pl.when(step == 1)
        def _():
            for steps in meta_steps:
                block = blk((chip + steps[0]) % chips, (core + steps[1]) % CORES, (tp + steps[2]) % tps)
                arrived(meta_all.at[block], meta_recv.at[block])
            for copy in weights:
                copy.wait()

        for piece in range(CUTS):
            for tp_of in range(tps):
                wait_rows(blk(group, 1 - core, tp_of), piece)
        compute(group, lambda piece: relays(step + 1, piece))
        hand_over(group)
        cross(group)
        before = group_at(chip, chips, step - 2)

        @pl.when((step > 1) & far(before))
        def _():
            settle(before)

        return carry

    for piece in range(CUTS):
        relays(1, piece)
    lax.fori_loop(1, chips + 1, wave, 0)
    for piece in range(CUTS):
        for step in range(1, tps):
            for way in range(2):
                @pl.when(chip > 0 if way == 0 else chip < chips - 1)
                def _():
                    arrived(z_near.at[way, step, piece], zn_recv.at[way, step, piece])
                    add(part, (blk(chip, core, (tp + step) % tps), piece), z_near,
                        (way, step, piece))

            part_x(chip, step, piece).start()

    settle(group_at(chip, chips, chips - 1))

    def chain(number, carry):
        for way in range(2):
            group = number if way == 0 else chips - 1 - number
            starts = chip == 0 if way == 0 else chip == chips - 1

            @pl.when((distance(way, group) >= 2) & jnp.logical_not(starts))
            def _():
                for piece in range(CUTS):
                    arrived(z_in.at[way, group, piece], zs_recv.at[way, group, piece])
                    add(part, (blk(group, core, tp), piece), z_in, (way, group, piece))
                    go_far(way, group, piece)

        return carry

    lax.fori_loop(1, chips, chain, 0)

    chunk = min(piece_rows, 16)

    def each_chunk(body):
        @pl.loop(0, piece_rows // chunk)
        def _(number):
            body(pl.ds(pl.multiple_of(number * chunk, chunk), chunk))

    for piece in range(CUTS):
        for step in range(1, tps):
            arrived(x_in.at[chip, step - 1, piece], xs_recv.at[chip, step - 1, piece])

        def begin(span):
            start = part[mine, piece, span, :].astype(jnp.float32)
            for step in range(1, tps):
                start = start + x_in[chip, step - 1, piece, span, :].astype(jnp.float32)
            sums[span, :] = start

        each_chunk(begin)
        for way in range(2):
            def more(span):
                sums[span, :] = sums[span, :] + z_near[way, 0, piece, span, :].astype(jnp.float32)

            def most(span):
                sums[span, :] = sums[span, :] + z_far[way, piece, span, :].astype(jnp.float32)

            behind = chip if way == 0 else chips - 1 - chip

            @pl.when(behind > 0)
            def _():
                arrived(z_near.at[way, 0, piece], zn_recv.at[way, 0, piece])
                each_chunk(more)

            @pl.when(behind > 1)
            def _():
                arrived(z_far.at[way, piece], zf_recv.at[way, piece])
                each_chunk(most)

        def close(span):
            out_ref[piece, span, :] = (
                base_ref[piece, span, :].astype(jnp.float32) + rms_norm(sums[span, :], gain_ref[...])
            ).astype(out_ref.dtype)

        each_chunk(close)

    for number, steps in enumerate(meta_steps):
        meta_copy(number, *steps).wait_send()
    for piece in range(CUTS):
        for step in range(1, tps):
            mix_copy(step, piece).wait_send()

    def finish(group, carry):
        for piece in range(CUTS):
            for step in range(1, tps):
                @pl.when((group == chip) | (piece not in EARLY))
                def _():
                    go_x(group, step, piece).wait_send()

                @pl.when(far(group) | (group == chip))
                def _():
                    part_x(group, step, piece).wait_send()

            for tp_of in range(tps):
                go_side(group, tp_of, piece).wait_send()

            for step in range(tps if piece in EARLY else 1):
                @pl.when((group <= chip) & (chip < chips - 1))
                def _():
                    go_up(group, step, piece).wait_send()

                @pl.when((group >= chip) & (chip > 0))
                def _():
                    go_dn(group, step, piece).wait_send()

            for way in range(2):
                @pl.when(distance(way, group) >= 2)
                def _():
                    far_z(way, group, piece, True).wait_send()

            for tp_of in range(tps):
                core_copy(group, tp_of, piece).wait_send()

        return carry

    lax.fori_loop(0, chips, finish, 0)
    for piece in range(CUTS):
        for step in range(tps):
            for way in range(2):
                @pl.when(chip < chips - 1 if way == 0 else chip > 0)
                def _():
                    near_z(way, step, piece).wait_send()


def experts_bytes(rows, width, ff, deep, chips, tps, capacity):
    blocks = chips * CORES * tps
    members = CORES * tps
    buffers = blocks * 2 + chips * (2 * tps - 1 + 2) + 2 * tps + 8
    return 2 * (
        rows * width * buffers + 3 * width * ff + members * capacity * (2 * width + ff) + 4 * rows * width
        + 2 * deep * (width + rows * tps) + (2 * tps + 1) * rows * width
    )


def run_experts(heads_out, mixers, residual, gains, meta, weights, chips, tps, capacity):
    rows, width = residual.shape
    gate, up, down = weights
    ff = gate.shape[1]
    blocks = chips * CORES * tps
    members = CORES * tps
    piece_rows = rows // CUTS
    vmem = pl.BlockSpec(memory_space=pltpu.VMEM)
    any_space = pl.BlockSpec(memory_space=pl.ANY)
    dma = pltpu.SemaphoreType.DMA
    bf16 = jnp.bfloat16
    return pl.pallas_call(
        lambda *refs: experts_kernel(chips, tps, capacity, *refs),
        name="run_experts",
        out_shape=jax.ShapeDtypeStruct((CUTS, piece_rows, width), bf16),
        in_specs=[vmem, any_space, any_space] + [vmem] * 4 + [any_space] * 3 + [vmem],
        out_specs=vmem,
        scratch_shapes=[
            pltpu.VMEM((2,) + mixers[0].shape, bf16),
            pltpu.VMEM((tps - 1, CUTS, piece_rows, width), bf16),
            pltpu.VMEM((CUTS, piece_rows, width), bf16),
            pltpu.VMEM((tps - 1, CUTS, piece_rows, width), bf16),
            pltpu.VMEM((CUTS, piece_rows, width), bf16),
            dma((tps - 1, CUTS)),
            dma((tps - 1, CUTS)),
            pltpu.VMEM((blocks, CUTS, piece_rows, width), bf16),
            pltpu.VMEM((blocks,) + meta.shape, meta.dtype),
            pltpu.VMEM(gate.shape, bf16),
            pltpu.VMEM(up.shape, bf16),
            pltpu.VMEM(down.shape, bf16),
            pltpu.VMEM((members * capacity, width), bf16),
            pltpu.VMEM((members * capacity, ff), bf16),
            pltpu.VMEM((members * capacity, width), bf16),
            pltpu.VMEM((members, rows, rows), bf16),
            pltpu.VMEM((blocks, CUTS, piece_rows, width), bf16),
            pltpu.VMEM((chips, tps, CUTS, piece_rows, width), bf16),
            pltpu.VMEM((chips, tps - 1, CUTS, piece_rows, width), bf16),
            pltpu.VMEM((2, chips, CUTS, piece_rows, width), bf16),
            pltpu.VMEM((2, tps, CUTS, piece_rows, width), bf16),
            pltpu.VMEM((2, CUTS, piece_rows, width), bf16),
            pltpu.VMEM((piece_rows, width), jnp.float32),
            dma((2,)),
            dma((3,)),
            dma((blocks, CUTS)),
            dma((blocks - 1,)),
            dma((blocks,)),
            dma((chips, tps, CUTS)),
            dma((chips, tps, CUTS)),
            dma((chips, tps - 1, CUTS)),
            dma((chips, tps, CUTS)),
            dma((chips, tps, CUTS)),
            dma((chips, tps, CUTS)),
            dma((chips, tps - 1, CUTS)),
            dma((chips, tps - 1, CUTS)),
            dma((2, chips, CUTS)),
            dma((2, chips, CUTS)),
            dma((2, tps, CUTS)),
            dma((2, tps, CUTS)),
            dma((2, CUTS)),
        ],
        compiler_params=pltpu.CompilerParams(
            collective_id=5, has_side_effects=True, vmem_limit_bytes=VMEM_BYTES
        ),
    )(
        heads_out, *mixers, residual.reshape(CUTS, piece_rows, width), gains[0], gains[1], meta, gate, up,
        down, gains[2],
    ).reshape(rows, width)


def slot_table(routes, route_weights, experts):
    rows = routes.shape[0]
    chosen = routes[None, :, :] == jnp.arange(experts, dtype=jnp.int32)[:, None, None]
    shares = jnp.sum(jnp.where(chosen, route_weights[None], 0.0), 2)
    named = jnp.any(chosen, 2)
    order = jnp.arange(rows, dtype=jnp.int32)
    slots = jnp.dot(
        named.astype(jnp.bfloat16),
        (order[:, None] < order[None, :]).astype(jnp.bfloat16),
        preferred_element_type=jnp.float32,
    )
    return jnp.concatenate([jnp.where(named, slots, -1.0), shares], 0)


def spread_experts(normed, routes, route_weights, seq_slot, experts, capacity, chips, tps, weights):
    width = normed.shape[1]
    extra = -(-experts // 128) * 128
    shares = jnp.sum(
        jnp.where(
            routes[:, :, None] == jnp.arange(extra, dtype=jnp.int32)[None, None, :],
            route_weights[:, :, None],
            0.0,
        ),
        1,
    ).astype(jnp.bfloat16)
    gathered = gather_rows(jnp.concatenate([normed, shares], 1), chips, tps)
    parts = expert_parts(gathered, seq_slot, experts, capacity, width, weights)
    return scatter_rows(parts, chips, tps)


def per_device(
    queries_a,
    keys_a,
    values_a,
    queries_b,
    keys_b,
    values_b,
    lambdas,
    head_gain_a,
    head_gain_b,
    out_a,
    out_b,
    residual,
    gain_mix,
    gain_pre,
    gain_post,
    routes,
    route_weights,
    expert_gate,
    expert_up,
    expert_down,
):
    length = queries_a.shape[0]
    heads_a = queries_a.shape[2] // DA
    heads_b = queries_b.shape[2] // DB
    head_slot = lax.axis_index("tp")
    seq_slot = lax.axis_index("sp")
    experts, tps = lax.axis_size("sp"), lax.axis_size("tp")
    chips = experts // CORES
    pivots = pivots_of(chips, heads_a + heads_b // 2)
    if pivots is not None:
        heads_out = attend_sliced(
            jnp.concatenate([queries_a.reshape(length, -1), queries_b.reshape(length, -1)], 1),
            jnp.concatenate([keys_a.reshape(length, -1), keys_b.reshape(length, -1)], 1),
            (values_a, values_b), lambdas[None], head_gain_a[None], head_gain_b[None], chips, tps,
            heads_a, heads_b, pivots,
        )
    else:
        lambda_a = lax.dynamic_slice_in_dim(lambdas, head_slot * heads_a, heads_a)
        lambda_b = lax.dynamic_slice_in_dim(lambdas, HA + head_slot * heads_b, heads_b)
        own = jnp.concatenate(
            [keys_a.reshape(length, -1), values_a, keys_b.reshape(length, -1), values_b], 1
        )
        queries = jnp.concatenate(
            [queries_a.reshape(length, -1), spread_pairs(queries_b, heads_b)], 1
        )
        heads_out = attend_blocks(
            queries,
            own,
            jnp.concatenate([lambda_a, lambda_b])[None],
            head_gain_a[None],
            head_gain_b[None],
            chips,
            heads_a,
            heads_b,
        )
    sub_rows = residual.shape[0]
    top_count = routes.shape[1]
    capacity = min(sub_rows, (5 * sub_rows * top_count + 4 * experts - 1) // (4 * experts))
    width = residual.shape[1]
    slots = -(-capacity // 16) * 16
    weights = (expert_gate[0], expert_up[0], expert_down[0])
    cut = heads_a * 2 * DA
    need = experts_bytes(sub_rows, width, weights[0].shape[1], cut, chips, tps, slots)
    if out_a.shape == out_b.shape and need < VMEM_BYTES:
        return run_experts(
            heads_out, (out_a, out_b), residual, (gain_mix[None], gain_pre[None], gain_post[None]),
            slot_table(routes, route_weights, experts), weights, chips, tps, slots,
        )
    mixed = (
        jnp.dot(heads_out[:, :cut], out_a, preferred_element_type=jnp.float32)
        + jnp.dot(heads_out[:, cut:], out_b, preferred_element_type=jnp.float32)
    ).astype(jnp.bfloat16)
    mixed_rows = share_rows(mixed.reshape(tps, length // tps, -1), tps)
    after_mix = (residual.astype(jnp.float32) + rms_norm(mixed_rows, gain_mix)).astype(jnp.bfloat16)
    normed = rms_norm(after_mix.astype(jnp.float32), gain_pre).astype(jnp.bfloat16)
    routed = spread_experts(
        normed, routes, route_weights, seq_slot, experts, capacity, chips, tps,
        weights,
    )
    return (after_mix.astype(jnp.float32) + rms_norm(routed, gain_post)).astype(jnp.bfloat16)


def solution(mesh):
    in_specs = (
        P(("grp", "sp"), None, "tp"),
        P(("grp", "sp"), None, "tp"),
        P(("grp", "sp"), "tp"),
        P(("grp", "sp"), None, "tp"),
        P(("grp", "sp"), None, "tp"),
        P(("grp", "sp"), "tp"),
        P(),
        P(),
        P(),
        P("tp", None),
        P("tp", None),
        P(("grp", "sp", "tp"), None),
        P(),
        P(),
        P(),
        P(("grp", "sp", "tp"), None),
        P(("grp", "sp", "tp"), None),
        P("sp", None, "tp"),
        P("sp", None, "tp"),
        P("sp", "tp", None),
    )
    out_specs = P(("grp", "sp", "tp"), None)
    return jax.shard_map(
        per_device, mesh=mesh, in_specs=in_specs, out_specs=out_specs, check_vma=False
    )
```
